128 devices in a mesh: sp: 64 (over z, y, x), tp: 2 (over core).
Axes of the slice: x: 4, y: 4, z: 4, core: 2. Of those that a mesh axis runs over, the one named last changes fastest.
Arguments:
- cotangent: bfloat16 [24576, 2048], P('sp'), may hold values from -16 to 16
- routes: int32 [24576, 2], P('sp'), may hold values from 0 to 63, all different within a row; in each aligned block of 384 rows (0 to 383, 384 to 767, ...) at most 18 rows name the same one
- route_weight: float32 [24576, 2], P('sp'), may hold values from 0.1 to 0.9
- expert_rows: bfloat16 [64, 1152, 2048], P('sp'), may hold values from -6 to 6
- gate_w: bfloat16 [64, 2048, 1024], P('sp', None, 'tp'), may hold values from -0.125 to 0.125
- up_w: bfloat16 [64, 2048, 1024], P('sp', None, 'tp'), may hold values from -0.125 to 0.125
- down_w: bfloat16 [64, 1024, 2048], P('sp', 'tp'), may hold values from -0.1875 to 0.1875
- in_x: bfloat16 [24576, 1024], P('sp', 'tp'), may hold values from -6 to 6
- in_y: bfloat16 [24576, 1024], P('sp', 'tp'), may hold values from -6 to 6
- state: bfloat16 [24576, 1024], P('sp', 'tp'), may hold values from -6 to 6
- conv_taps: float32 [4, 1024], P(None, 'tp'), may hold values from -3 to 3
- gate_a: bfloat16 [8, 128, 128], P('tp'), may hold values from -0.5 to 0.5
- gate_x: bfloat16 [8, 128, 128], P('tp'), may hold values from -0.5 to 0.5
- decay_rate: float32 [1024], P('tp'), as said below
- out_weight: bfloat16 [2048, 1024], P(None, 'tp'), may hold values from -0.1875 to 0.1875
Outputs:
- grad_gate: bfloat16 [64, 2048, 1024], P('sp', None, 'tp')
- grad_up: bfloat16 [64, 2048, 1024], P('sp', None, 'tp')
- grad_down: bfloat16 [64, 1024, 2048], P('sp', 'tp')
- grad_proj: float32 [2048, 1024], P('sp', 'tp')
- grad_x: float32 [24576, 1024], P('sp', 'tp')
- grad_y: float32 [24576, 1024], P('sp', 'tp')
The draws below stay inside these ranges and needn't reach their ends.
Inputs may be any that keep to these rules, and one draw needn't show every extreme that they name: `routes`: among the 768 pairs of one device's rows no expert appears more than 18 times, and some expert appears exactly 18 times; a row's two experts differ. `decay_rate`: positive.
All inputs are finite; a program needn't handle non-finite values.
Results may differ from the reference program's by a relative error of at most 0.0052.
The reference program's roundings to bfloat16 on the way count: a program that leaves them out, or rounds other values in their place, can miss the bound.
Values may be sent and summed in bfloat16 or wider, within the bound.
No kernel may reach another device: no remote copies, remote signals or barrier semaphores. Data moves between devices by JAX's collectives and lax.ppermute only.
A program may use at most 128 MiB of HBM per device.

```python
import math
import jax
import jax.numpy as jnp
import numpy as np
from jax import lax

D = 2048
FF = 1024
BW = 1024
BLK = 128
TAPS = 4
TOK_DEV = 384
TOKENS = 24576
EXPERTS = 64
CAP = 18
ROWS_IN = 1152
FF_PART = 512
BLOCKS = 8
N_SP = 64
N_TP = 2


def draw_decay_rate(key, part):
    pick_key, slow_key, fast_key = jax.random.split(key, 3)
    slow_rate = jax.random.uniform(slow_key, (BW,), jnp.float32, 0.3, 1.0) * (2.3 / (4.0 * TOKENS))
    fast_rate = jax.random.uniform(fast_key, (BW,), jnp.float32, 0.0025, 0.0083)
    fast_share = 0.5
    is_fast = jax.random.uniform(pick_key, (BW,), jnp.float32) < fast_share
    return jnp.where(is_fast, fast_rate, slow_rate).astype(jnp.float32)


def strengthened(result, own_key, source, target, shards_of, factor):
    def block_of(dim):
        return (jnp.arange(result.shape[dim]) // (result.shape[dim] // shards_of)).reshape((-1,) + (1,) * (result.ndim - 1 - dim))

    near = jax.random.permutation(own_key, shards_of)[block_of(target)]
    second = (block_of(target) + shards_of // 2) % shards_of
    return jnp.where((block_of(source) == near) | (block_of(source) == second), factor * result, result)


def steps_of(own_key, dims, cuts, smallest, largest):
    loudness, own = 1.0, jax.random.fold_in(own_key, 6)
    for dim, parts in cuts:
        draws = jnp.exp(jax.random.uniform(jax.random.fold_in(own, dim), (parts,), jnp.float32, smallest / len(cuts), largest / len(cuts)))
        loudness = loudness * jnp.repeat(draws, dims[dim] // parts).reshape([-1 if axis == dim else 1 for axis in range(len(dims))])
    return loudness


def assign_block(key, own, number, rows, number_of, top, reach, lean):
    sequence = jax.random.permutation(key, number_of)
    heavy_load, usual = portions_of(number_of, rows * top, reach, lean, True), portions_of(number_of, rows * top, reach, lean, False)
    places = jnp.arange(number_of)

    def named(sizes, turn):
        used = int((sizes > 0).sum())
        fixed = max(1, used // 4)
        shifted = fixed + (places - fixed + turn * (used - fixed)) % max(1, number_of - fixed)
        return jnp.zeros((number_of,), jnp.int32).at[sequence[jnp.where(places < fixed, places, shifted)]].set(jnp.asarray(sizes, jnp.int32))

    sizes = jnp.where(number % 4 == 0, named(heavy_load, number // 4), named(usual, number - number // 4 - 1))
    mixed = jax.random.permutation(jax.random.fold_in(own, 3), number_of)
    giver, taker = mixed[0:number_of // 2 * 2:2], mixed[1:number_of // 2 * 2:2]
    slack = jnp.minimum(sizes[giver] - 1, reach - sizes[taker]) // 2
    slack = jnp.where((giver == sequence[0]) | (taker == sequence[0]) | (sizes[taker] == 0), 0, jnp.maximum(slack, 0))
    shifted = jax.random.randint(jax.random.fold_in(own, 4), (number_of // 2,), 0, 1 << 20) % (slack + 1)
    sizes = sizes.at[giver].add(-shifted).at[taker].add(shifted)
    labels = jnp.searchsorted(jnp.cumsum(sizes), jnp.arange(rows * top), side="right").astype(jnp.int32)
    table = labels.reshape(top, rows).T
    table = table[jax.random.permutation(jax.random.fold_in(own, 1), rows)]
    turn = jax.random.randint(jax.random.fold_in(own, 2), (rows, 1), 0, top)
    return jnp.take_along_axis(table, (jnp.arange(top)[None, :] + turn) % top, axis=1)


def portions_of(number_of, total, bound, lean, full):
    loads = [(1 << 20) // math.isqrt(rank ** lean) + 1 for rank in range(1, number_of + 1)]
    largest = bound if full else min(bound, max(-(-total // number_of), total * loads[0] // sum(loads)))
    least = 1 if total - largest >= number_of - 1 else 0
    given, rest = [largest] + [least] * (number_of - 1), total - largest - least * (number_of - 1)
    while rest > 0:
        candidates = [i for i in range(1, number_of) if given[i] < largest] or [i for i in range(1, number_of) if given[i] < bound]
        mass, left = sum([loads[i] for i in candidates]), rest
        for i in candidates:
            more = min(bound - given[i], max(1, left * loads[i] // mass), rest)
            given[i] = given[i] + more
            rest = rest - more
    return np.array(given)


def gaussian(stream_key, extent, deviation, most, shards=(), held_as=jnp.bfloat16):
    result = deviation * jax.random.normal(stream_key, extent, jnp.float32)
    if shards:
        result = result * steps_of(stream_key, extent, shards, -0.22, 0.18)
    return jnp.clip(result, -most, most).astype(held_as)


def noise_with(stream_key, shape, deviation, most, cuts, heavy, held_as=jnp.bfloat16):
    values = deviation * jax.random.normal(stream_key, shape, jnp.float32)
    if cuts:
        values = values * steps_of(stream_key, shape, cuts, -0.22, 0.18)
    return jnp.clip(strengthened(values, jax.random.fold_in(stream_key, 3), *heavy), -most, most).astype(held_as)


def setup_inputs(seed: int = 0) -> dict:
    key_list = jax.random.split(jax.random.key(seed), 16)
    cotangent = noise_with(key_list[0], (TOKENS, D), 1.0, 16.0, ((0, 64),), (0, 1, 64, 4.0))
    routes_keys = jax.random.split(jax.random.fold_in(key_list[1], 1), TOKENS // TOK_DEV)
    routes_turns = jax.random.permutation(jax.random.fold_in(key_list[1], 3), TOKENS // TOK_DEV)
    routes = jax.vmap(lambda own, number: assign_block(jax.random.fold_in(key_list[1], 2), own, number, TOK_DEV, EXPERTS, 2, CAP, 2))(routes_keys, routes_turns).reshape((TOKENS, 2))
    route_weight = jnp.clip(0.1 + 0.79999997 * jax.random.uniform(key_list[2], (TOKENS, 2), jnp.float32) ** steps_of(key_list[2], (TOKENS, 2), ((0, 64),), -0.2, 0.2), 0.1, 0.9)
    expert_rows = gaussian(key_list[3], (EXPERTS, ROWS_IN, D), 1.0, 6.0, ((0, 64),))
    gate_w = gaussian(key_list[4], (EXPERTS, D, FF), D ** -0.5, 0.125, ((0, 64), (2, 2)))
    up_w = gaussian(key_list[5], (EXPERTS, D, FF), D ** -0.5, 0.125, ((0, 64), (2, 2)))
    down_w = gaussian(key_list[6], (EXPERTS, FF, D), FF ** -0.5, 0.1875, ((0, 64), (1, 2)))
    in_x = gaussian(key_list[7], (TOKENS, BW), 1.0, 6.0, ((0, 64), (1, 2)))
    in_y = gaussian(key_list[8], (TOKENS, BW), 1.0, 6.0, ((0, 64), (1, 2)))
    state = gaussian(key_list[9], (TOKENS, BW), 1.0, 6.0, ((0, 64), (1, 2)))
    conv_taps = gaussian(key_list[10], (TAPS, BW), TAPS ** -0.5, 3.0, ((1, 2),), jnp.float32)
    gate_a = gaussian(key_list[11], (BLOCKS, BLK, BLK), BLK ** -0.5, 0.5, ((0, 2),))
    gate_x = gaussian(key_list[12], (BLOCKS, BLK, BLK), BLK ** -0.5, 0.5, ((0, 2),))
    decay_rate = draw_decay_rate(jax.random.fold_in(key_list[15], 71), 0)
    out_weight = gaussian(key_list[14], (D, BW), BW ** -0.5, 0.1875, ((1, 2),))
    return dict(cotangent=cotangent, routes=routes, route_weight=route_weight, expert_rows=expert_rows, gate_w=gate_w, up_w=up_w, down_w=down_w, in_x=in_x, in_y=in_y, state=state, conv_taps=conv_taps, gate_a=gate_a, gate_x=gate_x, decay_rate=decay_rate, out_weight=out_weight)


rate_scale = 8.0
floor_square = 0.01
inv_root_two = 0.7071067811865476
inv_root_tau = 0.3989422804014327

def linear_combine(earlier, later):
    return (earlier[0] * later[0], later[0] * earlier[1] + later[1])

def expert_backward(expert_item):
    saved_rows, upstream, weight_gate, weight_up, weight_down = expert_item
    pre_gate = jnp.dot(saved_rows, weight_gate, preferred_element_type=jnp.float32)
    pre_up = jnp.dot(saved_rows, weight_up, preferred_element_type=jnp.float32)
    gate_sigmoid = jax.nn.sigmoid(pre_gate)
    silu_value = pre_gate * gate_sigmoid
    active = (silu_value * pre_up).astype(jnp.bfloat16)
    grad_active = jnp.dot(upstream, weight_down.T, preferred_element_type=jnp.float32)
    grad_down = jnp.dot(active.T, upstream, preferred_element_type=jnp.float32).astype(jnp.bfloat16)
    up_adjoint = (grad_active * silu_value).astype(jnp.bfloat16)
    gate_adjoint = (grad_active * pre_up * gate_sigmoid * (1.0 + pre_gate * (1.0 - gate_sigmoid))).astype(jnp.bfloat16)
    grad_gate = jnp.dot(saved_rows.T, gate_adjoint, preferred_element_type=jnp.float32).astype(jnp.bfloat16)
    grad_up = jnp.dot(saved_rows.T, up_adjoint, preferred_element_type=jnp.float32).astype(jnp.bfloat16)
    total = jnp.zeros((saved_rows.shape[0], saved_rows.shape[1]), jnp.float32)
    for block_index in range(N_TP):
        lower = block_index * FF_PART
        piece = jnp.dot(gate_adjoint[:, lower:lower + FF_PART], weight_gate[:, lower:lower + FF_PART].T, preferred_element_type=jnp.float32)
        piece = piece + jnp.dot(up_adjoint[:, lower:lower + FF_PART], weight_up[:, lower:lower + FF_PART].T, preferred_element_type=jnp.float32)
        total = total + piece.astype(jnp.bfloat16).astype(jnp.float32)
    return (grad_gate, grad_up, grad_down, total.astype(jnp.bfloat16))

def reference(cotangent, routes, route_weight, expert_rows, gate_w, up_w, down_w, in_x, in_y, state, conv_taps, gate_a, gate_x, decay_rate, out_weight):
    pair_expert = routes.reshape(N_SP, TOK_DEV * 2)
    onehot = (pair_expert[:, :, None] == jnp.arange(EXPERTS, dtype=jnp.int32)[None, None, :]).astype(jnp.int32)
    before = (jnp.cumsum(onehot, axis=1) - onehot).astype(jnp.int32)
    position = lax.optimization_barrier(jnp.sum(before * onehot, axis=2)).astype(jnp.int32)
    source = jnp.arange(N_SP, dtype=jnp.int32)[:, None]
    target = (pair_expert * ROWS_IN + source * CAP + position).reshape(-1).astype(jnp.int32)
    token_ids = jnp.repeat(jnp.arange(TOKENS, dtype=jnp.int32), 2)
    slot_token = jnp.zeros((EXPERTS * ROWS_IN,), jnp.int32).at[target].set(token_ids)
    slot_weight = jnp.zeros((EXPERTS * ROWS_IN,), jnp.float32).at[target].set(route_weight.reshape(-1))
    upstream = (cotangent[slot_token].astype(jnp.float32) * slot_weight[:, None]).astype(jnp.bfloat16)
    upstream = upstream.reshape(EXPERTS, ROWS_IN, D)
    grad_gate, grad_up, grad_down, back_rows = lax.map(expert_backward, (expert_rows, upstream, gate_w, up_w, down_w))
    picked = back_rows.reshape(EXPERTS * ROWS_IN, D)[target].astype(jnp.float32).reshape(TOKENS, 2, D)
    stream_grad = (cotangent.astype(jnp.float32) + lax.optimization_barrier(jnp.sum(picked, axis=1))).astype(jnp.bfloat16)
    y_float = in_y.astype(jnp.float32)
    gelu_y = jax.nn.gelu(y_float, approximate=False)
    gelu_slope = 0.5 * (1.0 + lax.erf(y_float * inv_root_two)) + y_float * jnp.exp(-0.5 * y_float * y_float) * inv_root_tau
    state_float = state.astype(jnp.float32)
    mixed_out = (state_float * gelu_y).astype(jnp.bfloat16)
    grad_proj = jnp.dot(stream_grad.T, mixed_out, preferred_element_type=jnp.float32)
    grad_mixed = jnp.dot(stream_grad, out_weight, preferred_element_type=jnp.float32)
    grad_y = grad_mixed * state_float * gelu_slope
    grad_state = grad_mixed * gelu_y
    padded_x = jnp.concatenate([jnp.zeros((TAPS - 1, BW), jnp.float32), in_x.astype(jnp.float32)], axis=0)
    conv_x = conv_taps[0][None, :] * padded_x[0:TOKENS]
    for offset in range(1, TAPS):
        conv_x = conv_x + conv_taps[offset][None, :] * padded_x[offset:offset + TOKENS]
    conv_b = conv_x.astype(jnp.bfloat16).astype(jnp.float32).reshape(TOKENS, BLOCKS, BLK)
    keep_gate = jax.nn.sigmoid(jnp.einsum('tci,cij->tcj', conv_b, gate_a.astype(jnp.float32))).reshape(TOKENS, BW)
    input_gate = jax.nn.sigmoid(jnp.einsum('tci,cij->tcj', conv_b, gate_x.astype(jnp.float32))).reshape(TOKENS, BW)
    decay_step = jnp.exp(-rate_scale * keep_gate * decay_rate[None, :])
    norm_factor = jnp.sqrt(1.0 - decay_step * decay_step + floor_square)
    ahead_decay = jnp.concatenate([decay_step[1:], jnp.ones((1, BW), jnp.float32)], axis=0)
    scanned = lax.associative_scan(linear_combine, (ahead_decay[::-1], grad_state[::-1]), axis=0)
    adjoint = scanned[1][::-1]
    state_prev = jnp.concatenate([jnp.zeros((1, BW), jnp.float32), state_float[:-1]], axis=0)
    grad_norm = adjoint * conv_x * input_gate
    log_grad = adjoint * decay_step * state_prev - grad_norm * decay_step * decay_step / norm_factor
    keep_adjoint = (log_grad * (-rate_scale * decay_rate[None, :]) * keep_gate * (1.0 - keep_gate)).astype(jnp.bfloat16)
    input_adjoint = (adjoint * conv_x * norm_factor * input_gate * (1.0 - input_gate)).astype(jnp.bfloat16)
    back_keep = jnp.einsum('tcj,cij->tci', keep_adjoint.astype(jnp.float32).reshape(TOKENS, BLOCKS, BLK), gate_a.astype(jnp.float32))
    back_input = jnp.einsum('tcj,cij->tci', input_adjoint.astype(jnp.float32).reshape(TOKENS, BLOCKS, BLK), gate_x.astype(jnp.float32))
    conv_grad = adjoint * input_gate * norm_factor + back_keep.reshape(TOKENS, BW) + back_input.reshape(TOKENS, BW)
    padded_grad = jnp.concatenate([conv_grad, jnp.zeros((TAPS - 1, BW), jnp.float32)], axis=0)
    grad_x = conv_taps[0][None, :] * padded_grad[TAPS - 1:TAPS - 1 + TOKENS]
    for offset in range(1, TAPS):
        grad_x = grad_x + conv_taps[offset][None, :] * padded_grad[TAPS - 1 - offset:TAPS - 1 - offset + TOKENS]
    return (grad_gate, grad_up, grad_down, grad_proj, grad_x, grad_y)
```

```python
import jax
import jax.numpy as jnp
from jax import lax
from jax.experimental import pallas as pl
from jax.experimental.pallas import tpu as pltpu
from jax.sharding import PartitionSpec as P

rate_scale = 8.0
floor_square = 0.01
inv_root_two = 0.7071067811865476
inv_root_tau = 0.3989422804014327

f32 = jnp.float32
bf16 = jnp.bfloat16
inner = (((1,), (1,)), ((), ()))
outer = (((0,), (0,)), ((), ()))
plain = (((1,), (0,)), ((), ()))

group = 8
main = 16
extra = 2
main_rows = group * main
group_rows = group * (main + extra)
segments = 8


def dot(a, b, dims):
    return lax.dot_general(a, b, dims, preferred_element_type=f32)


def params(n=1, mb=58):
    return pltpu.CompilerParams(dimension_semantics=("arbitrary",) * n, vmem_limit_bytes=mb << 20)


def whole(shape, memory_space=None):
    return pl.BlockSpec(shape, lambda *_: (0,) * len(shape))


def pack_extras(rows, scratch):
    for j in range(8):
        scratch[pl.ds(j, group * extra, stride=8), :] = rows[:, 128 * j : 128 * (j + 1)]
    return scratch[...]


def unpack_extras(tiles, scratch):
    scratch[...] = tiles
    return jnp.concatenate(
        [scratch[pl.ds(j, group * extra, stride=8), :] for j in range(8)], axis=1
    )


def send_kernel(core_ref, routes_ref, weight_ref, cot_ref, out_ref, target_ref, slot, scratch):
    step = pl.program_id(0)
    tokens = cot_ref.shape[0]
    experts = pl.num_programs(0) * group

    @pl.when(step == 0)
    def _():
        first = routes_ref[0:1, :]
        second = routes_ref[1:2, :]
        expert = lax.broadcasted_iota(jnp.int32, (experts, tokens), 0)
        hit_first = (expert == first).astype(f32)
        hit_second = (expert == second).astype(f32)
        earlier = (
            lax.broadcasted_iota(jnp.int32, (tokens, tokens), 0)
            < lax.broadcasted_iota(jnp.int32, (tokens, tokens), 1)
        ).astype(f32)
        before = dot((hit_first + hit_second).astype(bf16), earlier.astype(bf16), plain)
        place_first = jnp.sum(before * hit_first, axis=0, keepdims=True).astype(jnp.int32)
        place_second = jnp.sum(before * hit_second, axis=0, keepdims=True).astype(jnp.int32)
        place_second = place_second + (first == second).astype(jnp.int32)
        for k, (name, place) in enumerate(((first, place_first), (second, place_second))):
            base = group_rows * (name >> 3)
            inside = name & 7
            slot[k : k + 1, :] = base + jnp.where(
                place < main, main * inside + place, main_rows + extra * inside + place - main
            )
        target_ref[...] = jnp.concatenate(
            [slot[0:2, :], jnp.zeros((6, tokens), jnp.int32)], axis=0
        )

    rows = lax.broadcasted_iota(jnp.int32, (group_rows, tokens), 0) + step * group_rows
    hit_first = rows == slot[0:1, :]
    hit_second = rows == slot[1:2, :]
    chosen = jnp.where(hit_first | hit_second, 1.0, 0.0).astype(bf16)
    weight = jnp.sum(
        jnp.where(hit_first, weight_ref[0:1, :], 0.0)
        + jnp.where(hit_second, weight_ref[1:2, :], 0.0),
        axis=1,
        keepdims=True,
    )
    values = dot(chosen, cot_ref[...], plain) * weight
    width = values.shape[1]
    out_ref[:, :, 0:width] = values[0:main_rows].astype(bf16).reshape(group, main, width)
    tiles = pack_extras(values[main_rows:], scratch)
    out_ref[:, :, width:] = tiles.astype(bf16).reshape(group, main, 128)


def send(core, routes, weight, cotangent, experts):
    tokens, model = cotangent.shape
    half = model // 2
    return pl.pallas_call(
        send_kernel,
        grid_spec=pltpu.PrefetchScalarGridSpec(
            num_scalar_prefetch=1,
            grid=(experts // group,),
            in_specs=[
                whole((2, tokens)),
                whole((2, tokens)),
                pl.BlockSpec((tokens, half), lambda i, c: (0, c[0])),
            ],
            out_specs=[
                pl.BlockSpec((group, main, half + 128), lambda i, c: (i, 0, 0)),
                whole((8, tokens)),
            ],
            scratch_shapes=[pltpu.VMEM((8, tokens), jnp.int32), pltpu.VMEM((128, 128), f32)],
        ),
        out_shape=[
            jax.ShapeDtypeStruct((experts, main, half + 128), bf16),
            jax.ShapeDtypeStruct((8, tokens), jnp.int32),
        ],
        compiler_params=params(),
        name="send",
    )(core, routes, weight, cotangent)


pair = 2


def expert_pre_kernel(rows_ref, gate_ref, up_ref, packed_ref, silu_ref, slope_ref, active_ref):
    out_row = lax.broadcasted_iota(jnp.int32, (group_rows, group_rows), 0)
    column = lax.broadcasted_iota(jnp.int32, (group_rows, group_rows), 1)
    late = out_row - main_rows
    source = jnp.where(
        out_row < main_rows,
        (main + extra) * (out_row >> 4) + (out_row & 15),
        (main + extra) * (late >> 1) + main + (late & 1),
    )
    order = jnp.where(column == source, 1.0, 0.0).astype(bf16)
    for g in range(pair):
        lo = g * group_rows
        packed_ref[lo : lo + group_rows, :] = dot(
            order, rows_ref[lo : lo + group_rows, :], plain
        ).astype(bf16)
    packed = packed_ref[...]
    pre_gate = dot(packed, gate_ref[...], plain)
    pre_up = dot(packed, up_ref[...], plain)
    gate = jax.nn.sigmoid(pre_gate)
    silu = pre_gate * gate
    silu_ref[...] = silu
    slope_ref[...] = pre_up * gate * (1.0 + pre_gate * (1.0 - gate))
    active_ref[...] = (silu * pre_up).astype(bf16)


def expert_pre(rows, gate, up):
    count, model = rows.shape
    hidden = gate.shape[1]
    size = pair * group_rows
    by_row = lambda width: pl.BlockSpec((size, width), lambda i: (i, 0))
    return pl.pallas_call(
        expert_pre_kernel,
        grid=(count // size,),
        in_specs=[by_row(model), whole((model, hidden)), whole((model, hidden))],
        out_specs=[by_row(model), by_row(hidden), by_row(hidden), by_row(hidden)],
        out_shape=[
            jax.ShapeDtypeStruct((count, model), bf16),
            jax.ShapeDtypeStruct((count, hidden), f32),
            jax.ShapeDtypeStruct((count, hidden), f32),
            jax.ShapeDtypeStruct((count, hidden), bf16),
        ],
        compiler_params=params(),
        cost_estimate=pl.CostEstimate(
            flops=4 * count * model * hidden, transcendentals=0, bytes_accessed=20 << 20
        ),
        name="expert_pre",
    )(rows, gate, up)


def recur_pre_kernel(
    x_ref, y_ref, state_ref, edge_ref, taps_ref, a_ref, i_ref, rate_ref,
    mixed_ref, grad_y_ref, gelu_ref, ahead_ref, product_ref, keep_ref, input_ref, direct_ref,
    first_ref, scratch,
):
    tokens = x_ref.shape[0]
    x = x_ref[...].astype(f32)
    edge = edge_ref[...].astype(f32)
    scratch[5:8, :] = edge[0:3]
    scratch[8 : 8 + tokens, :] = x
    conv_x = taps_ref[0:1, :] * scratch[5 : 5 + tokens, :]
    for j in range(1, 4):
        conv_x = conv_x + taps_ref[j : j + 1, :] * scratch[5 + j : 5 + j + tokens, :]
    conv_b = conv_x.astype(bf16)
    keep = jax.nn.sigmoid(dot(conv_b, a_ref[0], plain))
    gate = jax.nn.sigmoid(dot(conv_b, i_ref[0], plain))
    rate = rate_ref[...]
    decay = jnp.exp(-rate_scale * keep * rate)
    norm = jnp.sqrt(1.0 - decay * decay + floor_square)
    state = state_ref[...].astype(f32)
    scratch[7:8, :] = edge[3:4]
    scratch[8 : 8 + tokens, :] = state
    state_prev = scratch[7 : 7 + tokens, :]
    log_part = decay * state_prev - conv_x * gate * decay * decay / norm
    keep_ref[...] = log_part * (-rate_scale * rate) * keep * (1.0 - keep)
    input_ref[...] = conv_x * norm * gate * (1.0 - gate)
    direct_ref[...] = gate * norm
    y = y_ref[...].astype(f32)
    below = 0.5 * (1.0 + lax.erf(y * inv_root_two))
    gelu = y * below
    gelu_ref[...] = gelu
    mixed_ref[...] = (state * gelu).astype(bf16)
    grad_y_ref[...] = state * (below + y * jnp.exp(-0.5 * y * y) * inv_root_tau)
    scratch[0:tokens, :] = decay
    scratch[tokens : tokens + 8, :] = jnp.ones((8, decay.shape[1]), f32)
    ahead_ref[0] = scratch[1 : 1 + tokens, :]
    length = tokens // segments
    product = None
    for j in reversed(range(length)):
        step = scratch[pl.ds(j + 1, segments, stride=length), :]
        product = step if product is None else step * product
        product_ref[0, pl.ds(j, segments, stride=length), :] = product
    total = decay[0:1]
    for s in range(segments):
        total = total * product[s : s + 1]
    first_ref[...] = jnp.concatenate([decay[0:1], total, jnp.zeros_like(decay[0:6])], axis=0)


def recur_pre(in_x, in_y, state, edge, taps, gate_a, gate_x, rate):
    tokens, channels = in_x.shape
    blocks, span = gate_a.shape[:2]
    col = lambda rows: pl.BlockSpec((rows, span), lambda i: (0, i))
    block = pl.BlockSpec((1, span, span), lambda i: (i, 0, 0))
    cube = pl.BlockSpec((1, tokens, span), lambda i: (i, 0, 0))
    big = jax.ShapeDtypeStruct((tokens, channels), f32)
    return pl.pallas_call(
        recur_pre_kernel,
        grid=(blocks,),
        in_specs=[col(tokens), col(tokens), col(tokens), col(4), col(4), block, block, col(1)],
        out_specs=[col(tokens)] * 3 + [cube] * 2 + [col(tokens)] * 3 + [col(8)],
        out_shape=[jax.ShapeDtypeStruct((tokens, channels), bf16)]
        + [big] * 2
        + [jax.ShapeDtypeStruct((blocks, tokens, span), f32)] * 2
        + [big] * 3
        + [jax.ShapeDtypeStruct((8, channels), f32)],
        scratch_shapes=[pltpu.VMEM((tokens + 16, span), f32)],
        compiler_params=params(),
        cost_estimate=pl.CostEstimate(
            flops=2000 * tokens * channels, transcendentals=0, bytes_accessed=8 << 20
        ),
        name="recur_pre",
    )(in_x, in_y, state, edge, taps, gate_a, gate_x, rate)


def unpack(block, scratch):
    width = block.shape[2] - 128
    parts = []
    for g in range(block.shape[0] // group):
        own = block[g * group : (g + 1) * group]
        parts.append(own[:, :, 0:width].reshape(main_rows, width))
        tiles = own[:, :, width:].reshape(128, 128).astype(f32)
        parts.append(unpack_extras(tiles, scratch).astype(bf16))
    return jnp.concatenate(parts, axis=0)


def pack_into(out_ref, values, scratch):
    width = values.shape[1]
    for g in range(out_ref.shape[0] // group):
        lo = g * group_rows
        out_ref[g * group : (g + 1) * group, :, 0:width] = (
            values[lo : lo + main_rows].astype(bf16).reshape(group, main, width)
        )
        tiles = pack_extras(values[lo + main_rows : lo + group_rows], scratch)
        out_ref[g * group : (g + 1) * group, :, width:] = tiles.astype(bf16).reshape(
            group, main, 128
        )


def near_kernel(core_ref, block_ref, down_ref, rows_ref, part_ref, scratch):
    rows = unpack(block_ref[...], scratch)
    rows_ref[...] = rows
    part_ref[...] = dot(rows, down_ref[...], inner)


def near(core, arrived, down):
    experts, _, wide = arrived.shape
    half = wide - 128
    hidden = down.shape[0]
    count = experts * (main + extra)
    size = pair * group_rows
    return pl.pallas_call(
        near_kernel,
        grid_spec=pltpu.PrefetchScalarGridSpec(
            num_scalar_prefetch=1,
            grid=(count // size,),
            in_specs=[
                pl.BlockSpec((pair * group, main, wide), lambda i, c: (i, 0, 0)),
                pl.BlockSpec((hidden, half), lambda i, c: (0, c[0])),
            ],
            out_specs=[
                pl.BlockSpec((size, half), lambda i, c: (i, 0)),
                pl.BlockSpec((size, hidden), lambda i, c: (i, 0)),
            ],
            scratch_shapes=[pltpu.VMEM((128, 128), f32)],
        ),
        out_shape=[
            jax.ShapeDtypeStruct((count, half), bf16),
            jax.ShapeDtypeStruct((count, hidden), f32),
        ],
        compiler_params=params(),
        cost_estimate=pl.CostEstimate(
            flops=2 * count * half * hidden, transcendentals=0, bytes_accessed=9 << 20
        ),
        name="near",
    )(core, arrived, down)


def far_kernel(
    core_ref, block_ref, down_ref, part_ref, silu_ref, slope_ref, gate_ref, up_ref,
    rows_ref, gate_adj_ref, up_adj_ref, back_ref, scratch,
):
    rows = unpack(block_ref[...], scratch)
    rows_ref[...] = rows
    grad = part_ref[...] + dot(rows, down_ref[...], inner)
    gate_adj = (grad * slope_ref[...]).astype(bf16)
    up_adj = (grad * silu_ref[...]).astype(bf16)
    gate_adj_ref[...] = gate_adj
    up_adj_ref[...] = up_adj
    back = dot(gate_adj, gate_ref[...], inner) + dot(up_adj, up_ref[...], inner)
    pack_into(back_ref, back, scratch)


def far(core, arrived, down, part, silu, slope, gate, up):
    experts, _, wide = arrived.shape
    half = wide - 128
    hidden = down.shape[0]
    count = experts * (main + extra)
    size = pair * group_rows
    by_row = lambda width: pl.BlockSpec((size, width), lambda i, c: (i, 0))
    block = pl.BlockSpec((pair * group, main, wide), lambda i, c: (i, 0, 0))
    weight = pl.BlockSpec((half, hidden), lambda i, c: (1 - c[0], 0))
    return pl.pallas_call(
        far_kernel,
        grid_spec=pltpu.PrefetchScalarGridSpec(
            num_scalar_prefetch=1,
            grid=(count // size,),
            in_specs=[
                block,
                pl.BlockSpec((hidden, half), lambda i, c: (0, 1 - c[0])),
                by_row(hidden),
                by_row(hidden),
                by_row(hidden),
                weight,
                weight,
            ],
            out_specs=[by_row(half), by_row(hidden), by_row(hidden), block],
            scratch_shapes=[pltpu.VMEM((128, 128), f32)],
        ),
        out_shape=[
            jax.ShapeDtypeStruct((count, half), bf16),
            jax.ShapeDtypeStruct((count, hidden), bf16),
            jax.ShapeDtypeStruct((count, hidden), bf16),
            jax.ShapeDtypeStruct(arrived.shape, bf16),
        ],
        compiler_params=params(),
        cost_estimate=pl.CostEstimate(
            flops=6 * count * half * hidden, transcendentals=0, bytes_accessed=16 << 20
        ),
        name="far",
    )(core, arrived, down, part, silu, slope, gate, up)


def back_kernel(core_ref, gate_adj_ref, up_adj_ref, gate_ref, up_ref, back_ref, scratch):
    back = dot(gate_adj_ref[...], gate_ref[...], inner) + dot(up_adj_ref[...], up_ref[...], inner)
    pack_into(back_ref, back, scratch)


def back_own(core, gate_adj, up_adj, gate, up, shape):
    experts, _, wide = shape
    half = wide - 128
    count, hidden = gate_adj.shape
    size = pair * group_rows
    by_row = lambda width: pl.BlockSpec((size, width), lambda i, c: (i, 0))
    weight = pl.BlockSpec((half, hidden), lambda i, c: (c[0], 0))
    return pl.pallas_call(
        back_kernel,
        grid_spec=pltpu.PrefetchScalarGridSpec(
            num_scalar_prefetch=1,
            grid=(count // size,),
            in_specs=[by_row(hidden), by_row(hidden), weight, weight],
            out_specs=pl.BlockSpec((pair * group, main, wide), lambda i, c: (i, 0, 0)),
            scratch_shapes=[pltpu.VMEM((128, 128), f32)],
        ),
        out_shape=jax.ShapeDtypeStruct(shape, bf16),
        compiler_params=params(),
        cost_estimate=pl.CostEstimate(
            flops=4 * count * half * hidden, transcendentals=0, bytes_accessed=7 << 20
        ),
        name="back_own",
    )(core, gate_adj, up_adj, gate, up)


def grad_in_kernel(packed_ref, gate_adj_ref, up_adj_ref, gate_ref, up_ref):
    packed = packed_ref[...]
    gate_ref[...] = dot(packed, gate_adj_ref[...], outer).astype(bf16)
    up_ref[...] = dot(packed, up_adj_ref[...], outer).astype(bf16)


def grad_in(packed, gate_adj, up_adj):
    count, model = packed.shape
    hidden = gate_adj.shape[1]
    size = 512
    out = pl.BlockSpec((size, hidden), lambda i: (i, 0))
    return pl.pallas_call(
        grad_in_kernel,
        grid=(model // size,),
        in_specs=[
            pl.BlockSpec((count, size), lambda i: (0, i)),
            whole((count, hidden)),
            whole((count, hidden)),
        ],
        out_specs=[out, out],
        out_shape=[jax.ShapeDtypeStruct((model, hidden), bf16)] * 2,
        compiler_params=params(),
        cost_estimate=pl.CostEstimate(
            flops=4 * count * model * hidden, transcendentals=0, bytes_accessed=11 << 20
        ),
        name="grad_in",
    )(packed, gate_adj, up_adj)


def grad_down_kernel(core_ref, active_ref, near_ref, far_ref, out_ref):
    active = active_ref[...]

    @pl.when(pl.program_id(0) == 0)
    def _():
        out_ref[...] = dot(active, near_ref[...], outer).astype(bf16)

    @pl.when(pl.program_id(0) == 1)
    def _():
        out_ref[...] = dot(active, far_ref[...], outer).astype(bf16)


def grad_down_of(core, active, near_rows, far_rows):
    count, hidden = active.shape
    half = near_rows.shape[1]
    return pl.pallas_call(
        grad_down_kernel,
        grid_spec=pltpu.PrefetchScalarGridSpec(
            num_scalar_prefetch=1,
            grid=(2,),
            in_specs=[whole((count, hidden)), whole((count, half)), whole((count, half))],
            out_specs=pl.BlockSpec((hidden, half), lambda i, c: (0, i + c[0] - 2 * i * c[0])),
        ),
        out_shape=jax.ShapeDtypeStruct((hidden, 2 * half), bf16),
        compiler_params=params(),
        cost_estimate=pl.CostEstimate(
            flops=4 * count * half * hidden, transcendentals=0, bytes_accessed=9 << 20
        ),
        name="grad_down",
    )(core, active, near_rows, far_rows)


def combine_kernel(core_ref, block_ref, target_ref, cot_ref, out_ref, total, scratch):
    step = pl.program_id(0)
    tokens = cot_ref.shape[0]
    rows = unpack(block_ref[...], scratch)
    size = rows.shape[0]
    place = lax.broadcasted_iota(jnp.int32, (tokens, size), 1) + step * size
    chosen = jnp.where(
        (place == target_ref[:, 0:1]) | (place == target_ref[:, 1:2]), 1.0, 0.0
    ).astype(bf16)
    found = dot(chosen, rows, plain)

    @pl.when(step == 0)
    def _():
        total[...] = found

    @pl.when(step > 0)
    def _():
        total[...] = total[...] + found

    @pl.when(step == pl.num_programs(0) - 1)
    def _():
        out_ref[...] = (cot_ref[...].astype(f32) + total[...]).astype(bf16)


def combine(core, returned, target, cotangent):
    experts, _, wide = returned.shape
    half = wide - 128
    tokens = cotangent.shape[0]
    return pl.pallas_call(
        combine_kernel,
        grid_spec=pltpu.PrefetchScalarGridSpec(
            num_scalar_prefetch=1,
            grid=(experts // (pair * group),),
            in_specs=[
                pl.BlockSpec((pair * group, main, wide), lambda i, c: (i, 0, 0)),
                whole((tokens, 8)),
                pl.BlockSpec((tokens, half), lambda i, c: (0, c[0])),
            ],
            out_specs=whole((tokens, half)),
            scratch_shapes=[pltpu.VMEM((tokens, half), f32), pltpu.VMEM((128, 128), f32)],
        ),
        out_shape=jax.ShapeDtypeStruct((tokens, half), bf16),
        compiler_params=params(),
        name="combine",
    )(core, returned, target, cotangent)


def scan_kernel(
    core_ref, own_ref, peer_ref, weight_ref, slope_ref, gelu_ref, ahead_ref, product_ref, first_ref,
    grad_y_ref, local_ref, total_ref, scratch,
):
    tokens, half = own_ref.shape
    core = core_ref[0]
    near_weight = weight_ref[pl.ds(pl.multiple_of(core * half, half), half), :]
    far_weight = weight_ref[pl.ds(pl.multiple_of((1 - core) * half, half), half), :]
    grad = dot(own_ref[...], near_weight, plain) + dot(peer_ref[...], far_weight, plain)
    grad_y_ref[...] = grad * slope_ref[...]
    state_grad = grad * gelu_ref[...]
    length = tokens // segments
    for b in range(scratch.shape[0]):
        at = slice(128 * b, 128 * (b + 1))
        scratch[b] = state_grad[:, at]
    for b in range(scratch.shape[0]):
        at = slice(128 * b, 128 * (b + 1))
        value = None
        for j in reversed(range(length)):
            here = scratch[b, pl.ds(j, segments, stride=length), :]
            if value is None:
                value = here
            else:
                value = here + ahead_ref[b, pl.ds(j, segments, stride=length), :] * value
            local_ref[b, pl.ds(j, segments, stride=length), :] = value
        product = product_ref[b, pl.ds(0, segments, stride=length), :]
        carry = value[segments - 1 : segments]
        for s in reversed(range(segments - 1)):
            carry = value[s : s + 1] + product[s : s + 1] * carry
        total_ref[:, at] = first_ref[0:1, at] * carry


def scan(core, own, peer, weight, slope, gelu, ahead, product, first):
    tokens, half = own.shape
    channels = weight.shape[1]
    return pl.pallas_call(
        scan_kernel,
        grid_spec=pltpu.PrefetchScalarGridSpec(
            num_scalar_prefetch=1,
            grid=(1,),
            in_specs=[
                whole((tokens, half)),
                whole((tokens, half)),
                whole(weight.shape),
                whole((tokens, channels)),
                whole((tokens, channels)),
                whole(ahead.shape),
                whole(ahead.shape),
                whole((8, channels)),
            ],
            out_specs=[whole((tokens, channels)), whole(ahead.shape), whole((1, channels))],
            scratch_shapes=[pltpu.VMEM(ahead.shape, f32)],
        ),
        out_shape=[
            jax.ShapeDtypeStruct((tokens, channels), f32),
            jax.ShapeDtypeStruct(ahead.shape, f32),
            jax.ShapeDtypeStruct((1, channels), f32),
        ],
        compiler_params=params(),
        name="scan",
    )(core, own, peer, weight, slope, gelu, ahead, product, first)


def project_kernel(core_ref, own_ref, peer_ref, mixed_ref, out_ref):
    half = own_ref.shape[1]
    core = core_ref[0]
    mixed = mixed_ref[...]
    near_rows = dot(own_ref[...], mixed, outer).astype(bf16)
    far_rows = dot(peer_ref[...], mixed, outer).astype(bf16)
    out_ref[pl.ds(pl.multiple_of(core * half, half), half), :] = near_rows
    out_ref[pl.ds(pl.multiple_of((1 - core) * half, half), half), :] = far_rows


def project(core, own, peer, mixed):
    tokens, half = own.shape
    channels = mixed.shape[1]
    return pl.pallas_call(
        project_kernel,
        grid_spec=pltpu.PrefetchScalarGridSpec(
            num_scalar_prefetch=1,
            grid=(1,),
            in_specs=[whole((tokens, half)), whole((tokens, half)), whole((tokens, channels))],
            out_specs=whole((2 * half, channels)),
        ),
        out_shape=jax.ShapeDtypeStruct((2 * half, channels), bf16),
        compiler_params=params(),
        name="project",
    )(core, own, peer, mixed)


def adjoint_kernel(
    carry_ref, local_ref, product_ref, keep_ref, input_ref, direct_ref, a_ref, i_ref,
    out_ref, scratch,
):
    tokens = local_ref.shape[1]
    length = tokens // segments
    carry = carry_ref[...]
    for s in reversed(range(segments)):
        lo = s * length
        piece = local_ref[0, lo : lo + length, :] + product_ref[0, lo : lo + length, :] * carry
        scratch[lo : lo + length, :] = piece
        carry = piece[0:1]
    adjoint = scratch[...]
    keep = (adjoint * keep_ref[...]).astype(bf16)
    gate = (adjoint * input_ref[...]).astype(bf16)
    out_ref[...] = adjoint * direct_ref[...] + dot(keep, a_ref[0], inner) + dot(gate, i_ref[0], inner)


def conv_grad_of(carry, local, product, keep, gate, direct, gate_a, gate_x):
    tokens = local.shape[1]
    blocks, span = gate_a.shape[:2]
    channels = blocks * span
    cube = pl.BlockSpec((1, tokens, span), lambda i: (i, 0, 0))
    col = lambda rows: pl.BlockSpec((rows, span), lambda i: (0, i))
    block = pl.BlockSpec((1, span, span), lambda i: (i, 0, 0))
    return pl.pallas_call(
        adjoint_kernel,
        grid=(blocks,),
        in_specs=[col(1), cube, cube] + [col(tokens)] * 3 + [block, block],
        out_specs=col(tokens),
        out_shape=jax.ShapeDtypeStruct((tokens, channels), f32),
        scratch_shapes=[pltpu.VMEM((tokens, span), f32)],
        compiler_params=params(),
        name="adjoint",
    )(carry, local, product, keep, gate, direct, gate_a, gate_x)


def grad_x_kernel(grad_ref, later_ref, taps_ref, out_ref, scratch):
    tokens = grad_ref.shape[0]
    scratch[0:tokens, :] = grad_ref[...]
    scratch[tokens : tokens + 3, :] = later_ref[...]
    total = taps_ref[0:1, :] * scratch[3 : 3 + tokens, :]
    for j in range(1, 4):
        total = total + taps_ref[j : j + 1, :] * scratch[3 - j : 3 - j + tokens, :]
    out_ref[...] = total


def grad_x_of(grad, later, taps):
    tokens, channels = grad.shape
    col = lambda rows: pl.BlockSpec((rows, 128), lambda i: (0, i))
    return pl.pallas_call(
        grad_x_kernel,
        grid=(channels // 128,),
        in_specs=[col(tokens), col(3), col(4)],
        out_specs=col(tokens),
        out_shape=jax.ShapeDtypeStruct((tokens, channels), f32),
        scratch_shapes=[pltpu.VMEM((tokens + 8, 128), f32)],
        compiler_params=params(),
        name="grad_x",
    )(grad, later, taps)


def exchange(value, axis):
    return lax.all_to_all(value, axis, split_axis=0, concat_axis=0, tiled=True)


def swapped(value):
    return lax.ppermute(value, "tp", [(0, 1), (1, 0)])


def shifted(value, axis, by):
    devices = lax.axis_size(axis)
    pairs = [(i, i + by) for i in range(devices) if 0 <= i + by < devices]
    return lax.ppermute(value, axis, pairs)


def sent_to_all(value, axis):
    copies = jnp.broadcast_to(value[None], (lax.axis_size(axis), *value.shape))
    return exchange(copies, axis)


def carry_weights(total_decay):
    devices, place = lax.axis_size("sp"), lax.axis_index("sp")
    number = jnp.arange(devices)[:, None, None]
    factors = jnp.where(number > place, total_decay, 1.0)
    upto = lax.associative_scan(jnp.multiply, factors, axis=0)
    between = jnp.concatenate([jnp.ones_like(upto[:1]), upto[:-1]], axis=0)
    return jnp.where(number > place, between, 0.0)


def body(
    cotangent,
    routes,
    route_weight,
    expert_rows,
    gate_w,
    up_w,
    down_w,
    in_x,
    in_y,
    state,
    conv_taps,
    gate_a,
    gate_x,
    decay_rate,
    out_weight,
):
    tokens = cotangent.shape[0]
    experts = lax.axis_size("sp")
    core = lax.axis_index("tp").astype(jnp.int32).reshape(1)
    taps = conv_taps.shape[0]
    channels = in_x.shape[1]

    outgoing, target = send(core, routes.T, route_weight.T, cotangent, experts)
    arrived = exchange(outgoing, "sp")
    target = target.T

    edge = shifted(
        jnp.concatenate([in_x[tokens - taps + 1 :], state[tokens - 1 :]], axis=0), "sp", 1
    )
    packed, silu, slope, active = expert_pre(expert_rows[0], gate_w[0], up_w[0])
    mixed, y_slope, gelu, ahead, product, keep_part, input_part, direct, first = recur_pre(
        in_x, in_y, state, edge, conv_taps, gate_a, gate_x, decay_rate[None]
    )
    decays = sent_to_all(first[1:2].reshape(channels // 128, 128), "sp")
    weights = carry_weights(decays)

    arrived_far = swapped(arrived)
    near_rows, part = near(core, arrived, down_w[0])
    far_rows, gate_adj, up_adj, back_far = far(
        core, arrived_far, down_w[0], part, silu, slope, gate_w[0], up_w[0]
    )
    back_in = swapped(back_far)
    own = back_own(core, gate_adj, up_adj, gate_w[0], up_w[0], arrived.shape)
    returning = (own.astype(f32) + back_in.astype(f32)).astype(bf16)
    returned = exchange(returning, "sp")

    grad_gate, grad_up = grad_in(packed, gate_adj, up_adj)
    grad_down = grad_down_of(core, active, near_rows, far_rows)

    stream_own = combine(core, returned, target, cotangent)
    stream_peer = swapped(stream_own)
    grad_y, local, total = scan(
        core, stream_own, stream_peer, out_weight, y_slope, gelu, ahead, product, first
    )
    totals = sent_to_all(total.reshape(channels // 128, 128), "sp")
    partial = project(core, stream_own, stream_peer, mixed)
    shares = exchange(partial.reshape(experts, -1, channels), "sp")

    carry = jnp.sum(totals * weights, axis=0).reshape(1, channels)
    conv_grad = conv_grad_of(
        carry, local, product, keep_part, input_part, direct, gate_a, gate_x
    )
    later = shifted(conv_grad[: taps - 1], "sp", -1)
    grad_x = grad_x_of(conv_grad, later, conv_taps)
    grad_proj = jnp.sum(shares.astype(f32), axis=0)
    return (grad_gate[None], grad_up[None], grad_down[None], grad_proj, grad_x, grad_y)


def solution(mesh):
    in_specs = (
        P("sp", None),
        P("sp", None),
        P("sp", None),
        P("sp", None, None),
        P("sp", None, "tp"),
        P("sp", None, "tp"),
        P("sp", "tp", None),
        P("sp", "tp"),
        P("sp", "tp"),
        P("sp", "tp"),
        P(None, "tp"),
        P("tp", None, None),
        P("tp", None, None),
        P("tp"),
        P(None, "tp"),
    )
    out_specs = (
        P("sp", None, "tp"),
        P("sp", None, "tp"),
        P("sp", "tp", None),
        P("sp", "tp"),
        P("sp", "tp"),
        P("sp", "tp"),
    )
    return jax.shard_map(body, mesh=mesh, in_specs=in_specs, out_specs=out_specs, check_vma=False)
```

```python
import jax
import jax.numpy as jnp
from jax import lax
from jax.experimental import pallas as pl
from jax.experimental.pallas import tpu as pltpu
from jax.sharding import PartitionSpec as P

rate_scale = 8.0
floor_square = 0.01
inv_root_two = 0.7071067811865476
inv_root_tau = 0.3989422804014327

f32 = jnp.float32
bf16 = jnp.bfloat16
inner = (((1,), (1,)), ((), ()))
outer = (((0,), (0,)), ((), ()))
plain = (((1,), (0,)), ((), ()))

group = 8
main = 16
extra = 2
main_rows = group * main
group_rows = group * (main + extra)
segments = 8


def dot(a, b, dims):
    return lax.dot_general(a, b, dims, preferred_element_type=f32)


def params(n=1, mb=58):
    return pltpu.CompilerParams(dimension_semantics=("arbitrary",) * n, vmem_limit_bytes=mb << 20)


def whole(shape):
    return pl.BlockSpec(shape, lambda *_: (0,) * len(shape))


def pack_extras(rows, scratch):
    for j in range(8):
        scratch[pl.ds(j, group * extra, stride=8), :] = rows[:, 128 * j : 128 * (j + 1)]
    return scratch[...]


def unpack_extras(tiles, scratch):
    scratch[...] = tiles
    return jnp.concatenate(
        [scratch[pl.ds(j, group * extra, stride=8), :] for j in range(8)], axis=1
    )


def send_kernel(core_ref, routes_ref, weight_ref, cot_ref, out_ref, target_ref, slot, scratch):
    step = pl.program_id(0)
    tokens = cot_ref.shape[0]
    experts = pl.num_programs(0) * group

    @pl.when(step == 0)
    def _():
        first = routes_ref[0:1, :]
        second = routes_ref[1:2, :]
        expert = lax.broadcasted_iota(jnp.int32, (experts, tokens), 0)
        hit_first = (expert == first).astype(f32)
        hit_second = (expert == second).astype(f32)
        earlier = (
            lax.broadcasted_iota(jnp.int32, (tokens, tokens), 0)
            < lax.broadcasted_iota(jnp.int32, (tokens, tokens), 1)
        ).astype(f32)
        before = dot((hit_first + hit_second).astype(bf16), earlier.astype(bf16), plain)
        place_first = jnp.sum(before * hit_first, axis=0, keepdims=True).astype(jnp.int32)
        place_second = jnp.sum(before * hit_second, axis=0, keepdims=True).astype(jnp.int32)
        place_second = place_second + (first == second).astype(jnp.int32)
        for k, (name, place) in enumerate(((first, place_first), (second, place_second))):
            base = group_rows * (name >> 3)
            inside = name & 7
            slot[k : k + 1, :] = base + jnp.where(
                place < main, main * inside + place, main_rows + extra * inside + place - main
            )
        target_ref[...] = jnp.concatenate(
            [slot[0:2, :], jnp.zeros((6, tokens), jnp.int32)], axis=0
        )

    rows = lax.broadcasted_iota(jnp.int32, (group_rows, tokens), 0) + step * group_rows
    hit_first = rows == slot[0:1, :]
    hit_second = rows == slot[1:2, :]
    chosen = jnp.where(hit_first | hit_second, 1.0, 0.0).astype(bf16)
    weight = jnp.sum(
        jnp.where(hit_first, weight_ref[0:1, :], 0.0)
        + jnp.where(hit_second, weight_ref[1:2, :], 0.0),
        axis=1,
        keepdims=True,
    )
    values = dot(chosen, cot_ref[...], plain) * weight
    width = values.shape[1]
    out_ref[:, :, 0:width] = values[0:main_rows].astype(bf16).reshape(group, main, width)
    tiles = pack_extras(values[main_rows:], scratch)
    out_ref[:, :, width:] = tiles.astype(bf16).reshape(group, main, 128)


def send(core, routes, weight, cotangent, experts):
    tokens, model = cotangent.shape
    half = model // 2
    return pl.pallas_call(
        send_kernel,
        grid_spec=pltpu.PrefetchScalarGridSpec(
            num_scalar_prefetch=1,
            grid=(experts // group,),
            in_specs=[
                whole((2, tokens)),
                whole((2, tokens)),
                pl.BlockSpec((tokens, half), lambda i, c: (0, c[0])),
            ],
            out_specs=[
                pl.BlockSpec((group, main, half + 128), lambda i, c: (i, 0, 0)),
                whole((8, tokens)),
            ],
            scratch_shapes=[pltpu.VMEM((8, tokens), jnp.int32), pltpu.VMEM((128, 128), f32)],
        ),
        out_shape=[
            jax.ShapeDtypeStruct((experts, main, half + 128), bf16),
            jax.ShapeDtypeStruct((8, tokens), jnp.int32),
        ],
        compiler_params=params(),
        name="send",
    )(core, routes, weight, cotangent)


pair = 2


def expert_pre_kernel(rows_ref, gate_ref, up_ref, packed_ref, silu_ref, slope_ref, active_ref):
    out_row = lax.broadcasted_iota(jnp.int32, (group_rows, group_rows), 0)
    column = lax.broadcasted_iota(jnp.int32, (group_rows, group_rows), 1)
    late = out_row - main_rows
    source = jnp.where(
        out_row < main_rows,
        (main + extra) * (out_row >> 4) + (out_row & 15),
        (main + extra) * (late >> 1) + main + (late & 1),
    )
    order = jnp.where(column == source, 1.0, 0.0).astype(bf16)
    for g in range(pair):
        lo = g * group_rows
        packed_ref[lo : lo + group_rows, :] = dot(
            order, rows_ref[lo : lo + group_rows, :], plain
        ).astype(bf16)
    packed = packed_ref[...]
    pre_gate = dot(packed, gate_ref[...], plain)
    pre_up = dot(packed, up_ref[...], plain)
    gate = jax.nn.sigmoid(pre_gate)
    silu = pre_gate * gate
    silu_ref[...] = silu
    slope_ref[...] = pre_up * gate * (1.0 + pre_gate * (1.0 - gate))
    active_ref[...] = (silu * pre_up).astype(bf16)


def expert_pre(rows, gate, up):
    count, model = rows.shape
    hidden = gate.shape[1]
    size = pair * group_rows
    by_row = lambda width: pl.BlockSpec((size, width), lambda i: (i, 0))
    return pl.pallas_call(
        expert_pre_kernel,
        grid=(count // size,),
        in_specs=[by_row(model), whole((model, hidden)), whole((model, hidden))],
        out_specs=[by_row(model), by_row(hidden), by_row(hidden), by_row(hidden)],
        out_shape=[
            jax.ShapeDtypeStruct((count, model), bf16),
            jax.ShapeDtypeStruct((count, hidden), f32),
            jax.ShapeDtypeStruct((count, hidden), f32),
            jax.ShapeDtypeStruct((count, hidden), bf16),
        ],
        compiler_params=params(),
        cost_estimate=pl.CostEstimate(
            flops=4 * count * model * hidden, transcendentals=0, bytes_accessed=20 << 20
        ),
        name="expert_pre",
    )(rows, gate, up)


def recur_pre_kernel(
    x_ref, y_ref, state_ref, edge_ref, taps_ref, a_ref, i_ref, rate_ref,
    mixed_ref, grad_y_ref, gelu_ref, ahead_ref, product_ref, keep_ref, input_ref, direct_ref,
    first_ref, scratch,
):
    tokens = x_ref.shape[0]
    x = x_ref[...].astype(f32)
    edge = edge_ref[...].astype(f32)
    scratch[5:8, :] = edge[0:3]
    scratch[8 : 8 + tokens, :] = x
    conv_x = taps_ref[0:1, :] * scratch[5 : 5 + tokens, :]
    for j in range(1, 4):
        conv_x = conv_x + taps_ref[j : j + 1, :] * scratch[5 + j : 5 + j + tokens, :]
    conv_b = conv_x.astype(bf16)
    keep = jax.nn.sigmoid(dot(conv_b, a_ref[0], plain))
    gate = jax.nn.sigmoid(dot(conv_b, i_ref[0], plain))
    rate = rate_ref[...]
    decay = jnp.exp(-rate_scale * keep * rate)
    norm = jnp.sqrt(1.0 - decay * decay + floor_square)
    state = state_ref[...].astype(f32)
    scratch[7:8, :] = edge[3:4]
    scratch[8 : 8 + tokens, :] = state
    state_prev = scratch[7 : 7 + tokens, :]
    log_part = decay * state_prev - conv_x * gate * decay * decay / norm
    keep_ref[...] = log_part * (-rate_scale * rate) * keep * (1.0 - keep)
    input_ref[...] = conv_x * norm * gate * (1.0 - gate)
    direct_ref[...] = gate * norm
    y = y_ref[...].astype(f32)
    below = 0.5 * (1.0 + lax.erf(y * inv_root_two))
    gelu = y * below
    gelu_ref[...] = gelu
    mixed_ref[...] = (state * gelu).astype(bf16)
    grad_y_ref[...] = state * (below + y * jnp.exp(-0.5 * y * y) * inv_root_tau)
    scratch[0:tokens, :] = decay
    scratch[tokens : tokens + 8, :] = jnp.ones((8, decay.shape[1]), f32)
    ahead_ref[0] = scratch[1 : 1 + tokens, :]
    length = tokens // segments
    product = None
    for j in reversed(range(length)):
        step = scratch[pl.ds(j + 1, segments, stride=length), :]
        product = step if product is None else step * product
        product_ref[0, pl.ds(j, segments, stride=length), :] = product
    rest = product[1:2]
    for s in range(2, segments):
        rest = rest * product[s : s + 1]
    total = decay[0:1] * product[0:1] * rest
    first_ref[...] = jnp.concatenate(
        [
            decay[0:1],
            total,
            jnp.zeros_like(total),
            product_ref[0, 0:3, :] * rest,
            keep_ref[0:3, :],
            input_ref[0:3, :],
            direct_ref[0:3, :],
            jnp.zeros_like(total),
        ],
        axis=0,
    )


def recur_pre(in_x, in_y, state, edge, taps, gate_a, gate_x, rate):
    tokens, channels = in_x.shape
    blocks, span = gate_a.shape[:2]
    col = lambda rows: pl.BlockSpec((rows, span), lambda i: (0, i))
    block = pl.BlockSpec((1, span, span), lambda i: (i, 0, 0))
    cube = pl.BlockSpec((1, tokens, span), lambda i: (i, 0, 0))
    big = jax.ShapeDtypeStruct((tokens, channels), f32)
    return pl.pallas_call(
        recur_pre_kernel,
        grid=(blocks,),
        in_specs=[col(tokens), col(tokens), col(tokens), col(4), col(4), block, block, col(1)],
        out_specs=[col(tokens)] * 3 + [cube] * 2 + [col(tokens)] * 3 + [col(16)],
        out_shape=[jax.ShapeDtypeStruct((tokens, channels), bf16)]
        + [big] * 2
        + [jax.ShapeDtypeStruct((blocks, tokens, span), f32)] * 2
        + [big] * 3
        + [jax.ShapeDtypeStruct((16, channels), f32)],
        scratch_shapes=[pltpu.VMEM((tokens + 16, span), f32)],
        compiler_params=params(),
        cost_estimate=pl.CostEstimate(
            flops=2000 * tokens * channels, transcendentals=0, bytes_accessed=8 << 20
        ),
        name="recur_pre",
    )(in_x, in_y, state, edge, taps, gate_a, gate_x, rate)


def unpack(block, scratch):
    width = block.shape[2] - 128
    parts = []
    for g in range(block.shape[0] // group):
        own = block[g * group : (g + 1) * group]
        parts.append(own[:, :, 0:width].reshape(main_rows, width))
        tiles = own[:, :, width:].reshape(128, 128).astype(f32)
        parts.append(unpack_extras(tiles, scratch).astype(bf16))
    return jnp.concatenate(parts, axis=0)


def pack_into(out_ref, values, scratch):
    width = values.shape[1]
    for g in range(out_ref.shape[0] // group):
        lo = g * group_rows
        out_ref[g * group : (g + 1) * group, :, 0:width] = (
            values[lo : lo + main_rows].astype(bf16).reshape(group, main, width)
        )
        tiles = pack_extras(values[lo + main_rows : lo + group_rows], scratch)
        out_ref[g * group : (g + 1) * group, :, width:] = tiles.astype(bf16).reshape(
            group, main, 128
        )


def near_kernel(core_ref, block_ref, down_ref, rows_ref, part_ref, scratch):
    rows = unpack(block_ref[...], scratch)
    rows_ref[...] = rows
    part_ref[...] = dot(rows, down_ref[...], inner)


def near(core, arrived, down):
    experts, _, wide = arrived.shape
    half = wide - 128
    hidden = down.shape[0]
    count = experts * (main + extra)
    size = pair * group_rows
    return pl.pallas_call(
        near_kernel,
        grid_spec=pltpu.PrefetchScalarGridSpec(
            num_scalar_prefetch=1,
            grid=(count // size,),
            in_specs=[
                pl.BlockSpec((pair * group, main, wide), lambda i, c: (i, 0, 0)),
                pl.BlockSpec((hidden, half), lambda i, c: (0, c[0])),
            ],
            out_specs=[
                pl.BlockSpec((size, half), lambda i, c: (i, 0)),
                pl.BlockSpec((size, hidden), lambda i, c: (i, 0)),
            ],
            scratch_shapes=[pltpu.VMEM((128, 128), f32)],
        ),
        out_shape=[
            jax.ShapeDtypeStruct((count, half), bf16),
            jax.ShapeDtypeStruct((count, hidden), f32),
        ],
        compiler_params=params(),
        cost_estimate=pl.CostEstimate(
            flops=2 * count * half * hidden, transcendentals=0, bytes_accessed=9 << 20
        ),
        name="near",
    )(core, arrived, down)


def far_kernel(
    core_ref, block_ref, down_ref, part_ref, silu_ref, slope_ref, gate_ref, up_ref,
    rows_ref, gate_adj_ref, up_adj_ref, back_ref, scratch,
):
    rows = unpack(block_ref[...], scratch)
    rows_ref[...] = rows
    grad = part_ref[...] + dot(rows, down_ref[...], inner)
    gate_adj = (grad * slope_ref[...]).astype(bf16)
    up_adj = (grad * silu_ref[...]).astype(bf16)
    gate_adj_ref[...] = gate_adj
    up_adj_ref[...] = up_adj
    back = dot(gate_adj, gate_ref[...], inner) + dot(up_adj, up_ref[...], inner)
    pack_into(back_ref, back, scratch)


def far(core, arrived, down, part, silu, slope, gate, up):
    experts, _, wide = arrived.shape
    half = wide - 128
    hidden = down.shape[0]
    count = experts * (main + extra)
    size = pair * group_rows
    by_row = lambda width: pl.BlockSpec((size, width), lambda i, c: (i, 0))
    block = pl.BlockSpec((pair * group, main, wide), lambda i, c: (i, 0, 0))
    weight = pl.BlockSpec((half, hidden), lambda i, c: (1 - c[0], 0))
    return pl.pallas_call(
        far_kernel,
        grid_spec=pltpu.PrefetchScalarGridSpec(
            num_scalar_prefetch=1,
            grid=(count // size,),
            in_specs=[
                block,
                pl.BlockSpec((hidden, half), lambda i, c: (0, 1 - c[0])),
                by_row(hidden),
                by_row(hidden),
                by_row(hidden),
                weight,
                weight,
            ],
            out_specs=[by_row(half), by_row(hidden), by_row(hidden), block],
            scratch_shapes=[pltpu.VMEM((128, 128), f32)],
        ),
        out_shape=[
            jax.ShapeDtypeStruct((count, half), bf16),
            jax.ShapeDtypeStruct((count, hidden), bf16),
            jax.ShapeDtypeStruct((count, hidden), bf16),
            jax.ShapeDtypeStruct(arrived.shape, bf16),
        ],
        compiler_params=params(),
        cost_estimate=pl.CostEstimate(
            flops=6 * count * half * hidden, transcendentals=0, bytes_accessed=16 << 20
        ),
        name="far",
    )(core, arrived, down, part, silu, slope, gate, up)


def back_kernel(core_ref, gate_adj_ref, up_adj_ref, gate_ref, up_ref, back_ref, scratch):
    back = dot(gate_adj_ref[...], gate_ref[...], inner) + dot(up_adj_ref[...], up_ref[...], inner)
    pack_into(back_ref, back, scratch)


def back_own(core, gate_adj, up_adj, gate, up, shape):
    _, _, wide = shape
    half = wide - 128
    count, hidden = gate_adj.shape
    size = pair * group_rows
    by_row = lambda width: pl.BlockSpec((size, width), lambda i, c: (i, 0))
    weight = pl.BlockSpec((half, hidden), lambda i, c: (c[0], 0))
    return pl.pallas_call(
        back_kernel,
        grid_spec=pltpu.PrefetchScalarGridSpec(
            num_scalar_prefetch=1,
            grid=(count // size,),
            in_specs=[by_row(hidden), by_row(hidden), weight, weight],
            out_specs=pl.BlockSpec((pair * group, main, wide), lambda i, c: (i, 0, 0)),
            scratch_shapes=[pltpu.VMEM((128, 128), f32)],
        ),
        out_shape=jax.ShapeDtypeStruct(shape, bf16),
        compiler_params=params(),
        cost_estimate=pl.CostEstimate(
            flops=4 * count * half * hidden, transcendentals=0, bytes_accessed=7 << 20
        ),
        name="back_own",
    )(core, gate_adj, up_adj, gate, up)


def grad_in_kernel(packed_ref, gate_adj_ref, up_adj_ref, gate_ref, up_ref):
    packed = packed_ref[...]
    gate_ref[...] = dot(packed, gate_adj_ref[...], outer).astype(bf16)
    up_ref[...] = dot(packed, up_adj_ref[...], outer).astype(bf16)


def grad_in(packed, gate_adj, up_adj):
    count, model = packed.shape
    hidden = gate_adj.shape[1]
    size = 512
    out = pl.BlockSpec((size, hidden), lambda i: (i, 0))
    return pl.pallas_call(
        grad_in_kernel,
        grid=(model // size,),
        in_specs=[
            pl.BlockSpec((count, size), lambda i: (0, i)),
            whole((count, hidden)),
            whole((count, hidden)),
        ],
        out_specs=[out, out],
        out_shape=[jax.ShapeDtypeStruct((model, hidden), bf16)] * 2,
        compiler_params=params(),
        cost_estimate=pl.CostEstimate(
            flops=4 * count * model * hidden, transcendentals=0, bytes_accessed=11 << 20
        ),
        name="grad_in",
    )(packed, gate_adj, up_adj)


def grad_down_kernel(core_ref, active_ref, near_ref, far_ref, out_ref):
    active = active_ref[...]

    @pl.when(pl.program_id(0) == 0)
    def _():
        out_ref[...] = dot(active, near_ref[...], outer).astype(bf16)

    @pl.when(pl.program_id(0) == 1)
    def _():
        out_ref[...] = dot(active, far_ref[...], outer).astype(bf16)


def grad_down_of(core, active, near_rows, far_rows):
    count, hidden = active.shape
    half = near_rows.shape[1]
    return pl.pallas_call(
        grad_down_kernel,
        grid_spec=pltpu.PrefetchScalarGridSpec(
            num_scalar_prefetch=1,
            grid=(2,),
            in_specs=[whole((count, hidden)), whole((count, half)), whole((count, half))],
            out_specs=pl.BlockSpec((hidden, half), lambda i, c: (0, i + c[0] - 2 * i * c[0])),
        ),
        out_shape=jax.ShapeDtypeStruct((hidden, 2 * half), bf16),
        compiler_params=params(),
        cost_estimate=pl.CostEstimate(
            flops=4 * count * half * hidden, transcendentals=0, bytes_accessed=9 << 20
        ),
        name="grad_down",
    )(core, active, near_rows, far_rows)


def combine_kernel(core_ref, block_ref, target_ref, cot_ref, out_ref, total, scratch):
    step = pl.program_id(0)
    tokens = cot_ref.shape[0]
    rows = unpack(block_ref[...], scratch)
    size = rows.shape[0]
    place = lax.broadcasted_iota(jnp.int32, (tokens, size), 1) + step * size
    chosen = jnp.where(
        (place == target_ref[:, 0:1]) | (place == target_ref[:, 1:2]), 1.0, 0.0
    ).astype(bf16)
    found = dot(chosen, rows, plain)

    @pl.when(step == 0)
    def _():
        total[...] = found

    @pl.when(step > 0)
    def _():
        total[...] = total[...] + found

    @pl.when(step == pl.num_programs(0) - 1)
    def _():
        out_ref[...] = (cot_ref[...].astype(f32) + total[...]).astype(bf16)


def combine(core, returned, target, cotangent):
    experts, _, wide = returned.shape
    half = wide - 128
    tokens = cotangent.shape[0]
    return pl.pallas_call(
        combine_kernel,
        grid_spec=pltpu.PrefetchScalarGridSpec(
            num_scalar_prefetch=1,
            grid=(experts // (pair * group),),
            in_specs=[
                pl.BlockSpec((pair * group, main, wide), lambda i, c: (i, 0, 0)),
                whole((tokens, 8)),
                pl.BlockSpec((tokens, half), lambda i, c: (0, c[0])),
            ],
            out_specs=whole((tokens, half)),
            scratch_shapes=[pltpu.VMEM((tokens, half), f32), pltpu.VMEM((128, 128), f32)],
        ),
        out_shape=jax.ShapeDtypeStruct((tokens, half), bf16),
        compiler_params=params(),
        name="combine",
    )(core, returned, target, cotangent)


def two_terms(value):
    high = value.astype(bf16)
    return high, (value - high.astype(f32)).astype(bf16)


def scan_kernel(
    core_ref, own_ref, peer_ref, weight_ref, slope_ref, gelu_ref, ahead_ref, product_ref, first_ref,
    share_ref, grad_y_ref, local_ref, out_ref, head_ref, scratch,
):
    tokens, half = own_ref.shape
    channels = weight_ref.shape[1]
    core = core_ref[0]
    near_weight = weight_ref[pl.ds(pl.multiple_of(core * half, half), half), :]
    far_weight = weight_ref[pl.ds(pl.multiple_of((1 - core) * half, half), half), :]
    grad = dot(own_ref[...], near_weight, plain) + dot(peer_ref[...], far_weight, plain)
    grad_y_ref[...] = grad * slope_ref[...]
    state_grad = grad * gelu_ref[...]
    length = tokens // segments
    blocks = scratch.shape[0]
    for b in range(blocks):
        scratch[b] = state_grad[:, 128 * b : 128 * (b + 1)]
    carries = []
    for b in range(blocks):
        at = slice(128 * b, 128 * (b + 1))
        value = None
        for j in reversed(range(length)):
            here = scratch[b, pl.ds(j, segments, stride=length), :]
            if value is None:
                value = here
            else:
                value = here + ahead_ref[b, pl.ds(j, segments, stride=length), :] * value
            local_ref[b, pl.ds(j, segments, stride=length), :] = value
        product = product_ref[b, pl.ds(0, segments, stride=length), :]
        carry = value[segments - 1 : segments]
        for s in reversed(range(1, segments - 1)):
            carry = value[s : s + 1] + product[s : s + 1] * carry
        ends = local_ref[b, 0:3, :] + product_ref[b, 0:3, :] * carry
        carries.append(first_ref[0:1, at] * ends[0:1])
        head_ref[:, at] = jnp.concatenate(
            [ends, first_ref[3:15, at], jnp.zeros((1, 128), f32)], axis=0
        )
    decay = jnp.concatenate([first_ref[1:2, 128 * b : 128 * (b + 1)] for b in range(blocks)], axis=0)
    terms = two_terms(decay) + two_terms(jnp.concatenate(carries, axis=0))
    line = jnp.concatenate([term.astype(f32) for term in terms], axis=0).astype(bf16)
    out_ref[:, :, 0:channels] = share_ref[...]
    out_ref[:, :, channels:] = jnp.broadcast_to(line[None], (out_ref.shape[0], *line.shape))


def scan(core, own, peer, weight, slope, gelu, ahead, product, first, share):
    tokens, half = own.shape
    channels = weight.shape[1]
    experts, rows, _ = share.shape
    return pl.pallas_call(
        scan_kernel,
        grid_spec=pltpu.PrefetchScalarGridSpec(
            num_scalar_prefetch=1,
            grid=(1,),
            in_specs=[
                whole((tokens, half)),
                whole((tokens, half)),
                whole(weight.shape),
                whole((tokens, channels)),
                whole((tokens, channels)),
                whole(ahead.shape),
                whole(ahead.shape),
                whole((16, channels)),
                whole(share.shape),
            ],
            out_specs=[
                whole((tokens, channels)),
                whole(ahead.shape),
                whole((experts, rows, channels + 128)),
                whole((16, channels)),
            ],
            scratch_shapes=[pltpu.VMEM(ahead.shape, f32)],
        ),
        out_shape=[
            jax.ShapeDtypeStruct((tokens, channels), f32),
            jax.ShapeDtypeStruct(ahead.shape, f32),
            jax.ShapeDtypeStruct((experts, rows, channels + 128), bf16),
            jax.ShapeDtypeStruct((16, channels), f32),
        ],
        compiler_params=params(),
        cost_estimate=pl.CostEstimate(
            flops=4 * tokens * half * channels, transcendentals=0, bytes_accessed=9 << 20
        ),
        name="scan",
    )(core, own, peer, weight, slope, gelu, ahead, product, first, share)


def project_kernel(core_ref, own_ref, peer_ref, mixed_ref, early_ref, late_ref):
    core = core_ref[0]
    mixed = mixed_ref[...]
    owners, rows, channels = early_ref.shape
    share = owners // 2
    for ref, place in ((own_ref, core), (peer_ref, 1 - core)):
        value = dot(ref[...], mixed, outer).astype(bf16).reshape(share, 2 * rows, channels)
        at = pl.ds(pl.multiple_of(place * share, share), share)
        early_ref[at] = value[:, 0:rows]
        late_ref[at] = value[:, rows:]


def project(core, own, peer, mixed, owners):
    tokens, half = own.shape
    channels = mixed.shape[1]
    shape = (owners, half // owners, channels)
    return pl.pallas_call(
        project_kernel,
        grid_spec=pltpu.PrefetchScalarGridSpec(
            num_scalar_prefetch=1,
            grid=(1,),
            in_specs=[whole((tokens, half)), whole((tokens, half)), whole((tokens, channels))],
            out_specs=[whole(shape), whole(shape)],
        ),
        out_shape=[jax.ShapeDtypeStruct(shape, bf16)] * 2,
        compiler_params=params(),
        name="project",
    )(core, own, peer, mixed)


def tail_kernel(
    place_ref, line_ref, head_ref, local_ref, product_ref, keep_ref, input_ref, direct_ref,
    a_ref, i_ref, taps_ref, out_ref, carries, adjoint, grads,
):
    step = pl.program_id(0)
    tokens = local_ref.shape[1]
    length = tokens // segments
    place = place_ref[0]

    @pl.when(step == 0)
    def _():
        own = jnp.zeros((4, 128), f32)
        beyond = jnp.zeros((4, 128), f32)
        for j in reversed(range(line_ref.shape[0])):
            line = line_ref[j].astype(f32)
            decay = line[0:4] + line[4:8]
            total = line[8:12] + line[12:16]
            own = jnp.where(j > place, total + decay * own, own)
            beyond = jnp.where(j > place + 1, total + decay * beyond, beyond)
        carries[0:4, :] = own
        carries[4:8, :] = beyond

    def conv_grad(value, keep, gate, direct):
        keep = (value * keep).astype(bf16)
        gate = (value * gate).astype(bf16)
        return value * direct + dot(keep, a_ref[0], inner) + dot(gate, i_ref[0], inner)

    carry = carries[pl.ds(step, 1), :]
    for s in reversed(range(segments)):
        lo = s * length
        piece = local_ref[0, lo : lo + length, :] + product_ref[0, lo : lo + length, :] * carry
        adjoint[lo : lo + length, :] = piece
        carry = piece[0:1]
    grads[0:tokens, :] = conv_grad(adjoint[...], keep_ref[...], input_ref[...], direct_ref[...])
    head = head_ref[...]
    spare = jnp.zeros((5, 128), f32)
    three = lambda k: jnp.concatenate([head[3 * k : 3 * k + 3], spare], axis=0)
    later = three(0) + three(1) * carries[pl.ds(step + 4, 1), :]
    grads[tokens : tokens + 8, :] = conv_grad(later, three(2), three(3), three(4))
    total = taps_ref[0:1, :] * grads[3 : 3 + tokens, :]
    for j in range(1, 4):
        total = total + taps_ref[j : j + 1, :] * grads[3 - j : 3 - j + tokens, :]
    out_ref[...] = total


def tail(place, shares, head, local, product, keep, gate, direct, gate_a, gate_x, taps):
    blocks, tokens, span = local.shape
    channels = blocks * span
    owners, rows, _ = shares.shape
    cube = pl.BlockSpec((1, tokens, span), lambda i, c: (i, 0, 0))
    col = lambda rows: pl.BlockSpec((rows, span), lambda i, c: (0, i))
    block = pl.BlockSpec((1, span, span), lambda i, c: (i, 0, 0))
    line = pl.BlockSpec((owners, rows, 128), lambda i, c: (0, 0, channels // 128))
    return pl.pallas_call(
        tail_kernel,
        grid_spec=pltpu.PrefetchScalarGridSpec(
            num_scalar_prefetch=1,
            grid=(blocks,),
            in_specs=[line, col(16), cube, cube] + [col(tokens)] * 3 + [block, block, col(4)],
            out_specs=col(tokens),
            scratch_shapes=[
                pltpu.VMEM((8, span), f32),
                pltpu.VMEM((tokens, span), f32),
                pltpu.VMEM((tokens + 8, span), f32),
            ],
        ),
        out_shape=jax.ShapeDtypeStruct((tokens, channels), f32),
        compiler_params=params(),
        name="tail",
    )(place, shares, head, local, product, keep, gate, direct, gate_a, gate_x, taps)


def exchange(value, axis):
    return lax.all_to_all(value, axis, split_axis=0, concat_axis=0, tiled=True)


def swapped(value):
    return lax.ppermute(value, "tp", [(0, 1), (1, 0)])


def shifted(value, axis, by):
    devices = lax.axis_size(axis)
    pairs = [(i, i + by) for i in range(devices) if 0 <= i + by < devices]
    return lax.ppermute(value, axis, pairs)


def body(
    cotangent,
    routes,
    route_weight,
    expert_rows,
    gate_w,
    up_w,
    down_w,
    in_x,
    in_y,
    state,
    conv_taps,
    gate_a,
    gate_x,
    decay_rate,
    out_weight,
):
    tokens = cotangent.shape[0]
    experts = lax.axis_size("sp")
    core = lax.axis_index("tp").astype(jnp.int32).reshape(1)
    taps = conv_taps.shape[0]
    channels = in_x.shape[1]

    place = lax.axis_index("sp").astype(jnp.int32).reshape(1)

    edge = shifted(
        jnp.concatenate([in_x[tokens - taps + 1 :], state[tokens - 1 :]], axis=0), "sp", 1
    )
    outgoing, target = send(core, routes.T, route_weight.T, cotangent, experts)
    outgoing, edge = lax.optimization_barrier((outgoing, edge))
    arrived = exchange(outgoing, "sp")
    target = target.T

    packed, silu, slope, active = expert_pre(expert_rows[0], gate_w[0], up_w[0])
    mixed, y_slope, gelu, ahead, product, keep_part, input_part, direct, first = recur_pre(
        in_x, in_y, state, edge, conv_taps, gate_a, gate_x, decay_rate[None]
    )

    arrived_far = swapped(arrived)
    near_rows, part = near(core, arrived, down_w[0])
    far_rows, gate_adj, up_adj, back_far = far(
        core, arrived_far, down_w[0], part, silu, slope, gate_w[0], up_w[0]
    )
    back_in = swapped(back_far)
    own = back_own(core, gate_adj, up_adj, gate_w[0], up_w[0], arrived.shape)
    returning = (own.astype(f32) + back_in.astype(f32)).astype(bf16)
    returned = exchange(returning, "sp")

    grad_gate, grad_up = grad_in(packed, gate_adj, up_adj)
    grad_down = grad_down_of(core, active, near_rows, far_rows)

    stream_own = combine(core, returned, target, cotangent)
    stream_peer = swapped(stream_own)
    early, late = project(core, stream_own, stream_peer, mixed, experts)
    early_shares = exchange(early, "sp")
    grad_y, local, late, head = scan(
        core, stream_own, stream_peer, out_weight, y_slope, gelu, ahead, product, first, late
    )
    head = shifted(head, "sp", -1)
    late_shares = exchange(late, "sp")
    grad_x = tail(
        place, late_shares, head, local, product, keep_part, input_part, direct,
        gate_a, gate_x, conv_taps,
    )
    grad_proj = jnp.concatenate(
        [
            jnp.sum(early_shares.astype(f32), axis=0),
            jnp.sum(late_shares[:, :, :channels].astype(f32), axis=0),
        ],
        axis=0,
    )
    return (grad_gate[None], grad_up[None], grad_down[None], grad_proj, grad_x, grad_y)


def solution(mesh):
    in_specs = (
        P("sp", None),
        P("sp", None),
        P("sp", None),
        P("sp", None, None),
        P("sp", None, "tp"),
        P("sp", None, "tp"),
        P("sp", "tp", None),
        P("sp", "tp"),
        P("sp", "tp"),
        P("sp", "tp"),
        P(None, "tp"),
        P("tp", None, None),
        P("tp", None, None),
        P("tp"),
        P(None, "tp"),
    )
    out_specs = (
        P("sp", None, "tp"),
        P("sp", None, "tp"),
        P("sp", "tp", None),
        P("sp", "tp"),
        P("sp", "tp"),
        P("sp", "tp"),
    )
    return jax.shard_map(body, mesh=mesh, in_specs=in_specs, out_specs=out_specs, check_vma=False)
```

```python
import jax
import jax.numpy as jnp
from jax import lax
from jax.experimental import pallas as pl
from jax.experimental.pallas import tpu as pltpu
from jax.sharding import PartitionSpec as P

rate_scale = 8.0
floor_square = 0.01
inv_root_two = 0.7071067811865476
inv_root_tau = 0.3989422804014327

f32 = jnp.float32
bf16 = jnp.bfloat16
inner = (((1,), (1,)), ((), ()))
outer = (((0,), (0,)), ((), ()))
plain = (((1,), (0,)), ((), ()))

group = 8
main = 16
extra = 2
main_rows = group * main
group_rows = group * (main + extra)
segments = 8


def dot(a, b, dims):
    return lax.dot_general(a, b, dims, preferred_element_type=f32)


def params(n=1, mb=32):
    return pltpu.CompilerParams(dimension_semantics=("arbitrary",) * n, vmem_limit_bytes=mb << 20)


def whole(shape):
    return pl.BlockSpec(shape, lambda *_: (0,) * len(shape))


def pack_extras(rows, scratch):
    for j in range(8):
        scratch[pl.ds(j, group * extra, stride=8), :] = rows[:, 128 * j : 128 * (j + 1)]
    return scratch[...]


def unpack_extras(tiles, scratch):
    scratch[...] = tiles
    return jnp.concatenate(
        [scratch[pl.ds(j, group * extra, stride=8), :] for j in range(8)], axis=1
    )


def send_kernel(core_ref, routes_ref, weight_ref, cot_ref, out_ref, target_ref, slot, scratch):
    step = pl.program_id(0)
    tokens = cot_ref.shape[0]
    experts = pl.num_programs(0) * group

    @pl.when(step == 0)
    def _():
        first = routes_ref[0:1, :]
        second = routes_ref[1:2, :]
        expert = lax.broadcasted_iota(jnp.int32, (experts, tokens), 0)
        hit_first = (expert == first).astype(f32)
        hit_second = (expert == second).astype(f32)
        earlier = (
            lax.broadcasted_iota(jnp.int32, (tokens, tokens), 0)
            < lax.broadcasted_iota(jnp.int32, (tokens, tokens), 1)
        ).astype(f32)
        before = dot((hit_first + hit_second).astype(bf16), earlier.astype(bf16), plain)
        place_first = jnp.sum(before * hit_first, axis=0, keepdims=True).astype(jnp.int32)
        place_second = jnp.sum(before * hit_second, axis=0, keepdims=True).astype(jnp.int32)
        place_second = place_second + (first == second).astype(jnp.int32)
        for k, (name, place) in enumerate(((first, place_first), (second, place_second))):
            base = group_rows * (name >> 3)
            inside = name & 7
            slot[k : k + 1, :] = base + jnp.where(
                place < main, main * inside + place, main_rows + extra * inside + place - main
            )
        target_ref[...] = jnp.concatenate(
            [slot[0:2, :], jnp.zeros((6, tokens), jnp.int32)], axis=0
        )

    rows = lax.broadcasted_iota(jnp.int32, (group_rows, tokens), 0) + step * group_rows
    hit_first = rows == slot[0:1, :]
    hit_second = rows == slot[1:2, :]
    chosen = jnp.where(hit_first | hit_second, 1.0, 0.0).astype(bf16)
    weight = jnp.sum(
        jnp.where(hit_first, weight_ref[0:1, :], 0.0)
        + jnp.where(hit_second, weight_ref[1:2, :], 0.0),
        axis=1,
        keepdims=True,
    )
    values = dot(chosen, cot_ref[...], plain) * weight
    width = values.shape[1]
    out_ref[:, :, 0:width] = values[0:main_rows].astype(bf16).reshape(group, main, width)
    tiles = pack_extras(values[main_rows:], scratch)
    out_ref[:, :, width:] = tiles.astype(bf16).reshape(group, main, 128)


def send(core, routes, weight, cotangent, experts):
    tokens, model = cotangent.shape
    half = model // 2
    return pl.pallas_call(
        send_kernel,
        grid_spec=pltpu.PrefetchScalarGridSpec(
            num_scalar_prefetch=1,
            grid=(experts // group,),
            in_specs=[
                whole((2, tokens)),
                whole((2, tokens)),
                pl.BlockSpec((tokens, half), lambda i, c: (0, c[0])),
            ],
            out_specs=[
                pl.BlockSpec((group, main, half + 128), lambda i, c: (i, 0, 0)),
                whole((8, tokens)),
            ],
            scratch_shapes=[pltpu.VMEM((8, tokens), jnp.int32), pltpu.VMEM((128, 128), f32)],
        ),
        out_shape=[
            jax.ShapeDtypeStruct((experts, main, half + 128), bf16),
            jax.ShapeDtypeStruct((8, tokens), jnp.int32),
        ],
        compiler_params=params(),
        name="send",
    )(core, routes, weight, cotangent)


pair = 2


def expert_pre_kernel(rows_ref, gate_ref, up_ref, packed_ref, silu_ref, slope_ref, active_ref):
    out_row = lax.broadcasted_iota(jnp.int32, (group_rows, group_rows), 0)
    column = lax.broadcasted_iota(jnp.int32, (group_rows, group_rows), 1)
    late = out_row - main_rows
    source = jnp.where(
        out_row < main_rows,
        (main + extra) * (out_row >> 4) + (out_row & 15),
        (main + extra) * (late >> 1) + main + (late & 1),
    )
    order = jnp.where(column == source, 1.0, 0.0).astype(bf16)
    for g in range(pair):
        lo = g * group_rows
        packed_ref[lo : lo + group_rows, :] = dot(
            order, rows_ref[lo : lo + group_rows, :], plain
        ).astype(bf16)
    packed = packed_ref[...]
    pre_gate = dot(packed, gate_ref[...], plain)
    pre_up = dot(packed, up_ref[...], plain)
    gate = jax.nn.sigmoid(pre_gate)
    silu = pre_gate * gate
    silu_ref[...] = silu
    slope_ref[...] = pre_up * gate * (1.0 + pre_gate * (1.0 - gate))
    active_ref[...] = (silu * pre_up).astype(bf16)


def expert_pre(rows, gate, up):
    count, model = rows.shape
    hidden = gate.shape[1]
    size = pair * group_rows
    by_row = lambda width: pl.BlockSpec((size, width), lambda i: (i, 0))
    return pl.pallas_call(
        expert_pre_kernel,
        grid=(count // size,),
        in_specs=[by_row(model), whole((model, hidden)), whole((model, hidden))],
        out_specs=[by_row(model), by_row(hidden), by_row(hidden), by_row(hidden)],
        out_shape=[
            jax.ShapeDtypeStruct((count, model), bf16),
            jax.ShapeDtypeStruct((count, hidden), f32),
            jax.ShapeDtypeStruct((count, hidden), f32),
            jax.ShapeDtypeStruct((count, hidden), bf16),
        ],
        compiler_params=params(),
        cost_estimate=pl.CostEstimate(
            flops=4 * count * model * hidden, transcendentals=0, bytes_accessed=20 << 20
        ),
        name="expert_pre",
    )(rows, gate, up)


def recur_pre_kernel(
    x_ref, y_ref, state_ref, edge_ref, taps_ref, a_ref, i_ref, rate_ref,
    mixed_ref, grad_y_ref, gelu_ref, ahead_ref, product_ref, keep_ref, input_ref, direct_ref,
    first_ref, scratch,
):
    tokens = x_ref.shape[0]
    x = x_ref[...].astype(f32)
    edge = edge_ref[...].astype(f32)
    scratch[5:8, :] = edge[0:3]
    scratch[8 : 8 + tokens, :] = x
    conv_x = taps_ref[0:1, :] * scratch[5 : 5 + tokens, :]
    for j in range(1, 4):
        conv_x = conv_x + taps_ref[j : j + 1, :] * scratch[5 + j : 5 + j + tokens, :]
    conv_b = conv_x.astype(bf16)
    keep = jax.nn.sigmoid(dot(conv_b, a_ref[0], plain))
    gate = jax.nn.sigmoid(dot(conv_b, i_ref[0], plain))
    rate = rate_ref[...]
    decay = jnp.exp(-rate_scale * keep * rate)
    norm = jnp.sqrt(1.0 - decay * decay + floor_square)
    state = state_ref[...].astype(f32)
    scratch[7:8, :] = edge[3:4]
    scratch[8 : 8 + tokens, :] = state
    state_prev = scratch[7 : 7 + tokens, :]
    log_part = decay * state_prev - conv_x * gate * decay * decay / norm
    keep_ref[...] = log_part * (-rate_scale * rate) * keep * (1.0 - keep)
    input_ref[...] = conv_x * norm * gate * (1.0 - gate)
    direct_ref[...] = gate * norm
    y = y_ref[...].astype(f32)
    below = 0.5 * (1.0 + lax.erf(y * inv_root_two))
    gelu = y * below
    gelu_ref[...] = gelu
    mixed_ref[...] = (state * gelu).astype(bf16)
    grad_y_ref[...] = state * (below + y * jnp.exp(-0.5 * y * y) * inv_root_tau)
    scratch[0:tokens, :] = decay
    scratch[tokens : tokens + 8, :] = jnp.ones((8, decay.shape[1]), f32)
    ahead_ref[0] = scratch[1 : 1 + tokens, :]
    length = tokens // segments
    product = None
    for j in reversed(range(length)):
        step = scratch[pl.ds(j + 1, segments, stride=length), :]
        product = step if product is None else step * product
        product_ref[0, pl.ds(j, segments, stride=length), :] = product
    rest = product[1:2]
    for s in range(2, segments):
        rest = rest * product[s : s + 1]
    total = decay[0:1] * product[0:1] * rest
    first_ref[...] = jnp.concatenate(
        [
            decay[0:1],
            total,
            jnp.zeros_like(total),
            product_ref[0, 0:3, :] * rest,
            keep_ref[0:3, :],
            input_ref[0:3, :],
            direct_ref[0:3, :],
            jnp.zeros_like(total),
        ],
        axis=0,
    )


def recur_pre(in_x, in_y, state, edge, taps, gate_a, gate_x, rate):
    tokens, channels = in_x.shape
    blocks, span = gate_a.shape[:2]
    col = lambda rows: pl.BlockSpec((rows, span), lambda i: (0, i))
    block = pl.BlockSpec((1, span, span), lambda i: (i, 0, 0))
    cube = pl.BlockSpec((1, tokens, span), lambda i: (i, 0, 0))
    big = jax.ShapeDtypeStruct((tokens, channels), f32)
    return pl.pallas_call(
        recur_pre_kernel,
        grid=(blocks,),
        in_specs=[col(tokens), col(tokens), col(tokens), col(4), col(4), block, block, col(1)],
        out_specs=[col(tokens)] * 3 + [cube] * 2 + [col(tokens)] * 3 + [col(16)],
        out_shape=[jax.ShapeDtypeStruct((tokens, channels), bf16)]
        + [big] * 2
        + [jax.ShapeDtypeStruct((blocks, tokens, span), f32)] * 2
        + [big] * 3
        + [jax.ShapeDtypeStruct((16, channels), f32)],
        scratch_shapes=[pltpu.VMEM((tokens + 16, span), f32)],
        compiler_params=params(),
        cost_estimate=pl.CostEstimate(
            flops=2000 * tokens * channels, transcendentals=0, bytes_accessed=8 << 20
        ),
        name="recur_pre",
    )(in_x, in_y, state, edge, taps, gate_a, gate_x, rate)


def unpack(block, scratch):
    width = block.shape[2] - 128
    parts = []
    for g in range(block.shape[0] // group):
        own = block[g * group : (g + 1) * group]
        parts.append(own[:, :, 0:width].reshape(main_rows, width))
        tiles = own[:, :, width:].reshape(128, 128).astype(f32)
        parts.append(unpack_extras(tiles, scratch).astype(bf16))
    return jnp.concatenate(parts, axis=0)


def pack_into(out_ref, values, scratch):
    width = values.shape[1]
    for g in range(out_ref.shape[0] // group):
        lo = g * group_rows
        out_ref[g * group : (g + 1) * group, :, 0:width] = (
            values[lo : lo + main_rows].astype(bf16).reshape(group, main, width)
        )
        tiles = pack_extras(values[lo + main_rows : lo + group_rows], scratch)
        out_ref[g * group : (g + 1) * group, :, width:] = tiles.astype(bf16).reshape(
            group, main, 128
        )


def near_kernel(core_ref, block_ref, down_ref, rows_ref, part_ref, scratch):
    rows = unpack(block_ref[...], scratch)
    rows_ref[...] = rows
    part_ref[...] = dot(rows, down_ref[...], inner)


def near(core, arrived, down):
    experts, _, wide = arrived.shape
    half = wide - 128
    hidden = down.shape[0]
    count = experts * (main + extra)
    size = pair * group_rows
    return pl.pallas_call(
        near_kernel,
        grid_spec=pltpu.PrefetchScalarGridSpec(
            num_scalar_prefetch=1,
            grid=(count // size,),
            in_specs=[
                pl.BlockSpec((pair * group, main, wide), lambda i, c: (i, 0, 0)),
                pl.BlockSpec((hidden, half), lambda i, c: (0, c[0])),
            ],
            out_specs=[
                pl.BlockSpec((size, half), lambda i, c: (i, 0)),
                pl.BlockSpec((size, hidden), lambda i, c: (i, 0)),
            ],
            scratch_shapes=[pltpu.VMEM((128, 128), f32)],
        ),
        out_shape=[
            jax.ShapeDtypeStruct((count, half), bf16),
            jax.ShapeDtypeStruct((count, hidden), f32),
        ],
        compiler_params=params(),
        cost_estimate=pl.CostEstimate(
            flops=2 * count * half * hidden, transcendentals=0, bytes_accessed=9 << 20
        ),
        name="near",
    )(core, arrived, down)


def far_kernel(
    core_ref, block_ref, down_ref, part_ref, silu_ref, slope_ref, gate_ref, up_ref,
    rows_ref, gate_adj_ref, up_adj_ref, back_ref, scratch,
):
    rows = unpack(block_ref[...], scratch)
    rows_ref[...] = rows
    grad = part_ref[...] + dot(rows, down_ref[...], inner)
    gate_adj = (grad * slope_ref[...]).astype(bf16)
    up_adj = (grad * silu_ref[...]).astype(bf16)
    gate_adj_ref[...] = gate_adj
    up_adj_ref[...] = up_adj
    back = dot(gate_adj, gate_ref[...], inner) + dot(up_adj, up_ref[...], inner)
    pack_into(back_ref, back, scratch)


def far(core, arrived, down, part, silu, slope, gate, up):
    experts, _, wide = arrived.shape
    half = wide - 128
    hidden = down.shape[0]
    count = experts * (main + extra)
    size = pair * group_rows
    by_row = lambda width: pl.BlockSpec((size, width), lambda i, c: (i, 0))
    block = pl.BlockSpec((pair * group, main, wide), lambda i, c: (i, 0, 0))
    weight = pl.BlockSpec((half, hidden), lambda i, c: (1 - c[0], 0))
    return pl.pallas_call(
        far_kernel,
        grid_spec=pltpu.PrefetchScalarGridSpec(
            num_scalar_prefetch=1,
            grid=(count // size,),
            in_specs=[
                block,
                pl.BlockSpec((hidden, half), lambda i, c: (0, 1 - c[0])),
                by_row(hidden),
                by_row(hidden),
                by_row(hidden),
                weight,
                weight,
            ],
            out_specs=[by_row(half), by_row(hidden), by_row(hidden), block],
            scratch_shapes=[pltpu.VMEM((128, 128), f32)],
        ),
        out_shape=[
            jax.ShapeDtypeStruct((count, half), bf16),
            jax.ShapeDtypeStruct((count, hidden), bf16),
            jax.ShapeDtypeStruct((count, hidden), bf16),
            jax.ShapeDtypeStruct(arrived.shape, bf16),
        ],
        compiler_params=params(),
        cost_estimate=pl.CostEstimate(
            flops=6 * count * half * hidden, transcendentals=0, bytes_accessed=16 << 20
        ),
        name="far",
    )(core, arrived, down, part, silu, slope, gate, up)


def back_kernel(core_ref, gate_adj_ref, up_adj_ref, gate_ref, up_ref, back_ref, scratch):
    back = dot(gate_adj_ref[...], gate_ref[...], inner) + dot(up_adj_ref[...], up_ref[...], inner)
    pack_into(back_ref, back, scratch)


def back_own(core, gate_adj, up_adj, gate, up, shape):
    _, _, wide = shape
    half = wide - 128
    count, hidden = gate_adj.shape
    size = pair * group_rows
    by_row = lambda width: pl.BlockSpec((size, width), lambda i, c: (i, 0))
    weight = pl.BlockSpec((half, hidden), lambda i, c: (c[0], 0))
    return pl.pallas_call(
        back_kernel,
        grid_spec=pltpu.PrefetchScalarGridSpec(
            num_scalar_prefetch=1,
            grid=(count // size,),
            in_specs=[by_row(hidden), by_row(hidden), weight, weight],
            out_specs=pl.BlockSpec((pair * group, main, wide), lambda i, c: (i, 0, 0)),
            scratch_shapes=[pltpu.VMEM((128, 128), f32)],
        ),
        out_shape=jax.ShapeDtypeStruct(shape, bf16),
        compiler_params=params(),
        cost_estimate=pl.CostEstimate(
            flops=4 * count * half * hidden, transcendentals=0, bytes_accessed=7 << 20
        ),
        name="back_own",
    )(core, gate_adj, up_adj, gate, up)


def grad_in_kernel(packed_ref, gate_adj_ref, up_adj_ref, gate_ref, up_ref):
    packed = packed_ref[...]
    gate_ref[...] = dot(packed, gate_adj_ref[...], outer).astype(bf16)
    up_ref[...] = dot(packed, up_adj_ref[...], outer).astype(bf16)


def grad_in(packed, gate_adj, up_adj):
    count, model = packed.shape
    hidden = gate_adj.shape[1]
    size = 512
    out = pl.BlockSpec((size, hidden), lambda i: (i, 0))
    return pl.pallas_call(
        grad_in_kernel,
        grid=(model // size,),
        in_specs=[
            pl.BlockSpec((count, size), lambda i: (0, i)),
            whole((count, hidden)),
            whole((count, hidden)),
        ],
        out_specs=[out, out],
        out_shape=[jax.ShapeDtypeStruct((model, hidden), bf16)] * 2,
        compiler_params=params(),
        cost_estimate=pl.CostEstimate(
            flops=4 * count * model * hidden, transcendentals=0, bytes_accessed=11 << 20
        ),
        name="grad_in",
    )(packed, gate_adj, up_adj)


def grad_down_kernel(core_ref, active_ref, near_ref, far_ref, out_ref):
    active = active_ref[...]

    @pl.when(pl.program_id(0) == 0)
    def _():
        out_ref[...] = dot(active, near_ref[...], outer).astype(bf16)

    @pl.when(pl.program_id(0) == 1)
    def _():
        out_ref[...] = dot(active, far_ref[...], outer).astype(bf16)


def grad_down_of(core, active, near_rows, far_rows):
    count, hidden = active.shape
    half = near_rows.shape[1]
    return pl.pallas_call(
        grad_down_kernel,
        grid_spec=pltpu.PrefetchScalarGridSpec(
            num_scalar_prefetch=1,
            grid=(2,),
            in_specs=[whole((count, hidden)), whole((count, half)), whole((count, half))],
            out_specs=pl.BlockSpec((hidden, half), lambda i, c: (0, i + c[0] - 2 * i * c[0])),
        ),
        out_shape=jax.ShapeDtypeStruct((hidden, 2 * half), bf16),
        compiler_params=params(),
        cost_estimate=pl.CostEstimate(
            flops=4 * count * half * hidden, transcendentals=0, bytes_accessed=9 << 20
        ),
        name="grad_down",
    )(core, active, near_rows, far_rows)


def combine_kernel(core_ref, block_ref, target_ref, cot_ref, out_ref, total, scratch):
    step = pl.program_id(0)
    tokens = cot_ref.shape[0]
    rows = unpack(block_ref[...], scratch)
    size = rows.shape[0]
    place = lax.broadcasted_iota(jnp.int32, (tokens, size), 1) + step * size
    chosen = jnp.where(
        (place == target_ref[:, 0:1]) | (place == target_ref[:, 1:2]), 1.0, 0.0
    ).astype(bf16)
    found = dot(chosen, rows, plain)

    @pl.when(step == 0)
    def _():
        total[...] = found

    @pl.when(step > 0)
    def _():
        total[...] = total[...] + found

    @pl.when(step == pl.num_programs(0) - 1)
    def _():
        out_ref[...] = (cot_ref[...].astype(f32) + total[...]).astype(bf16)


def combine(core, returned, target, cotangent):
    experts, _, wide = returned.shape
    half = wide - 128
    tokens = cotangent.shape[0]
    return pl.pallas_call(
        combine_kernel,
        grid_spec=pltpu.PrefetchScalarGridSpec(
            num_scalar_prefetch=1,
            grid=(experts // (pair * group),),
            in_specs=[
                pl.BlockSpec((pair * group, main, wide), lambda i, c: (i, 0, 0)),
                whole((tokens, 8)),
                pl.BlockSpec((tokens, half), lambda i, c: (0, c[0])),
            ],
            out_specs=whole((tokens, half)),
            scratch_shapes=[pltpu.VMEM((tokens, half), f32), pltpu.VMEM((128, 128), f32)],
        ),
        out_shape=jax.ShapeDtypeStruct((tokens, half), bf16),
        compiler_params=params(),
        name="combine",
    )(core, returned, target, cotangent)


def two_terms(value):
    high = value.astype(bf16)
    return high, (value - high.astype(f32)).astype(bf16)


def share_rows(values, owners):
    value = values.astype(bf16).reshape(owners, 2 * main, values.shape[1])
    return value[:, 0:main], value[:, main:]


def own_kernel(core_ref, own_ref, weight_ref, mixed_ref, grad_ref, share_ref):
    own = own_ref[...]
    grad_ref[...] = dot(own, weight_ref[...], plain)
    left, right = share_rows(dot(own, mixed_ref[...], outer), share_ref.shape[0])
    channels = left.shape[2]
    share_ref[:, :, 0:channels] = left
    share_ref[:, :, channels:] = right


def own_part(core, own, weight, mixed, owners):
    tokens, half = own.shape
    channels = mixed.shape[1]
    return pl.pallas_call(
        own_kernel,
        grid_spec=pltpu.PrefetchScalarGridSpec(
            num_scalar_prefetch=1,
            grid=(1,),
            in_specs=[
                whole((tokens, half)),
                pl.BlockSpec((half, channels), lambda i, c: (c[0], 0)),
                whole((tokens, channels)),
            ],
            out_specs=[whole((tokens, channels)), whole((owners // 2, main, 2 * channels))],
        ),
        out_shape=[
            jax.ShapeDtypeStruct((tokens, channels), f32),
            jax.ShapeDtypeStruct((owners // 2, main, 2 * channels), bf16),
        ],
        compiler_params=params(),
        cost_estimate=pl.CostEstimate(
            flops=4 * tokens * half * channels, transcendentals=0, bytes_accessed=4 << 20
        ),
        name="own_part",
    )(core, own, weight, mixed)


def scan_kernel(
    core_ref, peer_ref, weight_ref, mixed_ref, part_ref, share_ref, slope_ref, gelu_ref, ahead_ref,
    product_ref, first_ref,
    grad_y_ref, local_ref, out_ref, head_ref, scratch,
):
    tokens, _ = peer_ref.shape
    channels = weight_ref.shape[1]
    core = core_ref[0]
    peer = peer_ref[...]
    grad = part_ref[...] + dot(peer, weight_ref[...], plain)
    grad_y_ref[...] = grad * slope_ref[...]
    state_grad = grad * gelu_ref[...]
    length = tokens // segments
    blocks = scratch.shape[0]
    for b in range(blocks):
        scratch[b] = state_grad[:, 128 * b : 128 * (b + 1)]
    owners = share_ref.shape[0]
    left, right = share_rows(dot(peer, mixed_ref[...], outer), owners)
    own_at = pl.ds(pl.multiple_of(core * owners, owners), owners)
    peer_at = pl.ds(pl.multiple_of((1 - core) * owners, owners), owners)
    out_ref[own_at, :, 0 : 2 * channels] = share_ref[...]
    out_ref[peer_at, :, 0:channels] = left
    out_ref[peer_at, :, channels : 2 * channels] = right
    carries = []
    for b in range(blocks):
        at = slice(128 * b, 128 * (b + 1))
        value = None
        for j in reversed(range(length)):
            here = scratch[b, pl.ds(j, segments, stride=length), :]
            if value is None:
                value = here
            else:
                value = here + ahead_ref[b, pl.ds(j, segments, stride=length), :] * value
            local_ref[b, pl.ds(j, segments, stride=length), :] = value
        product = product_ref[b, pl.ds(0, segments, stride=length), :]
        carry = value[segments - 1 : segments]
        for s in reversed(range(1, segments - 1)):
            carry = value[s : s + 1] + product[s : s + 1] * carry
        ends = local_ref[b, 0:3, :] + product_ref[b, 0:3, :] * carry
        carries.append(first_ref[0:1, at] * ends[0:1])
        head_ref[:, at] = jnp.concatenate(
            [ends, first_ref[3:15, at], jnp.zeros((1, 128), f32)], axis=0
        )
    decay = jnp.concatenate([first_ref[1:2, 128 * b : 128 * (b + 1)] for b in range(blocks)], axis=0)
    terms = two_terms(decay) + two_terms(jnp.concatenate(carries, axis=0))
    line = jnp.concatenate([term.astype(f32) for term in terms], axis=0).astype(bf16)
    out_ref[:, :, 2 * channels :] = jnp.broadcast_to(line[None], (out_ref.shape[0], *line.shape))


def scan(core, peer, weight, mixed, part, share, slope, gelu, ahead, product, first):
    tokens, half = peer.shape
    channels = weight.shape[1]
    owners, rows, _ = share.shape
    out_shape = (2 * owners, rows, 2 * channels + 128)
    return pl.pallas_call(
        scan_kernel,
        grid_spec=pltpu.PrefetchScalarGridSpec(
            num_scalar_prefetch=1,
            grid=(1,),
            in_specs=[
                whole((tokens, half)),
                pl.BlockSpec((half, channels), lambda i, c: (1 - c[0], 0)),
                whole((tokens, channels)),
                whole((tokens, channels)),
                whole(share.shape),
                whole((tokens, channels)),
                whole((tokens, channels)),
                whole(ahead.shape),
                whole(ahead.shape),
                whole((16, channels)),
            ],
            out_specs=[
                whole((tokens, channels)),
                whole(ahead.shape),
                whole(out_shape),
                whole((16, channels)),
            ],
            scratch_shapes=[pltpu.VMEM(ahead.shape, f32)],
        ),
        out_shape=[
            jax.ShapeDtypeStruct((tokens, channels), f32),
            jax.ShapeDtypeStruct(ahead.shape, f32),
            jax.ShapeDtypeStruct(out_shape, bf16),
            jax.ShapeDtypeStruct((16, channels), f32),
        ],
        compiler_params=params(),
        cost_estimate=pl.CostEstimate(
            flops=4 * tokens * half * channels, transcendentals=0, bytes_accessed=9 << 20
        ),
        name="scan",
    )(core, peer, weight, mixed, part, share, slope, gelu, ahead, product, first)


def tail_kernel(
    place_ref, line_ref, head_ref, local_ref, product_ref, keep_ref, input_ref, direct_ref,
    a_ref, i_ref, taps_ref, out_ref, carries, adjoint, grads,
):
    step = pl.program_id(0)
    tokens = local_ref.shape[1]
    length = tokens // segments
    place = place_ref[0]

    @pl.when(step == 0)
    def _():
        own = jnp.zeros((4, 128), f32)
        beyond = jnp.zeros((4, 128), f32)
        for j in reversed(range(line_ref.shape[0])):
            line = line_ref[j].astype(f32)
            decay = line[0:4] + line[4:8]
            total = line[8:12] + line[12:16]
            own = jnp.where(j > place, total + decay * own, own)
            beyond = jnp.where(j > place + 1, total + decay * beyond, beyond)
        carries[0:4, :] = own
        carries[4:8, :] = beyond

    def conv_grad(value, keep, gate, direct):
        keep = (value * keep).astype(bf16)
        gate = (value * gate).astype(bf16)
        return value * direct + dot(keep, a_ref[0], inner) + dot(gate, i_ref[0], inner)

    carry = carries[pl.ds(step, 1), :]
    for s in reversed(range(segments)):
        lo = s * length
        piece = local_ref[0, lo : lo + length, :] + product_ref[0, lo : lo + length, :] * carry
        adjoint[lo : lo + length, :] = piece
        carry = piece[0:1]
    grads[0:tokens, :] = conv_grad(adjoint[...], keep_ref[...], input_ref[...], direct_ref[...])
    head = head_ref[...]
    spare = jnp.zeros((5, 128), f32)
    three = lambda k: jnp.concatenate([head[3 * k : 3 * k + 3], spare], axis=0)
    later = three(0) + three(1) * carries[pl.ds(step + 4, 1), :]
    grads[tokens : tokens + 8, :] = conv_grad(later, three(2), three(3), three(4))
    total = taps_ref[0:1, :] * grads[3 : 3 + tokens, :]
    for j in range(1, 4):
        total = total + taps_ref[j : j + 1, :] * grads[3 - j : 3 - j + tokens, :]
    out_ref[...] = total


def tail(place, shares, head, local, product, keep, gate, direct, gate_a, gate_x, taps):
    blocks, tokens, span = local.shape
    channels = blocks * span
    owners, rows, _ = shares.shape
    cube = pl.BlockSpec((1, tokens, span), lambda i, c: (i, 0, 0))
    col = lambda rows: pl.BlockSpec((rows, span), lambda i, c: (0, i))
    block = pl.BlockSpec((1, span, span), lambda i, c: (i, 0, 0))
    line = pl.BlockSpec((owners, rows, 128), lambda i, c: (0, 0, 2 * channels // 128))
    return pl.pallas_call(
        tail_kernel,
        grid_spec=pltpu.PrefetchScalarGridSpec(
            num_scalar_prefetch=1,
            grid=(blocks,),
            in_specs=[line, col(16), cube, cube] + [col(tokens)] * 3 + [block, block, col(4)],
            out_specs=col(tokens),
            scratch_shapes=[
                pltpu.VMEM((8, span), f32),
                pltpu.VMEM((tokens, span), f32),
                pltpu.VMEM((tokens + 8, span), f32),
            ],
        ),
        out_shape=jax.ShapeDtypeStruct((tokens, channels), f32),
        compiler_params=params(),
        name="tail",
    )(place, shares, head, local, product, keep, gate, direct, gate_a, gate_x, taps)


def exchange(value, axis):
    return lax.all_to_all(value, axis, split_axis=0, concat_axis=0, tiled=True)


def swapped(value):
    return lax.ppermute(value, "tp", [(0, 1), (1, 0)])


def shifted(value, axis, by):
    devices = lax.axis_size(axis)
    pairs = [(i, i + by) for i in range(devices) if 0 <= i + by < devices]
    return lax.ppermute(value, axis, pairs)


def body(
    cotangent,
    routes,
    route_weight,
    expert_rows,
    gate_w,
    up_w,
    down_w,
    in_x,
    in_y,
    state,
    conv_taps,
    gate_a,
    gate_x,
    decay_rate,
    out_weight,
):
    tokens = cotangent.shape[0]
    experts = lax.axis_size("sp")
    core = lax.axis_index("tp").astype(jnp.int32).reshape(1)
    taps = conv_taps.shape[0]
    channels = in_x.shape[1]

    place = lax.axis_index("sp").astype(jnp.int32).reshape(1)

    edge = shifted(
        jnp.concatenate([in_x[tokens - taps + 1 :], state[tokens - 1 :]], axis=0), "sp", 1
    )
    outgoing, target = send(core, routes.T, route_weight.T, cotangent, experts)
    arrived = exchange(outgoing, "sp")
    target = target.T

    packed, silu, slope, active = expert_pre(expert_rows[0], gate_w[0], up_w[0])
    mixed, y_slope, gelu, ahead, product, keep_part, input_part, direct, first = recur_pre(
        in_x, in_y, state, edge, conv_taps, gate_a, gate_x, decay_rate[None]
    )

    arrived_far = swapped(arrived)
    near_rows, part = near(core, arrived, down_w[0])
    far_rows, gate_adj, up_adj, back_far = far(
        core, arrived_far, down_w[0], part, silu, slope, gate_w[0], up_w[0]
    )
    back_in = swapped(back_far)
    own = back_own(core, gate_adj, up_adj, gate_w[0], up_w[0], arrived.shape)
    returning = (own.astype(f32) + back_in.astype(f32)).astype(bf16)
    returned = exchange(returning, "sp")

    grad_gate, grad_up = grad_in(packed, gate_adj, up_adj)
    grad_down = grad_down_of(core, active, near_rows, far_rows)

    stream_own = combine(core, returned, target, cotangent)
    stream_peer = swapped(stream_own)
    part, share = own_part(core, stream_own, out_weight, mixed, experts)
    grad_y, local, outgoing, head = scan(
        core, stream_peer, out_weight, mixed, part, share, y_slope, gelu, ahead, product, first
    )
    head = shifted(head, "sp", -1)
    shares = exchange(outgoing, "sp")
    grad_x = tail(
        place, shares, head, local, product, keep_part, input_part, direct,
        gate_a, gate_x, conv_taps,
    )
    summed = jnp.sum(shares[:, :, : 2 * channels].astype(f32), axis=0)
    grad_proj = jnp.concatenate([summed[:, :channels], summed[:, channels:]], axis=0)
    return (grad_gate[None], grad_up[None], grad_down[None], grad_proj, grad_x, grad_y)


def solution(mesh):
    in_specs = (
        P("sp", None),
        P("sp", None),
        P("sp", None),
        P("sp", None, None),
        P("sp", None, "tp"),
        P("sp", None, "tp"),
        P("sp", "tp", None),
        P("sp", "tp"),
        P("sp", "tp"),
        P("sp", "tp"),
        P(None, "tp"),
        P("tp", None, None),
        P("tp", None, None),
        P("tp"),
        P(None, "tp"),
    )
    out_specs = (
        P("sp", None, "tp"),
        P("sp", None, "tp"),
        P("sp", "tp", None),
        P("sp", "tp"),
        P("sp", "tp"),
        P("sp", "tp"),
    )
    return jax.shard_map(body, mesh=mesh, in_specs=in_specs, out_specs=out_specs, check_vma=False)
```

```python
import jax
import jax.numpy as jnp
from jax import lax
from jax.experimental import pallas as pl
from jax.experimental.pallas import tpu as pltpu
from jax.sharding import PartitionSpec as P

rate_scale = 8.0
floor_square = 0.01
inv_root_two = 0.7071067811865476
inv_root_tau = 0.3989422804014327

f32 = jnp.float32
bf16 = jnp.bfloat16
inner = (((1,), (1,)), ((), ()))
outer = (((0,), (0,)), ((), ()))
plain = (((1,), (0,)), ((), ()))

group = 8
main = 16
extra = 2
main_rows = group * main
group_rows = group * (main + extra)
segments = 8


def dot(a, b, dims):
    return lax.dot_general(a, b, dims, preferred_element_type=f32)


def params(n=1, mb=32):
    return pltpu.CompilerParams(dimension_semantics=("arbitrary",) * n, vmem_limit_bytes=mb << 20)


def held(value):
    return pltpu.with_memory_space_constraint(value, pltpu.HBM)


def whole(shape):
    return pl.BlockSpec(shape, lambda *_: (0,) * len(shape))


def pack_extras(rows, scratch):
    for j in range(8):
        scratch[pl.ds(j, group * extra, stride=8), :] = rows[:, 128 * j : 128 * (j + 1)]
    return scratch[...]


def unpack_extras(tiles, scratch):
    scratch[...] = tiles
    return jnp.concatenate(
        [scratch[pl.ds(j, group * extra, stride=8), :] for j in range(8)], axis=1
    )


def send_kernel(core_ref, routes_ref, weight_ref, cot_ref, out_ref, target_ref, slot, scratch):
    step = pl.program_id(0)
    tokens = cot_ref.shape[0]
    experts = pl.num_programs(0) * group

    @pl.when(step == 0)
    def _():
        first = routes_ref[0:1, :]
        second = routes_ref[1:2, :]
        expert = lax.broadcasted_iota(jnp.int32, (experts, tokens), 0)
        hit_first = (expert == first).astype(f32)
        hit_second = (expert == second).astype(f32)
        earlier = (
            lax.broadcasted_iota(jnp.int32, (tokens, tokens), 0)
            < lax.broadcasted_iota(jnp.int32, (tokens, tokens), 1)
        ).astype(f32)
        before = dot((hit_first + hit_second).astype(bf16), earlier.astype(bf16), plain)
        place_first = jnp.sum(before * hit_first, axis=0, keepdims=True).astype(jnp.int32)
        place_second = jnp.sum(before * hit_second, axis=0, keepdims=True).astype(jnp.int32)
        place_second = place_second + (first == second).astype(jnp.int32)
        for k, (name, place) in enumerate(((first, place_first), (second, place_second))):
            base = group_rows * (name >> 3)
            inside = name & 7
            slot[k : k + 1, :] = base + jnp.where(
                place < main, main * inside + place, main_rows + extra * inside + place - main
            )
        target_ref[...] = jnp.concatenate(
            [slot[0:2, :], jnp.zeros((6, tokens), jnp.int32)], axis=0
        )

    rows = lax.broadcasted_iota(jnp.int32, (group_rows, tokens), 0) + step * group_rows
    hit_first = rows == slot[0:1, :]
    hit_second = rows == slot[1:2, :]
    chosen = jnp.where(hit_first | hit_second, 1.0, 0.0).astype(bf16)
    weight = jnp.sum(
        jnp.where(hit_first, weight_ref[0:1, :], 0.0)
        + jnp.where(hit_second, weight_ref[1:2, :], 0.0),
        axis=1,
        keepdims=True,
    )
    values = dot(chosen, cot_ref[...], plain) * weight
    width = values.shape[1]
    out_ref[:, :, 0:width] = values[0:main_rows].astype(bf16).reshape(group, main, width)
    tiles = pack_extras(values[main_rows:], scratch)
    out_ref[:, :, width:] = tiles.astype(bf16).reshape(group, main, 128)


def send(core, routes, weight, cotangent, experts):
    tokens, model = cotangent.shape
    half = model // 2
    return pl.pallas_call(
        send_kernel,
        grid_spec=pltpu.PrefetchScalarGridSpec(
            num_scalar_prefetch=1,
            grid=(experts // group,),
            in_specs=[
                whole((2, tokens)),
                whole((2, tokens)),
                pl.BlockSpec((tokens, half), lambda i, c: (0, c[0])),
            ],
            out_specs=[
                pl.BlockSpec((group, main, half + 128), lambda i, c: (i, 0, 0)),
                whole((8, tokens)),
            ],
            scratch_shapes=[pltpu.VMEM((8, tokens), jnp.int32), pltpu.VMEM((128, 128), f32)],
        ),
        out_shape=[
            pltpu.HBM((experts, main, half + 128), bf16),
            jax.ShapeDtypeStruct((8, tokens), jnp.int32),
        ],
        compiler_params=params(),
        name="send",
    )(core, held(routes), held(weight), held(cotangent))


pair = 2


def expert_pre_kernel(rows_ref, gate_ref, up_ref, packed_ref, silu_ref, slope_ref, active_ref):
    out_row = lax.broadcasted_iota(jnp.int32, (group_rows, group_rows), 0)
    column = lax.broadcasted_iota(jnp.int32, (group_rows, group_rows), 1)
    late = out_row - main_rows
    source = jnp.where(
        out_row < main_rows,
        (main + extra) * (out_row >> 4) + (out_row & 15),
        (main + extra) * (late >> 1) + main + (late & 1),
    )
    order = jnp.where(column == source, 1.0, 0.0).astype(bf16)
    for g in range(pair):
        lo = g * group_rows
        packed_ref[lo : lo + group_rows, :] = dot(
            order, rows_ref[lo : lo + group_rows, :], plain
        ).astype(bf16)
    packed = packed_ref[...]
    pre_gate = dot(packed, gate_ref[...], plain)
    pre_up = dot(packed, up_ref[...], plain)
    gate = jax.nn.sigmoid(pre_gate)
    silu = pre_gate * gate
    silu_ref[...] = silu
    slope_ref[...] = pre_up * gate * (1.0 + pre_gate * (1.0 - gate))
    active_ref[...] = (silu * pre_up).astype(bf16)


def expert_pre(rows, gate, up):
    count, model = rows.shape
    hidden = gate.shape[1]
    size = pair * group_rows
    by_row = lambda width: pl.BlockSpec((size, width), lambda i: (i, 0))
    return pl.pallas_call(
        expert_pre_kernel,
        grid=(count // size,),
        in_specs=[by_row(model), whole((model, hidden)), whole((model, hidden))],
        out_specs=[by_row(model), by_row(hidden), by_row(hidden), by_row(hidden)],
        out_shape=[
            pltpu.HBM((count, model), bf16),
            pltpu.HBM((count, hidden), f32),
            pltpu.HBM((count, hidden), f32),
            pltpu.HBM((count, hidden), bf16),
        ],
        compiler_params=params(),
        cost_estimate=pl.CostEstimate(
            flops=4 * count * model * hidden, transcendentals=0, bytes_accessed=20 << 20
        ),
        name="expert_pre",
    )(held(rows), held(gate), held(up))


def recur_pre_kernel(
    x_ref, y_ref, state_ref, edge_ref, taps_ref, a_ref, i_ref, rate_ref,
    mixed_ref, grad_y_ref, gelu_ref, ahead_ref, product_ref, keep_ref, input_ref, direct_ref,
    first_ref, scratch,
):
    tokens = x_ref.shape[0]
    x = x_ref[...].astype(f32)
    edge = edge_ref[...].astype(f32)
    scratch[5:8, :] = edge[0:3]
    scratch[8 : 8 + tokens, :] = x
    conv_x = taps_ref[0:1, :] * scratch[5 : 5 + tokens, :]
    for j in range(1, 4):
        conv_x = conv_x + taps_ref[j : j + 1, :] * scratch[5 + j : 5 + j + tokens, :]
    conv_b = conv_x.astype(bf16)
    keep = jax.nn.sigmoid(dot(conv_b, a_ref[0], plain))
    gate = jax.nn.sigmoid(dot(conv_b, i_ref[0], plain))
    rate = rate_ref[...]
    decay = jnp.exp(-rate_scale * keep * rate)
    norm = jnp.sqrt(1.0 - decay * decay + floor_square)
    state = state_ref[...].astype(f32)
    scratch[7:8, :] = edge[3:4]
    scratch[8 : 8 + tokens, :] = state
    state_prev = scratch[7 : 7 + tokens, :]
    log_part = decay * state_prev - conv_x * gate * decay * decay / norm
    keep_ref[...] = log_part * (-rate_scale * rate) * keep * (1.0 - keep)
    input_ref[...] = conv_x * norm * gate * (1.0 - gate)
    direct_ref[...] = gate * norm
    y = y_ref[...].astype(f32)
    below = 0.5 * (1.0 + lax.erf(y * inv_root_two))
    gelu = y * below
    gelu_ref[...] = gelu
    mixed_ref[...] = (state * gelu).astype(bf16)
    grad_y_ref[...] = state * (below + y * jnp.exp(-0.5 * y * y) * inv_root_tau)
    scratch[0:tokens, :] = decay
    scratch[tokens : tokens + 8, :] = jnp.ones((8, decay.shape[1]), f32)
    ahead_ref[0] = scratch[1 : 1 + tokens, :]
    length = tokens // segments
    product = None
    for j in reversed(range(length)):
        step = scratch[pl.ds(j + 1, segments, stride=length), :]
        product = step if product is None else step * product
        product_ref[0, pl.ds(j, segments, stride=length), :] = product
    rest = product[1:2]
    for s in range(2, segments):
        rest = rest * product[s : s + 1]
    total = decay[0:1] * product[0:1] * rest
    first_ref[...] = jnp.concatenate(
        [
            decay[0:1],
            total,
            jnp.zeros_like(total),
            product_ref[0, 0:3, :] * rest,
            keep_ref[0:3, :],
            input_ref[0:3, :],
            direct_ref[0:3, :],
            jnp.zeros_like(total),
        ],
        axis=0,
    )


def recur_pre(in_x, in_y, state, edge, taps, gate_a, gate_x, rate):
    tokens, channels = in_x.shape
    blocks, span = gate_a.shape[:2]
    col = lambda rows: pl.BlockSpec((rows, span), lambda i: (0, i))
    block = pl.BlockSpec((1, span, span), lambda i: (i, 0, 0))
    cube = pl.BlockSpec((1, tokens, span), lambda i: (i, 0, 0))
    big = pltpu.HBM((tokens, channels), f32)
    return pl.pallas_call(
        recur_pre_kernel,
        grid=(blocks,),
        in_specs=[col(tokens), col(tokens), col(tokens), col(4), col(4), block, block, col(1)],
        out_specs=[col(tokens)] * 3 + [cube] * 2 + [col(tokens)] * 3 + [col(16)],
        out_shape=[pltpu.HBM((tokens, channels), bf16)]
        + [big] * 2
        + [pltpu.HBM((blocks, tokens, span), f32)] * 2
        + [big] * 3
        + [pltpu.HBM((16, channels), f32)],
        scratch_shapes=[pltpu.VMEM((tokens + 16, span), f32)],
        compiler_params=params(),
        cost_estimate=pl.CostEstimate(
            flops=2000 * tokens * channels, transcendentals=0, bytes_accessed=8 << 20
        ),
        name="recur_pre",
    )(held(in_x), held(in_y), held(state), held(edge), held(taps), held(gate_a), held(gate_x), held(rate))


def unpack(block, scratch):
    width = block.shape[2] - 128
    parts = []
    for g in range(block.shape[0] // group):
        own = block[g * group : (g + 1) * group]
        parts.append(own[:, :, 0:width].reshape(main_rows, width))
        tiles = own[:, :, width:].reshape(128, 128).astype(f32)
        parts.append(unpack_extras(tiles, scratch).astype(bf16))
    return jnp.concatenate(parts, axis=0)


def pack_into(out_ref, values, scratch):
    width = values.shape[1]
    for g in range(out_ref.shape[0] // group):
        lo = g * group_rows
        out_ref[g * group : (g + 1) * group, :, 0:width] = (
            values[lo : lo + main_rows].astype(bf16).reshape(group, main, width)
        )
        tiles = pack_extras(values[lo + main_rows : lo + group_rows], scratch)
        out_ref[g * group : (g + 1) * group, :, width:] = tiles.astype(bf16).reshape(
            group, main, 128
        )


def near_kernel(core_ref, block_ref, down_ref, part_ref, scratch):
    rows = unpack(block_ref[...], scratch)
    part_ref[...] = dot(rows, down_ref[...], inner)


def near(core, arrived, down):
    experts, _, wide = arrived.shape
    half = wide - 128
    hidden = down.shape[0]
    count = experts * (main + extra)
    size = pair * group_rows
    return pl.pallas_call(
        near_kernel,
        grid_spec=pltpu.PrefetchScalarGridSpec(
            num_scalar_prefetch=1,
            grid=(count // size,),
            in_specs=[
                pl.BlockSpec((pair * group, main, wide), lambda i, c: (i, 0, 0)),
                pl.BlockSpec((hidden, half), lambda i, c: (0, c[0])),
            ],
            out_specs=pl.BlockSpec((size, hidden), lambda i, c: (i, 0)),
            scratch_shapes=[pltpu.VMEM((128, 128), f32)],
        ),
        out_shape=jax.ShapeDtypeStruct((count, hidden), f32),
        compiler_params=params(),
        cost_estimate=pl.CostEstimate(
            flops=2 * count * half * hidden, transcendentals=0, bytes_accessed=9 << 20
        ),
        name="near",
    )(core, arrived, held(down))


def far_kernel(
    core_ref, block_ref, down_ref, part_ref, silu_ref, slope_ref, gate_ref, up_ref,
    gate_adj_ref, up_adj_ref, back_ref, scratch,
):
    rows = unpack(block_ref[...], scratch)
    grad = part_ref[...] + dot(rows, down_ref[...], inner)
    gate_adj = (grad * slope_ref[...]).astype(bf16)
    up_adj = (grad * silu_ref[...]).astype(bf16)
    gate_adj_ref[...] = gate_adj
    up_adj_ref[...] = up_adj
    back = dot(gate_adj, gate_ref[...], inner) + dot(up_adj, up_ref[...], inner)
    pack_into(back_ref, back, scratch)


def far(core, arrived, down, part, silu, slope, gate, up):
    experts, _, wide = arrived.shape
    half = wide - 128
    hidden = down.shape[0]
    count = experts * (main + extra)
    size = pair * group_rows
    by_row = lambda width: pl.BlockSpec((size, width), lambda i, c: (i, 0))
    block = pl.BlockSpec((pair * group, main, wide), lambda i, c: (i, 0, 0))
    weight = pl.BlockSpec((half, hidden), lambda i, c: (1 - c[0], 0))
    return pl.pallas_call(
        far_kernel,
        grid_spec=pltpu.PrefetchScalarGridSpec(
            num_scalar_prefetch=1,
            grid=(count // size,),
            in_specs=[
                block,
                pl.BlockSpec((hidden, half), lambda i, c: (0, 1 - c[0])),
                by_row(hidden),
                by_row(hidden),
                by_row(hidden),
                weight,
                weight,
            ],
            out_specs=[by_row(hidden), by_row(hidden), block],
            scratch_shapes=[pltpu.VMEM((128, 128), f32)],
        ),
        out_shape=[
            jax.ShapeDtypeStruct((count, hidden), bf16),
            jax.ShapeDtypeStruct((count, hidden), bf16),
            jax.ShapeDtypeStruct(arrived.shape, bf16),
        ],
        compiler_params=params(),
        cost_estimate=pl.CostEstimate(
            flops=6 * count * half * hidden, transcendentals=0, bytes_accessed=16 << 20
        ),
        name="far",
    )(core, arrived, held(down), part, silu, slope, held(gate), held(up))


def back_kernel(core_ref, gate_adj_ref, up_adj_ref, gate_ref, up_ref, back_ref, scratch):
    back = dot(gate_adj_ref[...], gate_ref[...], inner) + dot(up_adj_ref[...], up_ref[...], inner)
    pack_into(back_ref, back, scratch)


def back_own(core, gate_adj, up_adj, gate, up, shape):
    _, _, wide = shape
    half = wide - 128
    count, hidden = gate_adj.shape
    size = pair * group_rows
    by_row = lambda width: pl.BlockSpec((size, width), lambda i, c: (i, 0))
    weight = pl.BlockSpec((half, hidden), lambda i, c: (c[0], 0))
    return pl.pallas_call(
        back_kernel,
        grid_spec=pltpu.PrefetchScalarGridSpec(
            num_scalar_prefetch=1,
            grid=(count // size,),
            in_specs=[by_row(hidden), by_row(hidden), weight, weight],
            out_specs=pl.BlockSpec((pair * group, main, wide), lambda i, c: (i, 0, 0)),
            scratch_shapes=[pltpu.VMEM((128, 128), f32)],
        ),
        out_shape=jax.ShapeDtypeStruct(shape, bf16),
        compiler_params=params(),
        cost_estimate=pl.CostEstimate(
            flops=4 * count * half * hidden, transcendentals=0, bytes_accessed=7 << 20
        ),
        name="back_own",
    )(core, gate_adj, up_adj, held(gate), held(up))


def grad_in_kernel(packed_ref, gate_adj_ref, up_adj_ref, gate_ref, up_ref):
    packed = packed_ref[...]
    gate_ref[...] = dot(packed, gate_adj_ref[...], outer).astype(bf16)
    up_ref[...] = dot(packed, up_adj_ref[...], outer).astype(bf16)


def grad_in(packed, gate_adj, up_adj):
    count, model = packed.shape
    hidden = gate_adj.shape[1]
    size = 512
    out = pl.BlockSpec((size, hidden), lambda i: (i, 0))
    return pl.pallas_call(
        grad_in_kernel,
        grid=(model // size,),
        in_specs=[
            pl.BlockSpec((count, size), lambda i: (0, i)),
            whole((count, hidden)),
            whole((count, hidden)),
        ],
        out_specs=[out, out],
        out_shape=[jax.ShapeDtypeStruct((model, hidden), bf16)] * 2,
        compiler_params=params(),
        cost_estimate=pl.CostEstimate(
            flops=4 * count * model * hidden, transcendentals=0, bytes_accessed=11 << 20
        ),
        name="grad_in",
    )(held(packed), held(gate_adj), held(up_adj))


def grad_down_kernel(core_ref, active_ref, near_ref, far_ref, out_ref, scratch):
    active = active_ref[...]

    @pl.when(pl.program_id(0) == 0)
    def _():
        out_ref[...] = dot(active, unpack(near_ref[...], scratch), outer).astype(bf16)

    @pl.when(pl.program_id(0) == 1)
    def _():
        out_ref[...] = dot(active, unpack(far_ref[...], scratch), outer).astype(bf16)


def grad_down_of(core, active, arrived, arrived_far):
    count, hidden = active.shape
    half = arrived.shape[2] - 128
    return pl.pallas_call(
        grad_down_kernel,
        grid_spec=pltpu.PrefetchScalarGridSpec(
            num_scalar_prefetch=1,
            grid=(2,),
            in_specs=[whole((count, hidden)), whole(arrived.shape), whole(arrived.shape)],
            out_specs=pl.BlockSpec((hidden, half), lambda i, c: (0, i + c[0] - 2 * i * c[0])),
            scratch_shapes=[pltpu.VMEM((128, 128), f32)],
        ),
        out_shape=jax.ShapeDtypeStruct((hidden, 2 * half), bf16),
        compiler_params=params(),
        cost_estimate=pl.CostEstimate(
            flops=4 * count * half * hidden, transcendentals=0, bytes_accessed=9 << 20
        ),
        name="grad_down",
    )(core, held(active), held(arrived), held(arrived_far))


def combine_kernel(core_ref, block_ref, target_ref, cot_ref, out_ref, total, scratch):
    step = pl.program_id(0)
    tokens = cot_ref.shape[0]
    rows = unpack(block_ref[...], scratch)
    size = rows.shape[0]
    place = lax.broadcasted_iota(jnp.int32, (tokens, size), 1) + step * size
    chosen = jnp.where(
        (place == target_ref[:, 0:1]) | (place == target_ref[:, 1:2]), 1.0, 0.0
    ).astype(bf16)
    found = dot(chosen, rows, plain)

    @pl.when(step == 0)
    def _():
        total[...] = found

    @pl.when(step > 0)
    def _():
        total[...] = total[...] + found

    @pl.when(step == pl.num_programs(0) - 1)
    def _():
        out_ref[...] = (cot_ref[...].astype(f32) + total[...]).astype(bf16)


def combine(core, returned, target, cotangent):
    experts, _, wide = returned.shape
    half = wide - 128
    tokens = cotangent.shape[0]
    return pl.pallas_call(
        combine_kernel,
        grid_spec=pltpu.PrefetchScalarGridSpec(
            num_scalar_prefetch=1,
            grid=(experts // (pair * group),),
            in_specs=[
                pl.BlockSpec((pair * group, main, wide), lambda i, c: (i, 0, 0)),
                whole((tokens, 8)),
                pl.BlockSpec((tokens, half), lambda i, c: (0, c[0])),
            ],
            out_specs=whole((tokens, half)),
            scratch_shapes=[pltpu.VMEM((tokens, half), f32), pltpu.VMEM((128, 128), f32)],
        ),
        out_shape=jax.ShapeDtypeStruct((tokens, half), bf16),
        compiler_params=params(),
        name="combine",
    )(core, returned, held(target), held(cotangent))


def two_terms(value):
    high = value.astype(bf16)
    return high, (value - high.astype(f32)).astype(bf16)


def share_rows(values, owners):
    value = values.astype(bf16).reshape(owners, 2 * main, values.shape[1])
    return value[:, 0:main], value[:, main:]


def own_kernel(core_ref, own_ref, weight_ref, mixed_ref, grad_ref, share_ref):
    own = own_ref[...]
    grad_ref[...] = dot(own, weight_ref[...], plain)
    left, right = share_rows(dot(own, mixed_ref[...], outer), share_ref.shape[0])
    channels = left.shape[2]
    share_ref[:, :, 0:channels] = left
    share_ref[:, :, channels:] = right


def own_part(core, own, weight, mixed, owners):
    tokens, half = own.shape
    channels = mixed.shape[1]
    return pl.pallas_call(
        own_kernel,
        grid_spec=pltpu.PrefetchScalarGridSpec(
            num_scalar_prefetch=1,
            grid=(1,),
            in_specs=[
                whole((tokens, half)),
                pl.BlockSpec((half, channels), lambda i, c: (c[0], 0)),
                whole((tokens, channels)),
            ],
            out_specs=[whole((tokens, channels)), whole((owners // 2, main, 2 * channels))],
        ),
        out_shape=[
            jax.ShapeDtypeStruct((tokens, channels), f32),
            jax.ShapeDtypeStruct((owners // 2, main, 2 * channels), bf16),
        ],
        compiler_params=params(),
        cost_estimate=pl.CostEstimate(
            flops=4 * tokens * half * channels, transcendentals=0, bytes_accessed=4 << 20
        ),
        name="own_part",
    )(core, own, weight, mixed)


def scan_kernel(
    core_ref, peer_ref, weight_ref, mixed_ref, part_ref, share_ref, slope_ref, gelu_ref, ahead_ref,
    product_ref, first_ref,
    grad_y_out, local_out, share_out, head_out,
    state_grad, grad_y, local, peer_share, lines, head, sems,
):
    tokens, _ = peer_ref.shape
    channels = weight_ref.shape[1]
    core = core_ref[0]
    owners = share_ref.shape[0]
    own_at = pl.ds(pl.multiple_of(core * owners, owners), owners)
    peer_at = pl.ds(pl.multiple_of((1 - core) * owners, owners), owners)
    waits = []

    def copy_out(source, target):
        copy = pltpu.make_async_copy(source, target, sems.at[len(waits)])
        copy.start()
        waits.append(copy)

    copy_out(share_ref, share_out.at[own_at, :, pl.ds(0, 2 * channels)])
    peer = peer_ref[...]
    grad = part_ref[...] + dot(peer, weight_ref[...], plain)
    grad_y[...] = grad * slope_ref[...]
    copy_out(grad_y, grad_y_out)
    values = grad * gelu_ref[...]
    length = tokens // segments
    blocks = state_grad.shape[0]
    for b in range(blocks):
        state_grad[b] = values[:, 128 * b : 128 * (b + 1)]
    carries = []
    for b in range(blocks):
        at = slice(128 * b, 128 * (b + 1))
        value = None
        for j in reversed(range(length)):
            here = state_grad[b, pl.ds(j, segments, stride=length), :]
            if value is None:
                value = here
            else:
                value = here + ahead_ref[b, pl.ds(j, segments, stride=length), :] * value
            local[b, pl.ds(j, segments, stride=length), :] = value
        product = product_ref[b, pl.ds(0, segments, stride=length), :]
        carry = value[segments - 1 : segments]
        for s in reversed(range(1, segments - 1)):
            carry = value[s : s + 1] + product[s : s + 1] * carry
        ends = local[b, 0:3, :] + product_ref[b, 0:3, :] * carry
        carries.append(first_ref[0:1, at] * ends[0:1])
        head[:, at] = jnp.concatenate([ends, first_ref[3:15, at], jnp.zeros((1, 128), f32)], axis=0)
    decay = jnp.concatenate([first_ref[1:2, 128 * b : 128 * (b + 1)] for b in range(blocks)], axis=0)
    terms = two_terms(decay) + two_terms(jnp.concatenate(carries, axis=0))
    line = jnp.concatenate([term.astype(f32) for term in terms], axis=0).astype(bf16)
    lines[...] = jnp.broadcast_to(line[None], lines.shape)
    copy_out(lines, share_out.at[:, :, pl.ds(2 * channels, 128)])
    copy_out(local, local_out)
    copy_out(head, head_out)
    left, right = share_rows(dot(peer, mixed_ref[...], outer), owners)
    peer_share[:, :, 0:channels] = left
    peer_share[:, :, channels : 2 * channels] = right
    copy_out(peer_share, share_out.at[peer_at, :, pl.ds(0, 2 * channels)])
    for copy in waits:
        copy.wait()


def scan(core, peer, weight, mixed, part, share, slope, gelu, ahead, product, first):
    tokens, half = peer.shape
    channels = weight.shape[1]
    owners, rows, _ = share.shape
    out_shape = (2 * owners, rows, 2 * channels + 128)
    anywhere = pl.BlockSpec(memory_space=pl.ANY)
    return pl.pallas_call(
        scan_kernel,
        grid_spec=pltpu.PrefetchScalarGridSpec(
            num_scalar_prefetch=1,
            grid=(1,),
            in_specs=[
                whole((tokens, half)),
                pl.BlockSpec((half, channels), lambda i, c: (1 - c[0], 0)),
                whole((tokens, channels)),
                whole((tokens, channels)),
                whole(share.shape),
                whole((tokens, channels)),
                whole((tokens, channels)),
                whole(ahead.shape),
                whole(ahead.shape),
                whole((16, channels)),
            ],
            out_specs=[anywhere] * 4,
            scratch_shapes=[
                pltpu.VMEM(ahead.shape, f32),
                pltpu.VMEM((tokens, channels), f32),
                pltpu.VMEM(ahead.shape, f32),
                pltpu.VMEM(share.shape, bf16),
                pltpu.VMEM((2 * owners, rows, 128), bf16),
                pltpu.VMEM((16, channels), f32),
                pltpu.SemaphoreType.DMA((6,)),
            ],
        ),
        out_shape=[
            pltpu.HBM((tokens, channels), f32),
            pltpu.HBM(ahead.shape, f32),
            pltpu.HBM(out_shape, bf16),
            pltpu.HBM((16, channels), f32),
        ],
        compiler_params=params(),
        cost_estimate=pl.CostEstimate(
            flops=4 * tokens * half * channels, transcendentals=0, bytes_accessed=9 << 20
        ),
        name="scan",
    )(core, peer, weight, mixed, part, share, slope, gelu, ahead, product, first)


def tail_kernel(
    place_ref, line_ref, head_ref, local_ref, product_ref, keep_ref, input_ref, direct_ref,
    a_ref, i_ref, taps_ref, out_ref, carries, adjoint, grads,
):
    step = pl.program_id(0)
    tokens = local_ref.shape[1]
    length = tokens // segments
    place = place_ref[0]

    @pl.when(step == 0)
    def _():
        own = jnp.zeros((4, 128), f32)
        beyond = jnp.zeros((4, 128), f32)
        for j in reversed(range(line_ref.shape[0])):
            line = line_ref[j].astype(f32)
            decay = line[0:4] + line[4:8]
            total = line[8:12] + line[12:16]
            own = jnp.where(j > place, total + decay * own, own)
            beyond = jnp.where(j > place + 1, total + decay * beyond, beyond)
        carries[0:4, :] = own
        carries[4:8, :] = beyond

    def conv_grad(value, keep, gate, direct):
        keep = (value * keep).astype(bf16)
        gate = (value * gate).astype(bf16)
        return value * direct + dot(keep, a_ref[0], inner) + dot(gate, i_ref[0], inner)

    carry = carries[pl.ds(step, 1), :]
    for s in reversed(range(segments)):
        lo = s * length
        piece = local_ref[0, lo : lo + length, :] + product_ref[0, lo : lo + length, :] * carry
        adjoint[lo : lo + length, :] = piece
        carry = piece[0:1]
    grads[0:tokens, :] = conv_grad(adjoint[...], keep_ref[...], input_ref[...], direct_ref[...])
    head = head_ref[...]
    spare = jnp.zeros((5, 128), f32)
    three = lambda k: jnp.concatenate([head[3 * k : 3 * k + 3], spare], axis=0)
    later = three(0) + three(1) * carries[pl.ds(step + 4, 1), :]
    grads[tokens : tokens + 8, :] = conv_grad(later, three(2), three(3), three(4))
    total = taps_ref[0:1, :] * grads[3 : 3 + tokens, :]
    for j in range(1, 4):
        total = total + taps_ref[j : j + 1, :] * grads[3 - j : 3 - j + tokens, :]
    out_ref[...] = total


def tail(place, shares, head, local, product, keep, gate, direct, gate_a, gate_x, taps):
    blocks, tokens, span = local.shape
    channels = blocks * span
    owners, rows, _ = shares.shape
    cube = pl.BlockSpec((1, tokens, span), lambda i, c: (i, 0, 0))
    col = lambda rows: pl.BlockSpec((rows, span), lambda i, c: (0, i))
    block = pl.BlockSpec((1, span, span), lambda i, c: (i, 0, 0))
    line = pl.BlockSpec((owners, rows, 128), lambda i, c: (0, 0, 2 * channels // 128))
    return pl.pallas_call(
        tail_kernel,
        grid_spec=pltpu.PrefetchScalarGridSpec(
            num_scalar_prefetch=1,
            grid=(blocks,),
            in_specs=[line, col(16), cube, cube] + [col(tokens)] * 3 + [block, block, col(4)],
            out_specs=col(tokens),
            scratch_shapes=[
                pltpu.VMEM((8, span), f32),
                pltpu.VMEM((tokens, span), f32),
                pltpu.VMEM((tokens + 8, span), f32),
            ],
        ),
        out_shape=jax.ShapeDtypeStruct((tokens, channels), f32),
        compiler_params=params(),
        name="tail",
    )(place, shares, head, held(local), product, keep, gate, direct, held(gate_a), held(gate_x), held(taps))


def exchange(value, axis):
    return lax.all_to_all(value, axis, split_axis=0, concat_axis=0, tiled=True)


def swapped(value):
    return lax.ppermute(value, "tp", [(0, 1), (1, 0)])


def shifted(value, axis, by):
    devices = lax.axis_size(axis)
    pairs = [(i, i + by) for i in range(devices) if 0 <= i + by < devices]
    return lax.ppermute(value, axis, pairs)


def body(
    cotangent,
    routes,
    route_weight,
    expert_rows,
    gate_w,
    up_w,
    down_w,
    in_x,
    in_y,
    state,
    conv_taps,
    gate_a,
    gate_x,
    decay_rate,
    out_weight,
):
    tokens = cotangent.shape[0]
    experts = lax.axis_size("sp")
    core = lax.axis_index("tp").astype(jnp.int32).reshape(1)
    taps = conv_taps.shape[0]
    channels = in_x.shape[1]

    place = lax.axis_index("sp").astype(jnp.int32).reshape(1)

    edge = shifted(
        jnp.concatenate([in_x[tokens - taps + 1 :], state[tokens - 1 :]], axis=0), "sp", 1
    )
    outgoing, target = send(core, routes.T, route_weight.T, cotangent, experts)
    arrived = exchange(outgoing, "sp")
    target = target.T

    packed, silu, slope, active = expert_pre(expert_rows[0], gate_w[0], up_w[0])
    mixed, y_slope, gelu, ahead, product, keep_part, input_part, direct, first = recur_pre(
        in_x, in_y, state, edge, conv_taps, gate_a, gate_x, decay_rate[None]
    )

    arrived_far = swapped(arrived)
    part = near(core, arrived, down_w[0])
    gate_adj, up_adj, back_far = far(
        core, arrived_far, down_w[0], part, silu, slope, gate_w[0], up_w[0]
    )
    back_in = swapped(back_far)
    own = back_own(core, gate_adj, up_adj, gate_w[0], up_w[0], arrived.shape)
    returning = (own.astype(f32) + back_in.astype(f32)).astype(bf16)
    returned = exchange(returning, "sp")

    grad_gate, grad_up = grad_in(packed, gate_adj, up_adj)
    grad_down = grad_down_of(core, active, arrived, arrived_far)

    stream_own = combine(core, returned, target, cotangent)
    stream_peer = swapped(stream_own)
    part, share = own_part(core, stream_own, out_weight, mixed, experts)
    grad_y, local, outgoing, head = scan(
        core, stream_peer, out_weight, mixed, part, share, y_slope, gelu, ahead, product, first
    )
    head = shifted(head, "sp", -1)
    shares = exchange(outgoing, "sp")
    grad_x = tail(
        place, shares, head, local, product, keep_part, input_part, direct,
        gate_a, gate_x, conv_taps,
    )
    summed = jnp.sum(shares[:, :, : 2 * channels].astype(f32), axis=0)
    grad_proj = jnp.concatenate([summed[:, :channels], summed[:, channels:]], axis=0)
    return (grad_gate[None], grad_up[None], grad_down[None], grad_proj, grad_x, grad_y)


def solution(mesh):
    in_specs = (
        P("sp", None),
        P("sp", None),
        P("sp", None),
        P("sp", None, None),
        P("sp", None, "tp"),
        P("sp", None, "tp"),
        P("sp", "tp", None),
        P("sp", "tp"),
        P("sp", "tp"),
        P("sp", "tp"),
        P(None, "tp"),
        P("tp", None, None),
        P("tp", None, None),
        P("tp"),
        P(None, "tp"),
    )
    out_specs = (
        P("sp", None, "tp"),
        P("sp", None, "tp"),
        P("sp", "tp", None),
        P("sp", "tp"),
        P("sp", "tp"),
        P("sp", "tp"),
    )
    return jax.shard_map(body, mesh=mesh, in_specs=in_specs, out_specs=out_specs, check_vma=False)
```

```python
import jax
import jax.numpy as jnp
from jax import lax
from jax.experimental import pallas as pl
from jax.experimental.pallas import tpu as pltpu
from jax.sharding import PartitionSpec as P

rate_scale = 8.0
floor_square = 0.01
inv_root_two = 0.7071067811865476
inv_root_tau = 0.3989422804014327

f32 = jnp.float32
bf16 = jnp.bfloat16
inner = (((1,), (1,)), ((), ()))
outer = (((0,), (0,)), ((), ()))
plain = (((1,), (0,)), ((), ()))

group = 8
main = 16
extra = 2
main_rows = group * main
group_rows = group * (main + extra)
segments = 8


def dot(a, b, dims):
    return lax.dot_general(a, b, dims, preferred_element_type=f32)


def params(n=1, mb=32):
    return pltpu.CompilerParams(dimension_semantics=("arbitrary",) * n, vmem_limit_bytes=mb << 20)


def held(value):
    return pltpu.with_memory_space_constraint(value, pltpu.HBM)


def whole(shape):
    return pl.BlockSpec(shape, lambda *_: (0,) * len(shape))


def pack_extras(rows, scratch):
    for j in range(8):
        scratch[pl.ds(j, group * extra, stride=8), :] = rows[:, 128 * j : 128 * (j + 1)]
    return scratch[...]


def unpack_extras(tiles, scratch):
    scratch[...] = tiles
    return jnp.concatenate(
        [scratch[pl.ds(j, group * extra, stride=8), :] for j in range(8)], axis=1
    )


def send_kernel(core_ref, routes_ref, weight_ref, cot_ref, out_ref, target_ref, slot, scratch):
    step = pl.program_id(0)
    tokens = cot_ref.shape[0]
    experts = pl.num_programs(0) * group

    @pl.when(step == 0)
    def _():
        first = routes_ref[0:1, :]
        second = routes_ref[1:2, :]
        expert = lax.broadcasted_iota(jnp.int32, (experts, tokens), 0)
        hit_first = (expert == first).astype(f32)
        hit_second = (expert == second).astype(f32)
        earlier = (
            lax.broadcasted_iota(jnp.int32, (tokens, tokens), 0)
            < lax.broadcasted_iota(jnp.int32, (tokens, tokens), 1)
        ).astype(f32)
        before = dot((hit_first + hit_second).astype(bf16), earlier.astype(bf16), plain)
        place_first = jnp.sum(before * hit_first, axis=0, keepdims=True).astype(jnp.int32)
        place_second = jnp.sum(before * hit_second, axis=0, keepdims=True).astype(jnp.int32)
        place_second = place_second + (first == second).astype(jnp.int32)
        for k, (name, place) in enumerate(((first, place_first), (second, place_second))):
            base = group_rows * (name >> 3)
            inside = name & 7
            slot[k : k + 1, :] = base + jnp.where(
                place < main, main * inside + place, main_rows + extra * inside + place - main
            )
        target_ref[...] = jnp.concatenate(
            [slot[0:2, :], jnp.zeros((6, tokens), jnp.int32)], axis=0
        )

    rows = lax.broadcasted_iota(jnp.int32, (group_rows, tokens), 0) + step * group_rows
    hit_first = rows == slot[0:1, :]
    hit_second = rows == slot[1:2, :]
    chosen = jnp.where(hit_first | hit_second, 1.0, 0.0).astype(bf16)
    weight = jnp.sum(
        jnp.where(hit_first, weight_ref[0:1, :], 0.0)
        + jnp.where(hit_second, weight_ref[1:2, :], 0.0),
        axis=1,
        keepdims=True,
    )
    values = dot(chosen, cot_ref[...], plain) * weight
    width = values.shape[1]
    out_ref[:, :, 0:width] = values[0:main_rows].astype(bf16).reshape(group, main, width)
    tiles = pack_extras(values[main_rows:], scratch)
    out_ref[:, :, width:] = tiles.astype(bf16).reshape(group, main, 128)


def send(core, routes, weight, cotangent, experts):
    tokens, model = cotangent.shape
    half = model // 2
    return pl.pallas_call(
        send_kernel,
        grid_spec=pltpu.PrefetchScalarGridSpec(
            num_scalar_prefetch=1,
            grid=(experts // group,),
            in_specs=[
                whole((2, tokens)),
                whole((2, tokens)),
                pl.BlockSpec((tokens, half), lambda i, c: (0, c[0])),
            ],
            out_specs=[
                pl.BlockSpec((group, main, half + 128), lambda i, c: (i, 0, 0)),
                whole((8, tokens)),
            ],
            scratch_shapes=[pltpu.VMEM((8, tokens), jnp.int32), pltpu.VMEM((128, 128), f32)],
        ),
        out_shape=[
            pltpu.HBM((experts, main, half + 128), bf16),
            jax.ShapeDtypeStruct((8, tokens), jnp.int32),
        ],
        compiler_params=params(),
        name="send",
    )(core, held(routes), held(weight), held(cotangent))


pair = 2


def expert_pre_kernel(rows_ref, gate_ref, up_ref, packed_ref, silu_ref, slope_ref, active_ref):
    out_row = lax.broadcasted_iota(jnp.int32, (group_rows, group_rows), 0)
    column = lax.broadcasted_iota(jnp.int32, (group_rows, group_rows), 1)
    late = out_row - main_rows
    source = jnp.where(
        out_row < main_rows,
        (main + extra) * (out_row >> 4) + (out_row & 15),
        (main + extra) * (late >> 1) + main + (late & 1),
    )
    order = jnp.where(column == source, 1.0, 0.0).astype(bf16)
    for g in range(pair):
        lo = g * group_rows
        packed_ref[lo : lo + group_rows, :] = dot(
            order, rows_ref[lo : lo + group_rows, :], plain
        ).astype(bf16)
    packed = packed_ref[...]
    pre_gate = dot(packed, gate_ref[...], plain)
    pre_up = dot(packed, up_ref[...], plain)
    gate = jax.nn.sigmoid(pre_gate)
    silu = pre_gate * gate
    silu_ref[...] = silu
    slope_ref[...] = pre_up * gate * (1.0 + pre_gate * (1.0 - gate))
    active_ref[...] = (silu * pre_up).astype(bf16)


def expert_pre(rows, gate, up):
    count, model = rows.shape
    hidden = gate.shape[1]
    size = pair * group_rows
    by_row = lambda width: pl.BlockSpec((size, width), lambda i: (i, 0))
    return pl.pallas_call(
        expert_pre_kernel,
        grid=(count // size,),
        in_specs=[by_row(model), whole((model, hidden)), whole((model, hidden))],
        out_specs=[by_row(model), by_row(hidden), by_row(hidden), by_row(hidden)],
        out_shape=[
            pltpu.HBM((count, model), bf16),
            pltpu.HBM((count, hidden), f32),
            pltpu.HBM((count, hidden), f32),
            pltpu.HBM((count, hidden), bf16),
        ],
        compiler_params=params(),
        cost_estimate=pl.CostEstimate(
            flops=4 * count * model * hidden, transcendentals=0, bytes_accessed=20 << 20
        ),
        name="expert_pre",
    )(held(rows), held(gate), held(up))


def recur_pre_kernel(
    x_ref, y_ref, state_ref, edge_ref, taps_ref, a_ref, i_ref, rate_ref,
    mixed_ref, grad_y_ref, gelu_ref, ahead_ref, product_ref, keep_ref, input_ref, direct_ref,
    first_ref, scratch,
):
    tokens = x_ref.shape[0]
    x = x_ref[...].astype(f32)
    edge = edge_ref[...].astype(f32)
    scratch[5:8, :] = edge[0:3]
    scratch[8 : 8 + tokens, :] = x
    conv_x = taps_ref[0:1, :] * scratch[5 : 5 + tokens, :]
    for j in range(1, 4):
        conv_x = conv_x + taps_ref[j : j + 1, :] * scratch[5 + j : 5 + j + tokens, :]
    conv_b = conv_x.astype(bf16)
    keep = jax.nn.sigmoid(dot(conv_b, a_ref[0], plain))
    gate = jax.nn.sigmoid(dot(conv_b, i_ref[0], plain))
    rate = rate_ref[...]
    decay = jnp.exp(-rate_scale * keep * rate)
    norm = jnp.sqrt(1.0 - decay * decay + floor_square)
    state = state_ref[...].astype(f32)
    scratch[7:8, :] = edge[3:4]
    scratch[8 : 8 + tokens, :] = state
    state_prev = scratch[7 : 7 + tokens, :]
    log_part = decay * state_prev - conv_x * gate * decay * decay / norm
    keep_ref[...] = log_part * (-rate_scale * rate) * keep * (1.0 - keep)
    input_ref[...] = conv_x * norm * gate * (1.0 - gate)
    direct_ref[...] = gate * norm
    y = y_ref[...].astype(f32)
    below = 0.5 * (1.0 + lax.erf(y * inv_root_two))
    gelu = y * below
    gelu_ref[...] = gelu
    mixed_ref[...] = (state * gelu).astype(bf16)
    grad_y_ref[...] = state * (below + y * jnp.exp(-0.5 * y * y) * inv_root_tau)
    scratch[0:tokens, :] = decay
    scratch[tokens : tokens + 8, :] = jnp.ones((8, decay.shape[1]), f32)
    ahead_ref[0] = scratch[1 : 1 + tokens, :]
    length = tokens // segments
    product = None
    for j in reversed(range(length)):
        step = scratch[pl.ds(j + 1, segments, stride=length), :]
        product = step if product is None else step * product
        product_ref[0, pl.ds(j, segments, stride=length), :] = product
    rest = product[1:2]
    for s in range(2, segments):
        rest = rest * product[s : s + 1]
    total = decay[0:1] * product[0:1] * rest
    first_ref[...] = jnp.concatenate(
        [
            decay[0:1],
            total,
            jnp.zeros_like(total),
            product_ref[0, 0:3, :] * rest,
            keep_ref[0:3, :],
            input_ref[0:3, :],
            direct_ref[0:3, :],
            jnp.zeros_like(total),
        ],
        axis=0,
    )


def recur_pre(in_x, in_y, state, edge, taps, gate_a, gate_x, rate):
    tokens, channels = in_x.shape
    blocks, span = gate_a.shape[:2]
    col = lambda rows: pl.BlockSpec((rows, span), lambda i: (0, i))
    block = pl.BlockSpec((1, span, span), lambda i: (i, 0, 0))
    cube = pl.BlockSpec((1, tokens, span), lambda i: (i, 0, 0))
    big = pltpu.HBM((tokens, channels), f32)
    return pl.pallas_call(
        recur_pre_kernel,
        grid=(blocks,),
        in_specs=[col(tokens), col(tokens), col(tokens), col(4), col(4), block, block, col(1)],
        out_specs=[col(tokens)] * 3 + [cube] * 2 + [col(tokens)] * 3 + [col(16)],
        out_shape=[pltpu.HBM((tokens, channels), bf16)]
        + [big] * 2
        + [pltpu.HBM((blocks, tokens, span), f32)] * 2
        + [big] * 3
        + [pltpu.HBM((16, channels), f32)],
        scratch_shapes=[pltpu.VMEM((tokens + 16, span), f32)],
        compiler_params=params(),
        cost_estimate=pl.CostEstimate(
            flops=2000 * tokens * channels, transcendentals=0, bytes_accessed=8 << 20
        ),
        name="recur_pre",
    )(held(in_x), held(in_y), held(state), held(edge), held(taps), held(gate_a), held(gate_x), held(rate))


def unpack(block, scratch):
    width = block.shape[2] - 128
    parts = []
    for g in range(block.shape[0] // group):
        own = block[g * group : (g + 1) * group]
        parts.append(own[:, :, 0:width].reshape(main_rows, width))
        tiles = own[:, :, width:].reshape(128, 128).astype(f32)
        parts.append(unpack_extras(tiles, scratch).astype(bf16))
    return jnp.concatenate(parts, axis=0)


def pack_into(out_ref, values, scratch):
    width = values.shape[1]
    for g in range(out_ref.shape[0] // group):
        lo = g * group_rows
        out_ref[g * group : (g + 1) * group, :, 0:width] = (
            values[lo : lo + main_rows].astype(bf16).reshape(group, main, width)
        )
        tiles = pack_extras(values[lo + main_rows : lo + group_rows], scratch)
        out_ref[g * group : (g + 1) * group, :, width:] = tiles.astype(bf16).reshape(
            group, main, 128
        )


def near_by(value):
    return pltpu.with_memory_space_constraint(value, pltpu.VMEM)


def load_beside(copies):
    @pl.when(pl.program_id(0) == 0)
    def _():
        for copy in copies:
            copy.start()

    return copies


def finish(copies):
    @pl.when(pl.program_id(0) == pl.num_programs(0) - 1)
    def _():
        for copy in copies:
            copy.wait()


anywhere = pl.BlockSpec(memory_space=pl.ANY)


def near_kernel(core_ref, block_ref, down_ref, down_all, part_ref, down_next, scratch, sems):
    half = down_ref.shape[1]
    other = pl.multiple_of((1 - core_ref[0]) * half, half)
    copies = load_beside(
        [pltpu.make_async_copy(down_all.at[:, pl.ds(other, half)], down_next, sems.at[0])]
    )
    rows = unpack(block_ref[...], scratch)
    part_ref[...] = dot(rows, down_ref[...], inner)
    finish(copies)


def near(core, arrived, down):
    experts, _, wide = arrived.shape
    half = wide - 128
    hidden = down.shape[0]
    count = experts * (main + extra)
    size = pair * group_rows
    return pl.pallas_call(
        near_kernel,
        grid_spec=pltpu.PrefetchScalarGridSpec(
            num_scalar_prefetch=1,
            grid=(count // size,),
            in_specs=[
                pl.BlockSpec((pair * group, main, wide), lambda i, c: (i, 0, 0)),
                pl.BlockSpec((hidden, half), lambda i, c: (0, c[0])),
                anywhere,
            ],
            out_specs=[pl.BlockSpec((size, hidden), lambda i, c: (i, 0)), anywhere],
            scratch_shapes=[pltpu.VMEM((128, 128), f32), pltpu.SemaphoreType.DMA((1,))],
        ),
        out_shape=[
            jax.ShapeDtypeStruct((count, hidden), f32),
            pltpu.VMEM((hidden, half), bf16),
        ],
        compiler_params=params(),
        cost_estimate=pl.CostEstimate(
            flops=2 * count * half * hidden, transcendentals=0, bytes_accessed=9 << 20
        ),
        name="near",
    )(core, arrived, held(down), held(down))


def far_kernel(
    core_ref, block_ref, down_ref, part_ref, silu_ref, slope_ref, gate_all, up_all,
    adj_ref, gate_next, up_next, scratch, sems,
):
    half = gate_next.shape[0]
    own = pl.multiple_of(core_ref[0] * half, half)
    copies = load_beside(
        [
            pltpu.make_async_copy(gate_all.at[pl.ds(own, half)], gate_next, sems.at[0]),
            pltpu.make_async_copy(up_all.at[pl.ds(own, half)], up_next, sems.at[1]),
        ]
    )
    rows = unpack(block_ref[...], scratch)
    grad = part_ref[...] + dot(rows, down_ref[...], inner)
    hidden = grad.shape[1]
    adj_ref[:, 0:hidden] = (grad * slope_ref[...]).astype(bf16)
    adj_ref[:, hidden:] = (grad * silu_ref[...]).astype(bf16)
    finish(copies)


def far(core, arrived, down_half, part, silu, slope, gate, up):
    experts, _, wide = arrived.shape
    hidden, half = down_half.shape
    count = experts * (main + extra)
    size = pair * group_rows
    by_row = lambda width: pl.BlockSpec((size, width), lambda i, c: (i, 0))
    return pl.pallas_call(
        far_kernel,
        grid_spec=pltpu.PrefetchScalarGridSpec(
            num_scalar_prefetch=1,
            grid=(count // size,),
            in_specs=[
                pl.BlockSpec((pair * group, main, wide), lambda i, c: (i, 0, 0)),
                whole((hidden, half)),
                by_row(hidden),
                by_row(hidden),
                by_row(hidden),
                anywhere,
                anywhere,
            ],
            out_specs=[by_row(2 * hidden), anywhere, anywhere],
            scratch_shapes=[pltpu.VMEM((128, 128), f32), pltpu.SemaphoreType.DMA((2,))],
        ),
        out_shape=[
            jax.ShapeDtypeStruct((count, 2 * hidden), bf16),
            pltpu.VMEM((half, hidden), bf16),
            pltpu.VMEM((half, hidden), bf16),
        ],
        compiler_params=params(),
        cost_estimate=pl.CostEstimate(
            flops=2 * count * half * hidden, transcendentals=0, bytes_accessed=16 << 20
        ),
        name="far",
    )(core, arrived, near_by(down_half), part, silu, slope, held(gate), held(up))


def back_rows(adj, gate, up):
    hidden = gate.shape[1]
    back = dot(adj[:, 0:hidden], gate, inner) + dot(adj[:, hidden:], up, inner)
    return back.astype(bf16)


def back_own_kernel(
    core_ref, adj_ref, gate_ref, up_ref, gate_all, up_all, back_ref, gate_next, up_next, sems
):
    half = gate_next.shape[0]
    own = pl.multiple_of(core_ref[0] * half, half)
    copies = load_beside(
        [
            pltpu.make_async_copy(gate_all.at[pl.ds(own, half)], gate_next, sems.at[0]),
            pltpu.make_async_copy(up_all.at[pl.ds(own, half)], up_next, sems.at[1]),
        ]
    )
    back_ref[...] = back_rows(adj_ref[...], gate_ref[...], up_ref[...])
    finish(copies)


def back_own(core, adj, gate_half, up_half, gate_peer, up_peer):
    count = adj.shape[0]
    half, hidden = gate_half.shape
    size = pair * group_rows
    by_row = lambda width: pl.BlockSpec((size, width), lambda i, c: (i, 0))
    return pl.pallas_call(
        back_own_kernel,
        grid_spec=pltpu.PrefetchScalarGridSpec(
            num_scalar_prefetch=1,
            grid=(count // size,),
            in_specs=[
                by_row(2 * hidden),
                whole((half, hidden)),
                whole((half, hidden)),
                anywhere,
                anywhere,
            ],
            out_specs=[by_row(half), anywhere, anywhere],
            scratch_shapes=[pltpu.SemaphoreType.DMA((2,))],
        ),
        out_shape=[
            jax.ShapeDtypeStruct((count, half), bf16),
            pltpu.VMEM((half, hidden), bf16),
            pltpu.VMEM((half, hidden), bf16),
        ],
        compiler_params=params(),
        cost_estimate=pl.CostEstimate(
            flops=4 * count * half * hidden, transcendentals=0, bytes_accessed=7 << 20
        ),
        name="back_own",
    )(core, adj, near_by(gate_half), near_by(up_half), held(gate_peer), held(up_peer))


def back_sum_kernel(adj_ref, own_ref, gate_ref, up_ref, out_ref, scratch):
    peer = back_rows(adj_ref[...], gate_ref[...], up_ref[...])
    pack_into(out_ref, own_ref[...].astype(f32) + peer.astype(f32), scratch)


def back_sum(adj, own, gate_half, up_half, shape):
    count = adj.shape[0]
    half, hidden = gate_half.shape
    size = pair * group_rows
    by_row = lambda width: pl.BlockSpec((size, width), lambda i: (i, 0))
    return pl.pallas_call(
        back_sum_kernel,
        grid=(count // size,),
        in_specs=[by_row(2 * hidden), by_row(half), whole((half, hidden)), whole((half, hidden))],
        out_specs=pl.BlockSpec((pair * group, main, shape[2]), lambda i: (i, 0, 0)),
        scratch_shapes=[pltpu.VMEM((128, 128), f32)],
        out_shape=pltpu.HBM(shape, bf16),
        compiler_params=params(),
        cost_estimate=pl.CostEstimate(
            flops=4 * count * half * hidden, transcendentals=0, bytes_accessed=7 << 20
        ),
        name="back_sum",
    )(adj, own, near_by(gate_half), near_by(up_half))


def grad_in_kernel(packed_ref, adj_ref, gate_ref, up_ref):
    grad = dot(packed_ref[...], adj_ref[...], outer).astype(bf16)
    hidden = gate_ref.shape[1]
    gate_ref[...] = grad[:, 0:hidden]
    up_ref[...] = grad[:, hidden:]


def grad_in(packed, adj):
    count, model = packed.shape
    hidden = adj.shape[1] // 2
    size = 512
    out = pl.BlockSpec((size, hidden), lambda i: (i, 0))
    return pl.pallas_call(
        grad_in_kernel,
        grid=(model // size,),
        in_specs=[pl.BlockSpec((count, size), lambda i: (0, i)), whole((count, 2 * hidden))],
        out_specs=[out, out],
        out_shape=[jax.ShapeDtypeStruct((model, hidden), bf16)] * 2,
        compiler_params=params(),
        cost_estimate=pl.CostEstimate(
            flops=4 * count * model * hidden, transcendentals=0, bytes_accessed=11 << 20
        ),
        name="grad_in",
    )(held(packed), held(adj))


def grad_down_kernel(core_ref, active_ref, near_ref, far_ref, out_ref, scratch):
    active = active_ref[...]

    @pl.when(pl.program_id(0) == 0)
    def _():
        out_ref[...] = dot(active, unpack(near_ref[...], scratch), outer).astype(bf16)

    @pl.when(pl.program_id(0) == 1)
    def _():
        out_ref[...] = dot(active, unpack(far_ref[...], scratch), outer).astype(bf16)


def grad_down_of(core, active, arrived, arrived_far):
    count, hidden = active.shape
    half = arrived.shape[2] - 128
    return pl.pallas_call(
        grad_down_kernel,
        grid_spec=pltpu.PrefetchScalarGridSpec(
            num_scalar_prefetch=1,
            grid=(2,),
            in_specs=[whole((count, hidden)), whole(arrived.shape), whole(arrived.shape)],
            out_specs=pl.BlockSpec((hidden, half), lambda i, c: (0, i + c[0] - 2 * i * c[0])),
            scratch_shapes=[pltpu.VMEM((128, 128), f32)],
        ),
        out_shape=jax.ShapeDtypeStruct((hidden, 2 * half), bf16),
        compiler_params=params(),
        cost_estimate=pl.CostEstimate(
            flops=4 * count * half * hidden, transcendentals=0, bytes_accessed=9 << 20
        ),
        name="grad_down",
    )(core, held(active), held(arrived), held(arrived_far))


def combine_kernel(core_ref, block_ref, target_ref, cot_ref, out_ref, total, scratch):
    step = pl.program_id(0)
    tokens = cot_ref.shape[0]
    rows = unpack(block_ref[...], scratch)
    size = rows.shape[0]
    place = lax.broadcasted_iota(jnp.int32, (tokens, size), 1) + step * size
    chosen = jnp.where(
        (place == target_ref[:, 0:1]) | (place == target_ref[:, 1:2]), 1.0, 0.0
    ).astype(bf16)
    found = dot(chosen, rows, plain)

    @pl.when(step == 0)
    def _():
        total[...] = found

    @pl.when(step > 0)
    def _():
        total[...] = total[...] + found

    @pl.when(step == pl.num_programs(0) - 1)
    def _():
        out_ref[...] = (cot_ref[...].astype(f32) + total[...]).astype(bf16)


def combine(core, returned, target, cotangent):
    experts, _, wide = returned.shape
    half = wide - 128
    tokens = cotangent.shape[0]
    return pl.pallas_call(
        combine_kernel,
        grid_spec=pltpu.PrefetchScalarGridSpec(
            num_scalar_prefetch=1,
            grid=(experts // (pair * group),),
            in_specs=[
                pl.BlockSpec((pair * group, main, wide), lambda i, c: (i, 0, 0)),
                whole((tokens, 8)),
                pl.BlockSpec((tokens, half), lambda i, c: (0, c[0])),
            ],
            out_specs=whole((tokens, half)),
            scratch_shapes=[pltpu.VMEM((tokens, half), f32), pltpu.VMEM((128, 128), f32)],
        ),
        out_shape=jax.ShapeDtypeStruct((tokens, half), bf16),
        compiler_params=params(),
        name="combine",
    )(core, returned, held(target), held(cotangent))


def two_terms(value):
    high = value.astype(bf16)
    return high, (value - high.astype(f32)).astype(bf16)


def share_rows(values, owners):
    value = values.astype(bf16).reshape(owners, 2 * main, values.shape[1])
    return value[:, 0:main], value[:, main:]


def own_kernel(core_ref, own_ref, weight_ref, mixed_ref, grad_ref, share_ref):
    own = own_ref[...]
    grad_ref[...] = dot(own, weight_ref[...], plain)
    left, right = share_rows(dot(own, mixed_ref[...], outer), share_ref.shape[0])
    channels = left.shape[2]
    share_ref[:, :, 0:channels] = left
    share_ref[:, :, channels:] = right


def own_part(core, own, weight, mixed, owners):
    tokens, half = own.shape
    channels = mixed.shape[1]
    return pl.pallas_call(
        own_kernel,
        grid_spec=pltpu.PrefetchScalarGridSpec(
            num_scalar_prefetch=1,
            grid=(1,),
            in_specs=[
                whole((tokens, half)),
                pl.BlockSpec((half, channels), lambda i, c: (c[0], 0)),
                whole((tokens, channels)),
            ],
            out_specs=[whole((tokens, channels)), whole((owners // 2, main, 2 * channels))],
        ),
        out_shape=[
            jax.ShapeDtypeStruct((tokens, channels), f32),
            jax.ShapeDtypeStruct((owners // 2, main, 2 * channels), bf16),
        ],
        compiler_params=params(),
        cost_estimate=pl.CostEstimate(
            flops=4 * tokens * half * channels, transcendentals=0, bytes_accessed=4 << 20
        ),
        name="own_part",
    )(core, own, weight, mixed)


def scan_kernel(
    core_ref, peer_ref, weight_ref, mixed_ref, part_ref, share_ref, slope_ref, gelu_ref, ahead_ref,
    product_ref, first_ref,
    grad_y_out, local_out, share_out, head_out,
    state_grad, grad_y, local, peer_share, lines, head, sems,
):
    tokens, _ = peer_ref.shape
    channels = weight_ref.shape[1]
    core = core_ref[0]
    owners = share_ref.shape[0]
    own_at = pl.ds(pl.multiple_of(core * owners, owners), owners)
    peer_at = pl.ds(pl.multiple_of((1 - core) * owners, owners), owners)
    waits = []

    def copy_out(source, target):
        copy = pltpu.make_async_copy(source, target, sems.at[len(waits)])
        copy.start()
        waits.append(copy)

    copy_out(share_ref, share_out.at[own_at, :, pl.ds(0, 2 * channels)])
    peer = peer_ref[...]
    grad = part_ref[...] + dot(peer, weight_ref[...], plain)
    grad_y[...] = grad * slope_ref[...]
    copy_out(grad_y, grad_y_out)
    values = grad * gelu_ref[...]
    length = tokens // segments
    blocks = state_grad.shape[0]
    for b in range(blocks):
        state_grad[b] = values[:, 128 * b : 128 * (b + 1)]
    carries = []
    for b in range(blocks):
        at = slice(128 * b, 128 * (b + 1))
        value = None
        for j in reversed(range(length)):
            here = state_grad[b, pl.ds(j, segments, stride=length), :]
            if value is None:
                value = here
            else:
                value = here + ahead_ref[b, pl.ds(j, segments, stride=length), :] * value
            local[b, pl.ds(j, segments, stride=length), :] = value
        product = product_ref[b, pl.ds(0, segments, stride=length), :]
        carry = value[segments - 1 : segments]
        for s in reversed(range(1, segments - 1)):
            carry = value[s : s + 1] + product[s : s + 1] * carry
        ends = local[b, 0:3, :] + product_ref[b, 0:3, :] * carry
        carries.append(first_ref[0:1, at] * ends[0:1])
        head[:, at] = jnp.concatenate([ends, first_ref[3:15, at], jnp.zeros((1, 128), f32)], axis=0)
    decay = jnp.concatenate([first_ref[1:2, 128 * b : 128 * (b + 1)] for b in range(blocks)], axis=0)
    terms = two_terms(decay) + two_terms(jnp.concatenate(carries, axis=0))
    line = jnp.concatenate([term.astype(f32) for term in terms], axis=0).astype(bf16)
    lines[...] = jnp.broadcast_to(line[None], lines.shape)
    copy_out(lines, share_out.at[:, :, pl.ds(2 * channels, 128)])
    copy_out(local, local_out)
    copy_out(head, head_out)
    left, right = share_rows(dot(peer, mixed_ref[...], outer), owners)
    peer_share[:, :, 0:channels] = left
    peer_share[:, :, channels : 2 * channels] = right
    copy_out(peer_share, share_out.at[peer_at, :, pl.ds(0, 2 * channels)])
    for copy in waits:
        copy.wait()


def scan(core, peer, weight, mixed, part, share, slope, gelu, ahead, product, first):
    tokens, half = peer.shape
    channels = weight.shape[1]
    owners, rows, _ = share.shape
    out_shape = (2 * owners, rows, 2 * channels + 128)
    return pl.pallas_call(
        scan_kernel,
        grid_spec=pltpu.PrefetchScalarGridSpec(
            num_scalar_prefetch=1,
            grid=(1,),
            in_specs=[
                whole((tokens, half)),
                pl.BlockSpec((half, channels), lambda i, c: (1 - c[0], 0)),
                whole((tokens, channels)),
                whole((tokens, channels)),
                whole(share.shape),
                whole((tokens, channels)),
                whole((tokens, channels)),
                whole(ahead.shape),
                whole(ahead.shape),
                whole((16, channels)),
            ],
            out_specs=[anywhere] * 4,
            scratch_shapes=[
                pltpu.VMEM(ahead.shape, f32),
                pltpu.VMEM((tokens, channels), f32),
                pltpu.VMEM(ahead.shape, f32),
                pltpu.VMEM(share.shape, bf16),
                pltpu.VMEM((2 * owners, rows, 128), bf16),
                pltpu.VMEM((16, channels), f32),
                pltpu.SemaphoreType.DMA((6,)),
            ],
        ),
        out_shape=[
            pltpu.HBM((tokens, channels), f32),
            pltpu.HBM(ahead.shape, f32),
            pltpu.HBM(out_shape, bf16),
            pltpu.HBM((16, channels), f32),
        ],
        compiler_params=params(),
        cost_estimate=pl.CostEstimate(
            flops=4 * tokens * half * channels, transcendentals=0, bytes_accessed=9 << 20
        ),
        name="scan",
    )(core, peer, weight, mixed, part, share, slope, gelu, ahead, product, first)


def tail_kernel(
    place_ref, line_ref, head_ref, local_ref, product_ref, keep_ref, input_ref, direct_ref,
    a_ref, i_ref, taps_ref, out_ref, carries, adjoint, grads,
):
    step = pl.program_id(0)
    tokens = local_ref.shape[1]
    length = tokens // segments
    place = place_ref[0]

    @pl.when(step == 0)
    def _():
        own = jnp.zeros((4, 128), f32)
        beyond = jnp.zeros((4, 128), f32)
        for j in reversed(range(line_ref.shape[0])):
            line = line_ref[j].astype(f32)
            decay = line[0:4] + line[4:8]
            total = line[8:12] + line[12:16]
            own = jnp.where(j > place, total + decay * own, own)
            beyond = jnp.where(j > place + 1, total + decay * beyond, beyond)
        carries[0:4, :] = own
        carries[4:8, :] = beyond

    def conv_grad(value, keep, gate, direct):
        keep = (value * keep).astype(bf16)
        gate = (value * gate).astype(bf16)
        return value * direct + dot(keep, a_ref[0], inner) + dot(gate, i_ref[0], inner)

    carry = carries[pl.ds(step, 1), :]
    for s in reversed(range(segments)):
        lo = s * length
        piece = local_ref[0, lo : lo + length, :] + product_ref[0, lo : lo + length, :] * carry
        adjoint[lo : lo + length, :] = piece
        carry = piece[0:1]
    grads[0:tokens, :] = conv_grad(adjoint[...], keep_ref[...], input_ref[...], direct_ref[...])
    head = head_ref[...]
    spare = jnp.zeros((5, 128), f32)
    three = lambda k: jnp.concatenate([head[3 * k : 3 * k + 3], spare], axis=0)
    later = three(0) + three(1) * carries[pl.ds(step + 4, 1), :]
    grads[tokens : tokens + 8, :] = conv_grad(later, three(2), three(3), three(4))
    total = taps_ref[0:1, :] * grads[3 : 3 + tokens, :]
    for j in range(1, 4):
        total = total + taps_ref[j : j + 1, :] * grads[3 - j : 3 - j + tokens, :]
    out_ref[...] = total


def tail(place, shares, head, local, product, keep, gate, direct, gate_a, gate_x, taps):
    blocks, tokens, span = local.shape
    channels = blocks * span
    owners, rows, _ = shares.shape
    cube = pl.BlockSpec((1, tokens, span), lambda i, c: (i, 0, 0))
    col = lambda rows: pl.BlockSpec((rows, span), lambda i, c: (0, i))
    block = pl.BlockSpec((1, span, span), lambda i, c: (i, 0, 0))
    line = pl.BlockSpec((owners, rows, 128), lambda i, c: (0, 0, 2 * channels // 128))
    return pl.pallas_call(
        tail_kernel,
        grid_spec=pltpu.PrefetchScalarGridSpec(
            num_scalar_prefetch=1,
            grid=(blocks,),
            in_specs=[line, col(16), cube, cube] + [col(tokens)] * 3 + [block, block, col(4)],
            out_specs=col(tokens),
            scratch_shapes=[
                pltpu.VMEM((8, span), f32),
                pltpu.VMEM((tokens, span), f32),
                pltpu.VMEM((tokens + 8, span), f32),
            ],
        ),
        out_shape=jax.ShapeDtypeStruct((tokens, channels), f32),
        compiler_params=params(),
        name="tail",
    )(place, shares, head, held(local), product, keep, gate, direct, held(gate_a), held(gate_x), held(taps))


def exchange(value, axis):
    return lax.all_to_all(value, axis, split_axis=0, concat_axis=0, tiled=True)


def swapped(value):
    return lax.ppermute(value, "tp", [(0, 1), (1, 0)])


def shifted(value, axis, by):
    devices = lax.axis_size(axis)
    pairs = [(i, i + by) for i in range(devices) if 0 <= i + by < devices]
    return lax.ppermute(value, axis, pairs)


def body(
    cotangent,
    routes,
    route_weight,
    expert_rows,
    gate_w,
    up_w,
    down_w,
    in_x,
    in_y,
    state,
    conv_taps,
    gate_a,
    gate_x,
    decay_rate,
    out_weight,
):
    tokens = cotangent.shape[0]
    experts = lax.axis_size("sp")
    core = lax.axis_index("tp").astype(jnp.int32).reshape(1)
    taps = conv_taps.shape[0]
    channels = in_x.shape[1]

    place = lax.axis_index("sp").astype(jnp.int32).reshape(1)

    edge = shifted(
        jnp.concatenate([in_x[tokens - taps + 1 :], state[tokens - 1 :]], axis=0), "sp", 1
    )
    outgoing, target = send(core, routes.T, route_weight.T, cotangent, experts)
    arrived = exchange(outgoing, "sp")
    target = target.T

    gate_peer = swapped(gate_w[0])
    up_peer = swapped(up_w[0])
    packed, silu, slope, active = expert_pre(expert_rows[0], gate_w[0], up_w[0])
    mixed, y_slope, gelu, ahead, product, keep_part, input_part, direct, first = recur_pre(
        in_x, in_y, state, edge, conv_taps, gate_a, gate_x, decay_rate[None]
    )

    arrived_far = swapped(arrived)
    part, down_half = near(core, arrived, down_w[0])
    adj, gate_half, up_half = far(
        core, arrived_far, down_half, part, silu, slope, gate_w[0], up_w[0]
    )
    adj_peer = swapped(adj)
    own, gate_half, up_half = back_own(core, adj, gate_half, up_half, gate_peer, up_peer)
    returning = back_sum(adj_peer, own, gate_half, up_half, arrived.shape)
    returned = exchange(returning, "sp")

    grad_gate, grad_up = grad_in(packed, adj)
    grad_down = grad_down_of(core, active, arrived, arrived_far)

    stream_own = combine(core, returned, target, cotangent)
    stream_peer = swapped(stream_own)
    part, share = own_part(core, stream_own, out_weight, mixed, experts)
    grad_y, local, outgoing, head = scan(
        core, stream_peer, out_weight, mixed, part, share, y_slope, gelu, ahead, product, first
    )
    head = shifted(head, "sp", -1)
    shares = exchange(outgoing, "sp")
    grad_x = tail(
        place, shares, head, local, product, keep_part, input_part, direct,
        gate_a, gate_x, conv_taps,
    )
    summed = jnp.sum(shares[:, :, : 2 * channels].astype(f32), axis=0)
    grad_proj = jnp.concatenate([summed[:, :channels], summed[:, channels:]], axis=0)
    return (grad_gate[None], grad_up[None], grad_down[None], grad_proj, grad_x, grad_y)


def solution(mesh):
    in_specs = (
        P("sp", None),
        P("sp", None),
        P("sp", None),
        P("sp", None, None),
        P("sp", None, "tp"),
        P("sp", None, "tp"),
        P("sp", "tp", None),
        P("sp", "tp"),
        P("sp", "tp"),
        P("sp", "tp"),
        P(None, "tp"),
        P("tp", None, None),
        P("tp", None, None),
        P("tp"),
        P(None, "tp"),
    )
    out_specs = (
        P("sp", None, "tp"),
        P("sp", None, "tp"),
        P("sp", "tp", None),
        P("sp", "tp"),
        P("sp", "tp"),
        P("sp", "tp"),
    )
    return jax.shard_map(body, mesh=mesh, in_specs=in_specs, out_specs=out_specs, check_vma=False)
```

```python
import jax
import jax.numpy as jnp
from jax import lax
from jax.experimental import pallas as pl
from jax.experimental.pallas import tpu as pltpu
from jax.sharding import PartitionSpec as P

rate_scale = 8.0
floor_square = 0.01
inv_root_two = 0.7071067811865476
inv_root_tau = 0.3989422804014327

f32 = jnp.float32
bf16 = jnp.bfloat16
inner = (((1,), (1,)), ((), ()))
outer = (((0,), (0,)), ((), ()))
plain = (((1,), (0,)), ((), ()))

group = 8
main = 16
extra = 2
main_rows = group * main
group_rows = group * (main + extra)
segments = 8


def dot(a, b, dims):
    return lax.dot_general(a, b, dims, preferred_element_type=f32)


def params(n=1, mb=32):
    return pltpu.CompilerParams(dimension_semantics=("arbitrary",) * n, vmem_limit_bytes=mb << 20)


def held(value):
    return pltpu.with_memory_space_constraint(value, pltpu.HBM)


def whole(shape):
    return pl.BlockSpec(shape, lambda *_: (0,) * len(shape))


def pack_extras(rows, scratch):
    for j in range(8):
        scratch[pl.ds(j, group * extra, stride=8), :] = rows[:, 128 * j : 128 * (j + 1)]
    return scratch[...]


def unpack_extras(tiles, scratch):
    scratch[...] = tiles
    return jnp.concatenate(
        [scratch[pl.ds(j, group * extra, stride=8), :] for j in range(8)], axis=1
    )


def send_kernel(core_ref, routes_ref, weight_ref, cot_ref, out_ref, target_ref, slot, scratch):
    step = pl.program_id(0)
    tokens = cot_ref.shape[0]
    experts = pl.num_programs(0) * out_ref.shape[0]

    @pl.when(step == 0)
    def _():
        first = routes_ref[0:1, :]
        second = routes_ref[1:2, :]
        expert = lax.broadcasted_iota(jnp.int32, (experts, tokens), 0)
        hit_first = (expert == first).astype(f32)
        hit_second = (expert == second).astype(f32)
        earlier = (
            lax.broadcasted_iota(jnp.int32, (tokens, tokens), 0)
            < lax.broadcasted_iota(jnp.int32, (tokens, tokens), 1)
        ).astype(f32)
        before = dot((hit_first + hit_second).astype(bf16), earlier.astype(bf16), plain)
        place_first = jnp.sum(before * hit_first, axis=0, keepdims=True).astype(jnp.int32)
        place_second = jnp.sum(before * hit_second, axis=0, keepdims=True).astype(jnp.int32)
        place_second = place_second + (first == second).astype(jnp.int32)
        for k, (name, place) in enumerate(((first, place_first), (second, place_second))):
            base = group_rows * (name >> 3)
            inside = name & 7
            slot[k : k + 1, :] = base + jnp.where(
                place < main, main * inside + place, main_rows + extra * inside + place - main
            )
        target_ref[...] = jnp.concatenate(
            [slot[0:2, :], jnp.zeros((6, tokens), jnp.int32)], axis=0
        )

    size = out_ref.shape[0] // group * group_rows
    rows = lax.broadcasted_iota(jnp.int32, (size, tokens), 0) + step * size
    hit_first = rows == slot[0:1, :]
    hit_second = rows == slot[1:2, :]
    chosen = jnp.where(hit_first | hit_second, 1.0, 0.0).astype(bf16)
    weight = jnp.sum(
        jnp.where(hit_first, weight_ref[0:1, :], 0.0)
        + jnp.where(hit_second, weight_ref[1:2, :], 0.0),
        axis=1,
        keepdims=True,
    )
    values = dot(chosen, cot_ref[...], plain) * weight
    pack_into(out_ref, values, scratch)


def send(core, routes, weight, cotangent, experts):
    tokens, model = cotangent.shape
    half = model // 2
    return pl.pallas_call(
        send_kernel,
        grid_spec=pltpu.PrefetchScalarGridSpec(
            num_scalar_prefetch=1,
            grid=(experts // (send_groups * group),),
            in_specs=[
                whole((2, tokens)),
                whole((2, tokens)),
                pl.BlockSpec((tokens, half), lambda i, c: (0, c[0])),
            ],
            out_specs=[
                pl.BlockSpec((send_groups * group, main, half + 128), lambda i, c: (i, 0, 0)),
                whole((8, tokens)),
            ],
            scratch_shapes=[pltpu.VMEM((8, tokens), jnp.int32), pltpu.VMEM((128, 128), f32)],
        ),
        out_shape=[
            pltpu.HBM((experts, main, half + 128), bf16),
            jax.ShapeDtypeStruct((8, tokens), jnp.int32),
        ],
        compiler_params=params(),
        name="send",
    )(core, held(routes), held(weight), held(cotangent))


pair = 2
send_groups = 4
all_groups = 8
sum_groups = 4


def expert_pre_kernel(rows_ref, gate_ref, up_ref, packed_ref, silu_ref, slope_ref, active_ref):
    out_row = lax.broadcasted_iota(jnp.int32, (group_rows, group_rows), 0)
    column = lax.broadcasted_iota(jnp.int32, (group_rows, group_rows), 1)
    late = out_row - main_rows
    source = jnp.where(
        out_row < main_rows,
        (main + extra) * (out_row >> 4) + (out_row & 15),
        (main + extra) * (late >> 1) + main + (late & 1),
    )
    order = jnp.where(column == source, 1.0, 0.0).astype(bf16)
    for g in range(pair):
        lo = g * group_rows
        packed_ref[lo : lo + group_rows, :] = dot(
            order, rows_ref[lo : lo + group_rows, :], plain
        ).astype(bf16)
    packed = packed_ref[...]
    pre_gate = dot(packed, gate_ref[...], plain)
    pre_up = dot(packed, up_ref[...], plain)
    gate = jax.nn.sigmoid(pre_gate)
    silu = pre_gate * gate
    silu_ref[...] = silu
    slope_ref[...] = pre_up * gate * (1.0 + pre_gate * (1.0 - gate))
    active_ref[...] = (silu * pre_up).astype(bf16)


def expert_pre(rows, gate, up):
    count, model = rows.shape
    hidden = gate.shape[1]
    size = pair * group_rows
    by_row = lambda width: pl.BlockSpec((size, width), lambda i: (i, 0))
    return pl.pallas_call(
        expert_pre_kernel,
        grid=(count // size,),
        in_specs=[by_row(model), whole((model, hidden)), whole((model, hidden))],
        out_specs=[by_row(model), by_row(hidden), by_row(hidden), by_row(hidden)],
        out_shape=[
            pltpu.HBM((count, model), bf16),
            pltpu.HBM((count, hidden), f32),
            pltpu.HBM((count, hidden), f32),
            pltpu.HBM((count, hidden), bf16),
        ],
        compiler_params=params(),
        cost_estimate=pl.CostEstimate(
            flops=4 * count * model * hidden, transcendentals=0, bytes_accessed=20 << 20
        ),
        name="expert_pre",
    )(held(rows), held(gate), held(up))


def recur_pre_kernel(
    x_ref, y_ref, state_ref, edge_ref, taps_ref, a_ref, i_ref, rate_ref,
    mixed_ref, grad_y_ref, gelu_ref, ahead_ref, product_ref, keep_ref, input_ref, direct_ref,
    first_ref, scratch,
):
    tokens = x_ref.shape[0]
    x = x_ref[...].astype(f32)
    edge = edge_ref[...].astype(f32)
    scratch[5:8, :] = edge[0:3]
    scratch[8 : 8 + tokens, :] = x
    conv_x = taps_ref[0:1, :] * scratch[5 : 5 + tokens, :]
    for j in range(1, 4):
        conv_x = conv_x + taps_ref[j : j + 1, :] * scratch[5 + j : 5 + j + tokens, :]
    conv_b = conv_x.astype(bf16)
    keep = jax.nn.sigmoid(dot(conv_b, a_ref[0], plain))
    gate = jax.nn.sigmoid(dot(conv_b, i_ref[0], plain))
    rate = rate_ref[...]
    decay = jnp.exp(-rate_scale * keep * rate)
    norm = jnp.sqrt(1.0 - decay * decay + floor_square)
    state = state_ref[...].astype(f32)
    scratch[7:8, :] = edge[3:4]
    scratch[8 : 8 + tokens, :] = state
    state_prev = scratch[7 : 7 + tokens, :]
    log_part = decay * state_prev - conv_x * gate * decay * decay / norm
    keep_ref[...] = log_part * (-rate_scale * rate) * keep * (1.0 - keep)
    input_ref[...] = conv_x * norm * gate * (1.0 - gate)
    direct_ref[...] = gate * norm
    y = y_ref[...].astype(f32)
    below = 0.5 * (1.0 + lax.erf(y * inv_root_two))
    gelu = y * below
    gelu_ref[...] = gelu
    mixed_ref[...] = (state * gelu).astype(bf16)
    grad_y_ref[...] = state * (below + y * jnp.exp(-0.5 * y * y) * inv_root_tau)
    scratch[0:tokens, :] = decay
    scratch[tokens : tokens + 8, :] = jnp.ones((8, decay.shape[1]), f32)
    ahead_ref[0] = scratch[1 : 1 + tokens, :]
    length = tokens // segments
    product = None
    for j in reversed(range(length)):
        step = scratch[pl.ds(j + 1, segments, stride=length), :]
        product = step if product is None else step * product
        product_ref[0, pl.ds(j, segments, stride=length), :] = product
    rest = product[1:2]
    for s in range(2, segments):
        rest = rest * product[s : s + 1]
    total = decay[0:1] * product[0:1] * rest
    first_ref[...] = jnp.concatenate(
        [
            decay[0:1],
            total,
            jnp.zeros_like(total),
            product_ref[0, 0:3, :] * rest,
            keep_ref[0:3, :],
            input_ref[0:3, :],
            direct_ref[0:3, :],
            jnp.zeros_like(total),
        ],
        axis=0,
    )


def recur_pre(in_x, in_y, state, edge, taps, gate_a, gate_x, rate):
    tokens, channels = in_x.shape
    blocks, span = gate_a.shape[:2]
    col = lambda rows: pl.BlockSpec((rows, span), lambda i: (0, i))
    block = pl.BlockSpec((1, span, span), lambda i: (i, 0, 0))
    cube = pl.BlockSpec((1, tokens, span), lambda i: (i, 0, 0))
    big = pltpu.HBM((tokens, channels), f32)
    return pl.pallas_call(
        recur_pre_kernel,
        grid=(blocks,),
        in_specs=[col(tokens), col(tokens), col(tokens), col(4), col(4), block, block, col(1)],
        out_specs=[col(tokens)] * 3 + [cube] * 2 + [col(tokens)] * 3 + [col(16)],
        out_shape=[pltpu.HBM((tokens, channels), bf16)]
        + [big] * 2
        + [pltpu.HBM((blocks, tokens, span), f32)] * 2
        + [big] * 3
        + [pltpu.HBM((16, channels), f32)],
        scratch_shapes=[pltpu.VMEM((tokens + 16, span), f32)],
        compiler_params=params(),
        cost_estimate=pl.CostEstimate(
            flops=2000 * tokens * channels, transcendentals=0, bytes_accessed=8 << 20
        ),
        name="recur_pre",
    )(held(in_x), held(in_y), held(state), held(edge), held(taps), held(gate_a), held(gate_x), held(rate))


def unpack(block, scratch):
    width = block.shape[2] - 128
    parts = []
    for g in range(block.shape[0] // group):
        own = block[g * group : (g + 1) * group]
        parts.append(own[:, :, 0:width].reshape(main_rows, width))
        tiles = own[:, :, width:].reshape(128, 128).astype(f32)
        parts.append(unpack_extras(tiles, scratch).astype(bf16))
    return jnp.concatenate(parts, axis=0)


def pack_into(out_ref, values, scratch):
    width = values.shape[1]
    for g in range(out_ref.shape[0] // group):
        lo = g * group_rows
        out_ref[g * group : (g + 1) * group, :, 0:width] = (
            values[lo : lo + main_rows].astype(bf16).reshape(group, main, width)
        )
        tiles = pack_extras(values[lo + main_rows : lo + group_rows], scratch)
        out_ref[g * group : (g + 1) * group, :, width:] = tiles.astype(bf16).reshape(
            group, main, 128
        )


def near_by(value):
    return pltpu.with_memory_space_constraint(value, pltpu.VMEM)


def load_beside(copies):
    @pl.when(pl.program_id(0) == 0)
    def _():
        for copy in copies:
            copy.start()

    return copies


def finish(copies):
    @pl.when(pl.program_id(0) == pl.num_programs(0) - 1)
    def _():
        for copy in copies:
            copy.wait()


anywhere = pl.BlockSpec(memory_space=pl.ANY)


def near_kernel(core_ref, block_ref, down_ref, down_all, part_ref, down_next, scratch, sems):
    half = down_ref.shape[1]
    other = pl.multiple_of((1 - core_ref[0]) * half, half)
    copies = load_beside(
        [pltpu.make_async_copy(down_all.at[:, pl.ds(other, half)], down_next, sems.at[0])]
    )
    rows = unpack(block_ref[...], scratch)
    part_ref[...] = dot(rows, down_ref[...], inner)
    finish(copies)


def near(core, arrived, down):
    experts, _, wide = arrived.shape
    half = wide - 128
    hidden = down.shape[0]
    count = experts * (main + extra)
    size = all_groups * group_rows
    return pl.pallas_call(
        near_kernel,
        grid_spec=pltpu.PrefetchScalarGridSpec(
            num_scalar_prefetch=1,
            grid=(count // size,),
            in_specs=[
                pl.BlockSpec((all_groups * group, main, wide), lambda i, c: (i, 0, 0)),
                pl.BlockSpec((hidden, half), lambda i, c: (0, c[0])),
                anywhere,
            ],
            out_specs=[pl.BlockSpec((size, hidden), lambda i, c: (i, 0)), anywhere],
            scratch_shapes=[pltpu.VMEM((128, 128), f32), pltpu.SemaphoreType.DMA((1,))],
        ),
        out_shape=[
            jax.ShapeDtypeStruct((count, hidden), f32),
            pltpu.VMEM((hidden, half), bf16),
        ],
        compiler_params=params(),
        cost_estimate=pl.CostEstimate(
            flops=2 * count * half * hidden, transcendentals=0, bytes_accessed=9 << 20
        ),
        name="near",
    )(core, arrived, held(down), held(down))


def far_kernel(
    core_ref, block_ref, down_ref, part_ref, silu_ref, slope_ref, gate_all, up_all,
    adj_ref, gate_next, up_next, scratch, sems,
):
    half = gate_next.shape[0]
    own = pl.multiple_of(core_ref[0] * half, half)
    copies = load_beside(
        [
            pltpu.make_async_copy(gate_all.at[pl.ds(own, half)], gate_next, sems.at[0]),
            pltpu.make_async_copy(up_all.at[pl.ds(own, half)], up_next, sems.at[1]),
        ]
    )
    rows = unpack(block_ref[...], scratch)
    grad = part_ref[...] + dot(rows, down_ref[...], inner)
    hidden = grad.shape[1]
    adj_ref[:, 0:hidden] = (grad * slope_ref[...]).astype(bf16)
    adj_ref[:, hidden:] = (grad * silu_ref[...]).astype(bf16)
    finish(copies)


def far(core, arrived, down_half, part, silu, slope, gate, up):
    experts, _, wide = arrived.shape
    hidden, half = down_half.shape
    count = experts * (main + extra)
    size = all_groups * group_rows
    by_row = lambda width: pl.BlockSpec((size, width), lambda i, c: (i, 0))
    return pl.pallas_call(
        far_kernel,
        grid_spec=pltpu.PrefetchScalarGridSpec(
            num_scalar_prefetch=1,
            grid=(count // size,),
            in_specs=[
                pl.BlockSpec((all_groups * group, main, wide), lambda i, c: (i, 0, 0)),
                whole((hidden, half)),
                by_row(hidden),
                by_row(hidden),
                by_row(hidden),
                anywhere,
                anywhere,
            ],
            out_specs=[by_row(2 * hidden), anywhere, anywhere],
            scratch_shapes=[pltpu.VMEM((128, 128), f32), pltpu.SemaphoreType.DMA((2,))],
        ),
        out_shape=[
            jax.ShapeDtypeStruct((count, 2 * hidden), bf16),
            pltpu.VMEM((half, hidden), bf16),
            pltpu.VMEM((half, hidden), bf16),
        ],
        compiler_params=params(),
        cost_estimate=pl.CostEstimate(
            flops=2 * count * half * hidden, transcendentals=0, bytes_accessed=16 << 20
        ),
        name="far",
    )(core, arrived, near_by(down_half), part, silu, slope, held(gate), held(up))


def back_rows(adj, gate, up):
    hidden = gate.shape[1]
    back = dot(adj[:, 0:hidden], gate, inner) + dot(adj[:, hidden:], up, inner)
    return back.astype(bf16)


def back_own_kernel(
    core_ref, adj_ref, gate_ref, up_ref, gate_all, up_all, back_ref, gate_next, up_next, sems
):
    half = gate_next.shape[0]
    own = pl.multiple_of(core_ref[0] * half, half)
    copies = load_beside(
        [
            pltpu.make_async_copy(gate_all.at[pl.ds(own, half)], gate_next, sems.at[0]),
            pltpu.make_async_copy(up_all.at[pl.ds(own, half)], up_next, sems.at[1]),
        ]
    )
    back_ref[...] = back_rows(adj_ref[...], gate_ref[...], up_ref[...])
    finish(copies)


def back_own(core, adj, gate_half, up_half, gate_peer, up_peer):
    count = adj.shape[0]
    half, hidden = gate_half.shape
    size = all_groups * group_rows
    by_row = lambda width: pl.BlockSpec((size, width), lambda i, c: (i, 0))
    return pl.pallas_call(
        back_own_kernel,
        grid_spec=pltpu.PrefetchScalarGridSpec(
            num_scalar_prefetch=1,
            grid=(count // size,),
            in_specs=[
                by_row(2 * hidden),
                whole((half, hidden)),
                whole((half, hidden)),
                anywhere,
                anywhere,
            ],
            out_specs=[by_row(half), anywhere, anywhere],
            scratch_shapes=[pltpu.SemaphoreType.DMA((2,))],
        ),
        out_shape=[
            jax.ShapeDtypeStruct((count, half), bf16),
            pltpu.VMEM((half, hidden), bf16),
            pltpu.VMEM((half, hidden), bf16),
        ],
        compiler_params=params(),
        cost_estimate=pl.CostEstimate(
            flops=4 * count * half * hidden, transcendentals=0, bytes_accessed=7 << 20
        ),
        name="back_own",
    )(core, adj, near_by(gate_half), near_by(up_half), held(gate_peer), held(up_peer))


def back_sum_kernel(adj_ref, own_ref, gate_ref, up_ref, out_ref, scratch):
    peer = back_rows(adj_ref[...], gate_ref[...], up_ref[...])
    pack_into(out_ref, own_ref[...].astype(f32) + peer.astype(f32), scratch)


def back_sum(adj, own, gate_half, up_half, shape):
    count = adj.shape[0]
    half, hidden = gate_half.shape
    size = sum_groups * group_rows
    by_row = lambda width: pl.BlockSpec((size, width), lambda i: (i, 0))
    return pl.pallas_call(
        back_sum_kernel,
        grid=(count // size,),
        in_specs=[by_row(2 * hidden), by_row(half), whole((half, hidden)), whole((half, hidden))],
        out_specs=pl.BlockSpec((sum_groups * group, main, shape[2]), lambda i: (i, 0, 0)),
        scratch_shapes=[pltpu.VMEM((128, 128), f32)],
        out_shape=pltpu.HBM(shape, bf16),
        compiler_params=params(),
        cost_estimate=pl.CostEstimate(
            flops=4 * count * half * hidden, transcendentals=0, bytes_accessed=7 << 20
        ),
        name="back_sum",
    )(adj, own, near_by(gate_half), near_by(up_half))


def grad_in_kernel(packed_ref, adj_ref, gate_ref, up_ref):
    grad = dot(packed_ref[...], adj_ref[...], outer).astype(bf16)
    hidden = gate_ref.shape[1]
    gate_ref[...] = grad[:, 0:hidden]
    up_ref[...] = grad[:, hidden:]


def grad_in(packed, adj):
    count, model = packed.shape
    hidden = adj.shape[1] // 2
    size = 512
    out = pl.BlockSpec((size, hidden), lambda i: (i, 0))
    return pl.pallas_call(
        grad_in_kernel,
        grid=(model // size,),
        in_specs=[pl.BlockSpec((count, size), lambda i: (0, i)), whole((count, 2 * hidden))],
        out_specs=[out, out],
        out_shape=[jax.ShapeDtypeStruct((model, hidden), bf16)] * 2,
        compiler_params=params(),
        cost_estimate=pl.CostEstimate(
            flops=4 * count * model * hidden, transcendentals=0, bytes_accessed=11 << 20
        ),
        name="grad_in",
    )(held(packed), held(adj))


def grad_down_kernel(core_ref, active_ref, near_ref, far_ref, out_ref, scratch):
    active = active_ref[...]

    @pl.when(pl.program_id(0) == 0)
    def _():
        out_ref[...] = dot(active, unpack(near_ref[...], scratch), outer).astype(bf16)

    @pl.when(pl.program_id(0) == 1)
    def _():
        out_ref[...] = dot(active, unpack(far_ref[...], scratch), outer).astype(bf16)


def grad_down_of(core, active, arrived, arrived_far):
    count, hidden = active.shape
    half = arrived.shape[2] - 128
    return pl.pallas_call(
        grad_down_kernel,
        grid_spec=pltpu.PrefetchScalarGridSpec(
            num_scalar_prefetch=1,
            grid=(2,),
            in_specs=[whole((count, hidden)), whole(arrived.shape), whole(arrived.shape)],
            out_specs=pl.BlockSpec((hidden, half), lambda i, c: (0, i + c[0] - 2 * i * c[0])),
            scratch_shapes=[pltpu.VMEM((128, 128), f32)],
        ),
        out_shape=jax.ShapeDtypeStruct((hidden, 2 * half), bf16),
        compiler_params=params(),
        cost_estimate=pl.CostEstimate(
            flops=4 * count * half * hidden, transcendentals=0, bytes_accessed=9 << 20
        ),
        name="grad_down",
    )(core, held(active), held(arrived), held(arrived_far))


def combine_kernel(core_ref, block_ref, target_ref, cot_ref, out_ref, total, scratch):
    step = pl.program_id(0)
    tokens = cot_ref.shape[0]
    rows = unpack(block_ref[...], scratch)
    size = rows.shape[0]
    place = lax.broadcasted_iota(jnp.int32, (tokens, size), 1) + step * size
    chosen = jnp.where(
        (place == target_ref[:, 0:1]) | (place == target_ref[:, 1:2]), 1.0, 0.0
    ).astype(bf16)
    found = dot(chosen, rows, plain)

    @pl.when(step == 0)
    def _():
        total[...] = found

    @pl.when(step > 0)
    def _():
        total[...] = total[...] + found

    @pl.when(step == pl.num_programs(0) - 1)
    def _():
        out_ref[...] = (cot_ref[...].astype(f32) + total[...]).astype(bf16)


def combine(core, returned, target, cotangent):
    experts, _, wide = returned.shape
    half = wide - 128
    tokens = cotangent.shape[0]
    return pl.pallas_call(
        combine_kernel,
        grid_spec=pltpu.PrefetchScalarGridSpec(
            num_scalar_prefetch=1,
            grid=(experts // (all_groups * group),),
            in_specs=[
                pl.BlockSpec((all_groups * group, main, wide), lambda i, c: (i, 0, 0)),
                whole((tokens, 8)),
                pl.BlockSpec((tokens, half), lambda i, c: (0, c[0])),
            ],
            out_specs=whole((tokens, half)),
            scratch_shapes=[pltpu.VMEM((tokens, half), f32), pltpu.VMEM((128, 128), f32)],
        ),
        out_shape=jax.ShapeDtypeStruct((tokens, half), bf16),
        compiler_params=params(),
        name="combine",
    )(core, returned, held(target), held(cotangent))


def two_terms(value):
    high = value.astype(bf16)
    return high, (value - high.astype(f32)).astype(bf16)


def share_rows(values, owners):
    value = values.astype(bf16).reshape(owners, 2 * main, values.shape[1])
    return value[:, 0:main], value[:, main:]


def own_kernel(core_ref, own_ref, weight_ref, mixed_ref, grad_ref, share_ref):
    own = own_ref[...]
    grad_ref[...] = dot(own, weight_ref[...], plain)
    left, right = share_rows(dot(own, mixed_ref[...], outer), share_ref.shape[0])
    channels = left.shape[2]
    share_ref[:, :, 0:channels] = left
    share_ref[:, :, channels:] = right


def own_part(core, own, weight, mixed, owners):
    tokens, half = own.shape
    channels = mixed.shape[1]
    return pl.pallas_call(
        own_kernel,
        grid_spec=pltpu.PrefetchScalarGridSpec(
            num_scalar_prefetch=1,
            grid=(1,),
            in_specs=[
                whole((tokens, half)),
                pl.BlockSpec((half, channels), lambda i, c: (c[0], 0)),
                whole((tokens, channels)),
            ],
            out_specs=[whole((tokens, channels)), whole((owners // 2, main, 2 * channels))],
        ),
        out_shape=[
            jax.ShapeDtypeStruct((tokens, channels), f32),
            jax.ShapeDtypeStruct((owners // 2, main, 2 * channels), bf16),
        ],
        compiler_params=params(),
        cost_estimate=pl.CostEstimate(
            flops=4 * tokens * half * channels, transcendentals=0, bytes_accessed=4 << 20
        ),
        name="own_part",
    )(core, own, weight, mixed)


def scan_kernel(
    core_ref, peer_ref, weight_ref, mixed_ref, part_ref, share_ref, slope_ref, gelu_ref, ahead_ref,
    product_ref, first_ref,
    grad_y_out, local_out, share_out, head_out,
    state_grad, grad_y, local, peer_share, lines, head, sems,
):
    tokens, _ = peer_ref.shape
    channels = weight_ref.shape[1]
    core = core_ref[0]
    owners = share_ref.shape[0]
    own_at = pl.ds(pl.multiple_of(core * owners, owners), owners)
    peer_at = pl.ds(pl.multiple_of((1 - core) * owners, owners), owners)
    waits = []

    def copy_out(source, target):
        copy = pltpu.make_async_copy(source, target, sems.at[len(waits)])
        copy.start()
        waits.append(copy)

    copy_out(share_ref, share_out.at[own_at, :, pl.ds(0, 2 * channels)])
    peer = peer_ref[...]
    grad = part_ref[...] + dot(peer, weight_ref[...], plain)
    grad_y[...] = grad * slope_ref[...]
    copy_out(grad_y, grad_y_out)
    values = grad * gelu_ref[...]
    length = tokens // segments
    blocks = state_grad.shape[0]
    for b in range(blocks):
        state_grad[b] = values[:, 128 * b : 128 * (b + 1)]
    carries = []
    for b in range(blocks):
        at = slice(128 * b, 128 * (b + 1))
        value = None
        for j in reversed(range(length)):
            here = state_grad[b, pl.ds(j, segments, stride=length), :]
            if value is None:
                value = here
            else:
                value = here + ahead_ref[b, pl.ds(j, segments, stride=length), :] * value
            local[b, pl.ds(j, segments, stride=length), :] = value
        product = product_ref[b, pl.ds(0, segments, stride=length), :]
        carry = value[segments - 1 : segments]
        for s in reversed(range(1, segments - 1)):
            carry = value[s : s + 1] + product[s : s + 1] * carry
        ends = local[b, 0:3, :] + product_ref[b, 0:3, :] * carry
        carries.append(first_ref[0:1, at] * ends[0:1])
        head[:, at] = jnp.concatenate([ends, first_ref[3:15, at], jnp.zeros((1, 128), f32)], axis=0)
    decay = jnp.concatenate([first_ref[1:2, 128 * b : 128 * (b + 1)] for b in range(blocks)], axis=0)
    terms = two_terms(decay) + two_terms(jnp.concatenate(carries, axis=0))
    line = jnp.concatenate([term.astype(f32) for term in terms], axis=0).astype(bf16)
    lines[...] = jnp.broadcast_to(line[None], lines.shape)
    copy_out(lines, share_out.at[:, :, pl.ds(2 * channels, 128)])
    copy_out(local, local_out)
    copy_out(head, head_out)
    left, right = share_rows(dot(peer, mixed_ref[...], outer), owners)
    peer_share[:, :, 0:channels] = left
    peer_share[:, :, channels : 2 * channels] = right
    copy_out(peer_share, share_out.at[peer_at, :, pl.ds(0, 2 * channels)])
    for copy in waits:
        copy.wait()


def scan(core, peer, weight, mixed, part, share, slope, gelu, ahead, product, first):
    tokens, half = peer.shape
    channels = weight.shape[1]
    owners, rows, _ = share.shape
    out_shape = (2 * owners, rows, 2 * channels + 128)
    return pl.pallas_call(
        scan_kernel,
        grid_spec=pltpu.PrefetchScalarGridSpec(
            num_scalar_prefetch=1,
            grid=(1,),
            in_specs=[
                whole((tokens, half)),
                pl.BlockSpec((half, channels), lambda i, c: (1 - c[0], 0)),
                whole((tokens, channels)),
                whole((tokens, channels)),
                whole(share.shape),
                whole((tokens, channels)),
                whole((tokens, channels)),
                whole(ahead.shape),
                whole(ahead.shape),
                whole((16, channels)),
            ],
            out_specs=[anywhere] * 4,
            scratch_shapes=[
                pltpu.VMEM(ahead.shape, f32),
                pltpu.VMEM((tokens, channels), f32),
                pltpu.VMEM(ahead.shape, f32),
                pltpu.VMEM(share.shape, bf16),
                pltpu.VMEM((2 * owners, rows, 128), bf16),
                pltpu.VMEM((16, channels), f32),
                pltpu.SemaphoreType.DMA((6,)),
            ],
        ),
        out_shape=[
            pltpu.HBM((tokens, channels), f32),
            pltpu.HBM(ahead.shape, f32),
            pltpu.HBM(out_shape, bf16),
            pltpu.HBM((16, channels), f32),
        ],
        compiler_params=params(),
        cost_estimate=pl.CostEstimate(
            flops=4 * tokens * half * channels, transcendentals=0, bytes_accessed=9 << 20
        ),
        name="scan",
    )(core, peer, weight, mixed, part, share, slope, gelu, ahead, product, first)


def tail_kernel(
    place_ref, line_ref, head_ref, local_ref, product_ref, keep_ref, input_ref, direct_ref,
    a_ref, i_ref, taps_ref, out_ref, carries, adjoint, grads,
):
    step = pl.program_id(0)
    tokens = local_ref.shape[1]
    length = tokens // segments
    place = place_ref[0]

    @pl.when(step == 0)
    def _():
        own = jnp.zeros((4, 128), f32)
        beyond = jnp.zeros((4, 128), f32)
        for j in reversed(range(line_ref.shape[0])):
            line = line_ref[j].astype(f32)
            decay = line[0:4] + line[4:8]
            total = line[8:12] + line[12:16]
            own = jnp.where(j > place, total + decay * own, own)
            beyond = jnp.where(j > place + 1, total + decay * beyond, beyond)
        carries[0:4, :] = own
        carries[4:8, :] = beyond

    def conv_grad(value, keep, gate, direct):
        keep = (value * keep).astype(bf16)
        gate = (value * gate).astype(bf16)
        return value * direct + dot(keep, a_ref[0], inner) + dot(gate, i_ref[0], inner)

    carry = carries[pl.ds(step, 1), :]
    for s in reversed(range(segments)):
        lo = s * length
        piece = local_ref[0, lo : lo + length, :] + product_ref[0, lo : lo + length, :] * carry
        adjoint[lo : lo + length, :] = piece
        carry = piece[0:1]
    grads[0:tokens, :] = conv_grad(adjoint[...], keep_ref[...], input_ref[...], direct_ref[...])
    head = head_ref[...]
    spare = jnp.zeros((5, 128), f32)
    three = lambda k: jnp.concatenate([head[3 * k : 3 * k + 3], spare], axis=0)
    later = three(0) + three(1) * carries[pl.ds(step + 4, 1), :]
    grads[tokens : tokens + 8, :] = conv_grad(later, three(2), three(3), three(4))
    total = taps_ref[0:1, :] * grads[3 : 3 + tokens, :]
    for j in range(1, 4):
        total = total + taps_ref[j : j + 1, :] * grads[3 - j : 3 - j + tokens, :]
    out_ref[...] = total


def tail(place, shares, head, local, product, keep, gate, direct, gate_a, gate_x, taps):
    blocks, tokens, span = local.shape
    channels = blocks * span
    owners, rows, _ = shares.shape
    cube = pl.BlockSpec((1, tokens, span), lambda i, c: (i, 0, 0))
    col = lambda rows: pl.BlockSpec((rows, span), lambda i, c: (0, i))
    block = pl.BlockSpec((1, span, span), lambda i, c: (i, 0, 0))
    line = pl.BlockSpec((owners, rows, 128), lambda i, c: (0, 0, 2 * channels // 128))
    return pl.pallas_call(
        tail_kernel,
        grid_spec=pltpu.PrefetchScalarGridSpec(
            num_scalar_prefetch=1,
            grid=(blocks,),
            in_specs=[line, col(16), cube, cube] + [col(tokens)] * 3 + [block, block, col(4)],
            out_specs=col(tokens),
            scratch_shapes=[
                pltpu.VMEM((8, span), f32),
                pltpu.VMEM((tokens, span), f32),
                pltpu.VMEM((tokens + 8, span), f32),
            ],
        ),
        out_shape=jax.ShapeDtypeStruct((tokens, channels), f32),
        compiler_params=params(),
        name="tail",
    )(place, shares, head, held(local), product, keep, gate, direct, held(gate_a), held(gate_x), held(taps))


def exchange(value, axis):
    return lax.all_to_all(value, axis, split_axis=0, concat_axis=0, tiled=True)


def swapped(value):
    return lax.ppermute(value, "tp", [(0, 1), (1, 0)])


def shifted(value, axis, by):
    devices = lax.axis_size(axis)
    pairs = [(i, i + by) for i in range(devices) if 0 <= i + by < devices]
    return lax.ppermute(value, axis, pairs)


def body(
    cotangent,
    routes,
    route_weight,
    expert_rows,
    gate_w,
    up_w,
    down_w,
    in_x,
    in_y,
    state,
    conv_taps,
    gate_a,
    gate_x,
    decay_rate,
    out_weight,
):
    tokens = cotangent.shape[0]
    experts = lax.axis_size("sp")
    core = lax.axis_index("tp").astype(jnp.int32).reshape(1)
    taps = conv_taps.shape[0]
    channels = in_x.shape[1]

    place = lax.axis_index("sp").astype(jnp.int32).reshape(1)

    edge = shifted(
        jnp.concatenate([in_x[tokens - taps + 1 :], state[tokens - 1 :]], axis=0), "sp", 1
    )
    outgoing, target = send(core, routes.T, route_weight.T, cotangent, experts)
    arrived = exchange(outgoing, "sp")
    target = target.T

    gate_peer = swapped(gate_w[0])
    up_peer = swapped(up_w[0])
    packed, silu, slope, active = expert_pre(expert_rows[0], gate_w[0], up_w[0])
    mixed, y_slope, gelu, ahead, product, keep_part, input_part, direct, first = recur_pre(
        in_x, in_y, state, edge, conv_taps, gate_a, gate_x, decay_rate[None]
    )

    arrived_far = swapped(arrived)
    part, down_half = near(core, arrived, down_w[0])
    adj, gate_half, up_half = far(
        core, arrived_far, down_half, part, silu, slope, gate_w[0], up_w[0]
    )
    adj_peer = swapped(adj)
    own, gate_half, up_half = back_own(core, adj, gate_half, up_half, gate_peer, up_peer)
    returning = back_sum(adj_peer, own, gate_half, up_half, arrived.shape)
    returned = exchange(returning, "sp")

    grad_gate, grad_up = grad_in(packed, adj)
    grad_down = grad_down_of(core, active, arrived, arrived_far)

    stream_own = combine(core, returned, target, cotangent)
    stream_peer = swapped(stream_own)
    part, share = own_part(core, stream_own, out_weight, mixed, experts)
    grad_y, local, outgoing, head = scan(
        core, stream_peer, out_weight, mixed, part, share, y_slope, gelu, ahead, product, first
    )
    head = shifted(head, "sp", -1)
    shares = exchange(outgoing, "sp")
    grad_x = tail(
        place, shares, head, local, product, keep_part, input_part, direct,
        gate_a, gate_x, conv_taps,
    )
    summed = jnp.sum(shares[:, :, : 2 * channels].astype(f32), axis=0)
    grad_proj = jnp.concatenate([summed[:, :channels], summed[:, channels:]], axis=0)
    return (grad_gate[None], grad_up[None], grad_down[None], grad_proj, grad_x, grad_y)


def solution(mesh):
    in_specs = (
        P("sp", None),
        P("sp", None),
        P("sp", None),
        P("sp", None, None),
        P("sp", None, "tp"),
        P("sp", None, "tp"),
        P("sp", "tp", None),
        P("sp", "tp"),
        P("sp", "tp"),
        P("sp", "tp"),
        P(None, "tp"),
        P("tp", None, None),
        P("tp", None, None),
        P("tp"),
        P(None, "tp"),
    )
    out_specs = (
        P("sp", None, "tp"),
        P("sp", None, "tp"),
        P("sp", "tp", None),
        P("sp", "tp"),
        P("sp", "tp"),
        P("sp", "tp"),
    )
    return jax.shard_map(body, mesh=mesh, in_specs=in_specs, out_specs=out_specs, check_vma=False)
```

```python
import jax
import jax.numpy as jnp
from jax import lax
from jax.experimental import pallas as pl
from jax.experimental.pallas import tpu as pltpu
from jax.sharding import PartitionSpec as P

rate_scale = 8.0
floor_square = 0.01
inv_root_two = 0.7071067811865476
inv_root_tau = 0.3989422804014327

f32 = jnp.float32
bf16 = jnp.bfloat16
inner = (((1,), (1,)), ((), ()))
outer = (((0,), (0,)), ((), ()))
plain = (((1,), (0,)), ((), ()))

group = 8
main = 16
extra = 2
main_rows = group * main
group_rows = group * (main + extra)
segments = 8


def dot(a, b, dims):
    return lax.dot_general(a, b, dims, preferred_element_type=f32)


def params(n=1, mb=32):
    return pltpu.CompilerParams(dimension_semantics=("arbitrary",) * n, vmem_limit_bytes=mb << 20)


def held(value):
    return pltpu.with_memory_space_constraint(value, pltpu.HBM)


def whole(shape):
    return pl.BlockSpec(shape, lambda *_: (0,) * len(shape))


def pack_extras(rows, scratch):
    for j in range(8):
        scratch[pl.ds(j, group * extra, stride=8), :] = rows[:, 128 * j : 128 * (j + 1)]
    return scratch[...]


def unpack_extras(tiles, scratch):
    scratch[...] = tiles
    return jnp.concatenate(
        [scratch[pl.ds(j, group * extra, stride=8), :] for j in range(8)], axis=1
    )


def send_kernel(core_ref, routes_ref, weight_ref, cot_ref, out_ref, target_ref, slot, scratch):
    step = pl.program_id(0)
    tokens = cot_ref.shape[0]
    experts = pl.num_programs(0) * out_ref.shape[0]

    @pl.when(step == 0)
    def _():
        first = routes_ref[0:1, :]
        second = routes_ref[1:2, :]
        expert = lax.broadcasted_iota(jnp.int32, (experts, tokens), 0)
        hit_first = (expert == first).astype(f32)
        hit_second = (expert == second).astype(f32)
        earlier = (
            lax.broadcasted_iota(jnp.int32, (tokens, tokens), 0)
            < lax.broadcasted_iota(jnp.int32, (tokens, tokens), 1)
        ).astype(f32)
        before = dot((hit_first + hit_second).astype(bf16), earlier.astype(bf16), plain)
        place_first = jnp.sum(before * hit_first, axis=0, keepdims=True).astype(jnp.int32)
        place_second = jnp.sum(before * hit_second, axis=0, keepdims=True).astype(jnp.int32)
        place_second = place_second + (first == second).astype(jnp.int32)
        for k, (name, place) in enumerate(((first, place_first), (second, place_second))):
            base = group_rows * (name >> 3)
            inside = name & 7
            slot[k : k + 1, :] = base + jnp.where(
                place < main, main * inside + place, main_rows + extra * inside + place - main
            )
        target_ref[...] = jnp.concatenate(
            [slot[0:2, :], jnp.zeros((6, tokens), jnp.int32)], axis=0
        )

    size = out_ref.shape[0] // group * group_rows
    rows = lax.broadcasted_iota(jnp.int32, (size, tokens), 0) + step * size
    hit_first = rows == slot[0:1, :]
    hit_second = rows == slot[1:2, :]
    chosen = jnp.where(hit_first | hit_second, 1.0, 0.0).astype(bf16)
    weight = jnp.sum(
        jnp.where(hit_first, weight_ref[0:1, :], 0.0)
        + jnp.where(hit_second, weight_ref[1:2, :], 0.0),
        axis=1,
        keepdims=True,
    )
    values = dot(chosen, cot_ref[...], plain) * weight
    pack_into(out_ref, values, scratch)


def send(core, routes, weight, cotangent, experts):
    tokens, model = cotangent.shape
    half = model // 2
    return pl.pallas_call(
        send_kernel,
        grid_spec=pltpu.PrefetchScalarGridSpec(
            num_scalar_prefetch=1,
            grid=(experts // (send_groups * group),),
            in_specs=[
                whole((2, tokens)),
                whole((2, tokens)),
                pl.BlockSpec((tokens, half), lambda i, c: (0, c[0])),
            ],
            out_specs=[
                pl.BlockSpec((send_groups * group, main, half + 128), lambda i, c: (i, 0, 0)),
                whole((8, tokens)),
            ],
            scratch_shapes=[pltpu.VMEM((8, tokens), jnp.int32), pltpu.VMEM((128, 128), f32)],
        ),
        out_shape=[
            pltpu.HBM((experts, main, half + 128), bf16),
            jax.ShapeDtypeStruct((8, tokens), jnp.int32),
        ],
        compiler_params=params(),
        name="send",
    )(core, held(routes), held(weight), held(cotangent))


pair = 2
send_groups = 4
all_groups = 8
sum_groups = 4


def expert_pre_kernel(rows_ref, gate_ref, up_ref, packed_ref, silu_ref, slope_ref, active_ref):
    out_row = lax.broadcasted_iota(jnp.int32, (group_rows, group_rows), 0)
    column = lax.broadcasted_iota(jnp.int32, (group_rows, group_rows), 1)
    late = out_row - main_rows
    source = jnp.where(
        out_row < main_rows,
        (main + extra) * (out_row >> 4) + (out_row & 15),
        (main + extra) * (late >> 1) + main + (late & 1),
    )
    order = jnp.where(column == source, 1.0, 0.0).astype(bf16)
    for g in range(pair):
        lo = g * group_rows
        packed_ref[lo : lo + group_rows, :] = dot(
            order, rows_ref[lo : lo + group_rows, :], plain
        ).astype(bf16)
    packed = packed_ref[...]
    pre_gate = dot(packed, gate_ref[...], plain)
    pre_up = dot(packed, up_ref[...], plain)
    gate = jax.nn.sigmoid(pre_gate)
    silu = pre_gate * gate
    silu_ref[...] = silu
    slope_ref[...] = pre_up * gate * (1.0 + pre_gate * (1.0 - gate))
    active_ref[...] = (silu * pre_up).astype(bf16)


def expert_pre(rows, gate, up):
    count, model = rows.shape
    hidden = gate.shape[1]
    size = pair * group_rows
    by_row = lambda width: pl.BlockSpec((size, width), lambda i: (i, 0))
    return pl.pallas_call(
        expert_pre_kernel,
        grid=(count // size,),
        in_specs=[by_row(model), whole((model, hidden)), whole((model, hidden))],
        out_specs=[by_row(model), by_row(hidden), by_row(hidden), by_row(hidden)],
        out_shape=[
            pltpu.HBM((count, model), bf16),
            pltpu.HBM((count, hidden), f32),
            pltpu.HBM((count, hidden), f32),
            pltpu.HBM((count, hidden), bf16),
        ],
        compiler_params=params(),
        cost_estimate=pl.CostEstimate(
            flops=4 * count * model * hidden, transcendentals=0, bytes_accessed=20 << 20
        ),
        name="expert_pre",
    )(held(rows), held(gate), held(up))


def recur_pre_kernel(
    x_ref, y_ref, state_ref, edge_ref, taps_ref, a_ref, i_ref, rate_ref,
    mixed_ref, grad_y_ref, gelu_ref, ahead_ref, product_ref, keep_ref, input_ref, direct_ref,
    first_ref, scratch,
):
    tokens = x_ref.shape[0]
    x = x_ref[...].astype(f32)
    edge = edge_ref[...].astype(f32)
    scratch[5:8, :] = edge[0:3]
    scratch[8 : 8 + tokens, :] = x
    conv_x = taps_ref[0:1, :] * scratch[5 : 5 + tokens, :]
    for j in range(1, 4):
        conv_x = conv_x + taps_ref[j : j + 1, :] * scratch[5 + j : 5 + j + tokens, :]
    conv_b = conv_x.astype(bf16)
    keep = jax.nn.sigmoid(dot(conv_b, a_ref[0], plain))
    gate = jax.nn.sigmoid(dot(conv_b, i_ref[0], plain))
    rate = rate_ref[...]
    decay = jnp.exp(-rate_scale * keep * rate)
    norm = jnp.sqrt(1.0 - decay * decay + floor_square)
    state = state_ref[...].astype(f32)
    scratch[7:8, :] = edge[3:4]
    scratch[8 : 8 + tokens, :] = state
    state_prev = scratch[7 : 7 + tokens, :]
    log_part = decay * state_prev - conv_x * gate * decay * decay / norm
    keep_ref[...] = log_part * (-rate_scale * rate) * keep * (1.0 - keep)
    input_ref[...] = conv_x * norm * gate * (1.0 - gate)
    direct_ref[...] = gate * norm
    y = y_ref[...].astype(f32)
    below = 0.5 * (1.0 + lax.erf(y * inv_root_two))
    gelu = y * below
    gelu_ref[...] = gelu
    mixed_ref[...] = (state * gelu).astype(bf16)
    grad_y_ref[...] = state * (below + y * jnp.exp(-0.5 * y * y) * inv_root_tau)
    scratch[0:tokens, :] = decay
    scratch[tokens : tokens + 8, :] = jnp.ones((8, decay.shape[1]), f32)
    ahead_ref[0] = scratch[1 : 1 + tokens, :]
    length = tokens // segments
    product = None
    for j in reversed(range(length)):
        step = scratch[pl.ds(j + 1, segments, stride=length), :]
        product = step if product is None else step * product
        product_ref[0, pl.ds(j, segments, stride=length), :] = product
    rest = product[1:2]
    for s in range(2, segments):
        rest = rest * product[s : s + 1]
    total = decay[0:1] * product[0:1] * rest
    first_ref[...] = jnp.concatenate(
        [
            decay[0:1],
            total,
            rate_scale * rate * jnp.sum(keep, axis=0, keepdims=True),
            product_ref[0, 0:3, :] * rest,
            keep_ref[0:3, :],
            input_ref[0:3, :],
            direct_ref[0:3, :],
            jnp.zeros_like(total),
        ],
        axis=0,
    )


def recur_pre(in_x, in_y, state, edge, taps, gate_a, gate_x, rate):
    tokens, channels = in_x.shape
    blocks, span = gate_a.shape[:2]
    col = lambda rows: pl.BlockSpec((rows, span), lambda i: (0, i))
    block = pl.BlockSpec((1, span, span), lambda i: (i, 0, 0))
    cube = pl.BlockSpec((1, tokens, span), lambda i: (i, 0, 0))
    big = pltpu.HBM((tokens, channels), f32)
    return pl.pallas_call(
        recur_pre_kernel,
        grid=(blocks,),
        in_specs=[col(tokens), col(tokens), col(tokens), col(4), col(4), block, block, col(1)],
        out_specs=[col(tokens)] * 3 + [cube] * 2 + [col(tokens)] * 3 + [col(16)],
        out_shape=[pltpu.HBM((tokens, channels), bf16)]
        + [big] * 2
        + [pltpu.HBM((blocks, tokens, span), f32)] * 2
        + [big] * 3
        + [pltpu.HBM((16, channels), f32)],
        scratch_shapes=[pltpu.VMEM((tokens + 16, span), f32)],
        compiler_params=params(),
        cost_estimate=pl.CostEstimate(
            flops=2000 * tokens * channels, transcendentals=0, bytes_accessed=8 << 20
        ),
        name="recur_pre",
    )(held(in_x), held(in_y), held(state), held(edge), held(taps), held(gate_a), held(gate_x), held(rate))


def unpack(block, scratch):
    width = block.shape[2] - 128
    parts = []
    for g in range(block.shape[0] // group):
        own = block[g * group : (g + 1) * group]
        parts.append(own[:, :, 0:width].reshape(main_rows, width))
        tiles = own[:, :, width:].reshape(128, 128).astype(f32)
        parts.append(unpack_extras(tiles, scratch).astype(bf16))
    return jnp.concatenate(parts, axis=0)


def pack_into(out_ref, values, scratch):
    width = values.shape[1]
    for g in range(out_ref.shape[0] // group):
        lo = g * group_rows
        out_ref[g * group : (g + 1) * group, :, 0:width] = (
            values[lo : lo + main_rows].astype(bf16).reshape(group, main, width)
        )
        tiles = pack_extras(values[lo + main_rows : lo + group_rows], scratch)
        out_ref[g * group : (g + 1) * group, :, width:] = tiles.astype(bf16).reshape(
            group, main, 128
        )


def near_by(value):
    return pltpu.with_memory_space_constraint(value, pltpu.VMEM)


def load_beside(copies):
    @pl.when(pl.program_id(0) == 0)
    def _():
        for copy in copies:
            copy.start()

    return copies


def finish(copies):
    @pl.when(pl.program_id(0) == pl.num_programs(0) - 1)
    def _():
        for copy in copies:
            copy.wait()


anywhere = pl.BlockSpec(memory_space=pl.ANY)
resident = pl.BlockSpec(memory_space=pltpu.VMEM)


def near_kernel(core_ref, block_ref, down_ref, down_all, part_ref, down_next, scratch, sems):
    half = down_ref.shape[1]
    other = pl.multiple_of((1 - core_ref[0]) * half, half)
    copies = load_beside(
        [pltpu.make_async_copy(down_all.at[:, pl.ds(other, half)], down_next, sems.at[0])]
    )
    rows = unpack(block_ref[...], scratch)
    part_ref[...] = dot(rows, down_ref[...], inner)
    finish(copies)


def near(core, arrived, down):
    experts, _, wide = arrived.shape
    half = wide - 128
    hidden = down.shape[0]
    count = experts * (main + extra)
    size = all_groups * group_rows
    return pl.pallas_call(
        near_kernel,
        grid_spec=pltpu.PrefetchScalarGridSpec(
            num_scalar_prefetch=1,
            grid=(count // size,),
            in_specs=[
                pl.BlockSpec((all_groups * group, main, wide), lambda i, c: (i, 0, 0)),
                pl.BlockSpec((hidden, half), lambda i, c: (0, c[0])),
                anywhere,
            ],
            out_specs=[pl.BlockSpec((size, hidden), lambda i, c: (i, 0)), anywhere],
            scratch_shapes=[pltpu.VMEM((128, 128), f32), pltpu.SemaphoreType.DMA((1,))],
        ),
        out_shape=[
            jax.ShapeDtypeStruct((count, hidden), f32),
            pltpu.VMEM((hidden, half), bf16),
        ],
        compiler_params=params(),
        cost_estimate=pl.CostEstimate(
            flops=2 * count * half * hidden, transcendentals=0, bytes_accessed=9 << 20
        ),
        name="near",
    )(core, arrived, held(down), held(down))


def far_kernel(
    core_ref, block_ref, down_ref, part_ref, silu_ref, slope_ref, gate_all, up_all,
    adj_ref, gate_next, up_next, scratch, sems,
):
    half = gate_next.shape[0]
    own = pl.multiple_of(core_ref[0] * half, half)
    copies = load_beside(
        [
            pltpu.make_async_copy(gate_all.at[pl.ds(own, half)], gate_next, sems.at[0]),
            pltpu.make_async_copy(up_all.at[pl.ds(own, half)], up_next, sems.at[1]),
        ]
    )
    rows = unpack(block_ref[...], scratch)
    grad = part_ref[...] + dot(rows, down_ref[...], inner)
    hidden = grad.shape[1]
    adj_ref[:, 0:hidden] = (grad * slope_ref[...]).astype(bf16)
    adj_ref[:, hidden:] = (grad * silu_ref[...]).astype(bf16)
    finish(copies)


def far(core, arrived, down_half, part, silu, slope, gate, up):
    experts, _, _ = arrived.shape
    hidden, half = down_half.shape
    count = experts * (main + extra)
    size = all_groups * group_rows
    by_row = lambda width: pl.BlockSpec((size, width), lambda i, c: (i, 0))
    return pl.pallas_call(
        far_kernel,
        grid_spec=pltpu.PrefetchScalarGridSpec(
            num_scalar_prefetch=1,
            grid=(count // size,),
            in_specs=[
                resident,
                resident,
                resident,
                resident,
                resident,
                anywhere,
                anywhere,
            ],
            out_specs=[by_row(2 * hidden), anywhere, anywhere],
            scratch_shapes=[pltpu.VMEM((128, 128), f32), pltpu.SemaphoreType.DMA((2,))],
        ),
        out_shape=[
            jax.ShapeDtypeStruct((count, 2 * hidden), bf16),
            pltpu.VMEM((half, hidden), bf16),
            pltpu.VMEM((half, hidden), bf16),
        ],
        compiler_params=params(),
        cost_estimate=pl.CostEstimate(
            flops=2 * count * half * hidden, transcendentals=0, bytes_accessed=16 << 20
        ),
        name="far",
    )(core, arrived, near_by(down_half), part, silu, slope, held(gate), held(up))


def back_rows(adj, gate, up):
    hidden = gate.shape[1]
    back = dot(adj[:, 0:hidden], gate, inner) + dot(adj[:, hidden:], up, inner)
    return back.astype(bf16)


def back_own_kernel(
    core_ref, adj_ref, gate_ref, up_ref, gate_all, up_all, back_ref, gate_next, up_next, sems
):
    half = gate_next.shape[0]
    own = pl.multiple_of(core_ref[0] * half, half)
    copies = load_beside(
        [
            pltpu.make_async_copy(gate_all.at[pl.ds(own, half)], gate_next, sems.at[0]),
            pltpu.make_async_copy(up_all.at[pl.ds(own, half)], up_next, sems.at[1]),
        ]
    )
    back_ref[...] = back_rows(adj_ref[...], gate_ref[...], up_ref[...])
    finish(copies)


def back_own(core, adj, gate_half, up_half, gate_peer, up_peer):
    count = adj.shape[0]
    half, hidden = gate_half.shape
    size = all_groups * group_rows
    by_row = lambda width: pl.BlockSpec((size, width), lambda i, c: (i, 0))
    return pl.pallas_call(
        back_own_kernel,
        grid_spec=pltpu.PrefetchScalarGridSpec(
            num_scalar_prefetch=1,
            grid=(count // size,),
            in_specs=[
                resident,
                resident,
                resident,
                anywhere,
                anywhere,
            ],
            out_specs=[by_row(half), anywhere, anywhere],
            scratch_shapes=[pltpu.SemaphoreType.DMA((2,))],
        ),
        out_shape=[
            jax.ShapeDtypeStruct((count, half), bf16),
            pltpu.VMEM((half, hidden), bf16),
            pltpu.VMEM((half, hidden), bf16),
        ],
        compiler_params=params(),
        cost_estimate=pl.CostEstimate(
            flops=4 * count * half * hidden, transcendentals=0, bytes_accessed=7 << 20
        ),
        name="back_own",
    )(core, adj, near_by(gate_half), near_by(up_half), held(gate_peer), held(up_peer))


def back_sum_kernel(adj_ref, own_ref, gate_ref, up_ref, out_ref, scratch):
    peer = back_rows(adj_ref[...], gate_ref[...], up_ref[...])
    pack_into(out_ref, own_ref[...].astype(f32) + peer.astype(f32), scratch)


def back_sum(adj, own, gate_half, up_half, shape):
    count = adj.shape[0]
    half, hidden = gate_half.shape
    size = sum_groups * group_rows
    by_row = lambda width: pl.BlockSpec((size, width), lambda i: (i, 0))
    return pl.pallas_call(
        back_sum_kernel,
        grid=(count // size,),
        in_specs=[by_row(2 * hidden), by_row(half), whole((half, hidden)), whole((half, hidden))],
        out_specs=pl.BlockSpec((sum_groups * group, main, shape[2]), lambda i: (i, 0, 0)),
        scratch_shapes=[pltpu.VMEM((128, 128), f32)],
        out_shape=pltpu.HBM(shape, bf16),
        compiler_params=params(),
        cost_estimate=pl.CostEstimate(
            flops=4 * count * half * hidden, transcendentals=0, bytes_accessed=7 << 20
        ),
        name="back_sum",
    )(adj, own, near_by(gate_half), near_by(up_half))


def grad_in_kernel(packed_ref, adj_ref, gate_ref, up_ref):
    grad = dot(packed_ref[...], adj_ref[...], outer).astype(bf16)
    hidden = gate_ref.shape[1]
    gate_ref[...] = grad[:, 0:hidden]
    up_ref[...] = grad[:, hidden:]


def grad_in(packed, adj):
    count, model = packed.shape
    hidden = adj.shape[1] // 2
    size = 512
    out = pl.BlockSpec((size, hidden), lambda i: (i, 0))
    return pl.pallas_call(
        grad_in_kernel,
        grid=(model // size,),
        in_specs=[pl.BlockSpec((count, size), lambda i: (0, i)), whole((count, 2 * hidden))],
        out_specs=[out, out],
        out_shape=[jax.ShapeDtypeStruct((model, hidden), bf16)] * 2,
        compiler_params=params(),
        cost_estimate=pl.CostEstimate(
            flops=4 * count * model * hidden, transcendentals=0, bytes_accessed=11 << 20
        ),
        name="grad_in",
    )(held(packed), held(adj))


def grad_down_kernel(core_ref, active_ref, near_ref, far_ref, out_ref, scratch):
    active = active_ref[...]

    @pl.when(pl.program_id(0) == 0)
    def _():
        out_ref[...] = dot(active, unpack(near_ref[...], scratch), outer).astype(bf16)

    @pl.when(pl.program_id(0) == 1)
    def _():
        out_ref[...] = dot(active, unpack(far_ref[...], scratch), outer).astype(bf16)


def grad_down_of(core, active, arrived, arrived_far):
    count, hidden = active.shape
    half = arrived.shape[2] - 128
    return pl.pallas_call(
        grad_down_kernel,
        grid_spec=pltpu.PrefetchScalarGridSpec(
            num_scalar_prefetch=1,
            grid=(2,),
            in_specs=[whole((count, hidden)), whole(arrived.shape), whole(arrived.shape)],
            out_specs=pl.BlockSpec((hidden, half), lambda i, c: (0, i + c[0] - 2 * i * c[0])),
            scratch_shapes=[pltpu.VMEM((128, 128), f32)],
        ),
        out_shape=jax.ShapeDtypeStruct((hidden, 2 * half), bf16),
        compiler_params=params(),
        cost_estimate=pl.CostEstimate(
            flops=4 * count * half * hidden, transcendentals=0, bytes_accessed=9 << 20
        ),
        name="grad_down",
    )(core, held(active), held(arrived), held(arrived_far))


def combine_kernel(
    core_ref, block_ref, target_ref, cot_ref, weight_all, mixed_all,
    out_ref, weight_next, mixed_next, scratch, sems,
):
    half = weight_next.shape[0]
    own = pl.multiple_of(core_ref[0] * half, half)
    copies = load_beside(
        [
            pltpu.make_async_copy(weight_all.at[pl.ds(own, half)], weight_next, sems.at[0]),
            pltpu.make_async_copy(mixed_all, mixed_next, sems.at[1]),
        ]
    )
    tokens = cot_ref.shape[0]
    rows = unpack(block_ref[...], scratch)
    place = lax.broadcasted_iota(jnp.int32, (tokens, rows.shape[0]), 1)
    chosen = jnp.where(
        (place == target_ref[:, 0:1]) | (place == target_ref[:, 1:2]), 1.0, 0.0
    ).astype(bf16)
    out_ref[...] = (cot_ref[...].astype(f32) + dot(chosen, rows, plain)).astype(bf16)
    finish(copies)


def combine(core, returned, target, cotangent, weight, mixed):
    half = returned.shape[2] - 128
    tokens = cotangent.shape[0]
    return pl.pallas_call(
        combine_kernel,
        grid_spec=pltpu.PrefetchScalarGridSpec(
            num_scalar_prefetch=1,
            grid=(1,),
            in_specs=[
                resident,
                whole((tokens, 8)),
                pl.BlockSpec((tokens, half), lambda i, c: (0, c[0])),
                anywhere,
                anywhere,
            ],
            out_specs=[whole((tokens, half)), anywhere, anywhere],
            scratch_shapes=[pltpu.VMEM((128, 128), f32), pltpu.SemaphoreType.DMA((2,))],
        ),
        out_shape=[
            jax.ShapeDtypeStruct((tokens, half), bf16),
            pltpu.VMEM((half, weight.shape[1]), bf16),
            pltpu.VMEM(mixed.shape, bf16),
        ],
        compiler_params=params(),
        name="combine",
    )(core, returned, held(target), held(cotangent), held(weight), held(mixed))


def write_shares(ref, values):
    pieces = values.astype(bf16).reshape(ref.shape[0], 4, 8, values.shape[1])
    channels = values.shape[1]
    for k in range(4):
        ref[:, :, channels * k : channels * (k + 1)] = pieces[:, k]


def own_kernel(
    core_ref, own_ref, weight_ref, mixed_ref, weight_all, grad_ref, share_out, weight_next, share, sems
):
    half = weight_next.shape[0]
    other = pl.multiple_of((1 - core_ref[0]) * half, half)
    copies = load_beside(
        [pltpu.make_async_copy(weight_all.at[pl.ds(other, half)], weight_next, sems.at[1])]
    )
    owners = share.shape[0]
    at = pl.ds(pl.multiple_of(core_ref[0] * owners, owners), owners)
    own = own_ref[...]
    write_shares(share, dot(own, mixed_ref[...], outer))
    copy = pltpu.make_async_copy(share, share_out.at[at, :, pl.ds(0, share.shape[2])], sems.at[0])
    copy.start()
    grad_ref[...] = dot(own, weight_ref[...], plain)
    copy.wait()
    finish(copies)


def own_part(core, own, weight_half, mixed, weight, owners):
    tokens, half = own.shape
    channels = mixed.shape[1]
    return pl.pallas_call(
        own_kernel,
        grid_spec=pltpu.PrefetchScalarGridSpec(
            num_scalar_prefetch=1,
            grid=(1,),
            in_specs=[
                resident,
                resident,
                resident,
                anywhere,
            ],
            out_specs=[whole((tokens, channels)), anywhere, anywhere],
            scratch_shapes=[
                pltpu.VMEM((owners // 2, 8, 4 * channels), bf16),
                pltpu.SemaphoreType.DMA((2,)),
            ],
        ),
        out_shape=[
            jax.ShapeDtypeStruct((tokens, channels), f32),
            pltpu.HBM((owners, 8, 4 * channels + 128), bf16),
            pltpu.VMEM((half, channels), bf16),
        ],
        compiler_params=params(),
        cost_estimate=pl.CostEstimate(
            flops=4 * tokens * half * channels, transcendentals=0, bytes_accessed=4 << 20
        ),
        name="own_part",
    )(core, own, near_by(weight_half), near_by(mixed), held(weight))


def segment_scan(values, ahead_ref, state_grad, local):
    blocks, tokens, span = state_grad.shape
    length = tokens // segments
    for b in range(blocks):
        state_grad[b] = values[:, span * b : span * (b + 1)]
    last = [None] * blocks
    for j in reversed(range(length)):
        at = pl.ds(j, segments, stride=length)
        for b in range(blocks):
            here = state_grad[b, at, :]
            last[b] = here if last[b] is None else here + ahead_ref[b, at, :] * last[b]
            local[b, at, :] = last[b]
    return last


def scan_kernel(
    core_ref, peer_ref, weight_ref, mixed_ref, part_ref, gelu_ref, ahead_ref, product_ref, first_ref,
    share_in, share_out, head_ref,
    state_grad, local, share, lines, sems,
):
    owners = share.shape[0]
    other = pl.ds(pl.multiple_of((1 - core_ref[0]) * owners, owners), owners)
    columns = share.shape[2]
    peer = peer_ref[...]
    grad = part_ref[...] + dot(peer, weight_ref[...], plain)
    write_shares(share, dot(peer, mixed_ref[...], outer))
    main_copy = pltpu.make_async_copy(share, share_out.at[other, :, pl.ds(0, columns)], sems.at[0])
    main_copy.start()
    values = grad * gelu_ref[...]
    blocks, tokens, _ = state_grad.shape
    length = tokens // segments
    last = segment_scan(values, ahead_ref, state_grad, local)
    tiles = []
    for b in range(blocks):
        at = slice(128 * b, 128 * (b + 1))
        value = last[b]
        product = product_ref[b, pl.ds(0, segments, stride=length), :]
        carry = value[segments - 1 : segments]
        for s in reversed(range(1, segments - 1)):
            carry = value[s : s + 1] + product[s : s + 1] * carry
        ends = local[b, 0:3, :] + product_ref[b, 0:3, :] * carry
        tiles.append(first_ref[0:1, at] * ends[0:1])
        head_ref[:, at] = jnp.concatenate(
            [ends, first_ref[3:15, at], jnp.zeros((1, 128), f32)], axis=0
        )
    power = [first_ref[2:3, 128 * b : 128 * (b + 1)] for b in range(blocks)]
    line = jnp.concatenate(power + tiles, axis=0).astype(bf16)
    lines[...] = jnp.broadcast_to(line[None], lines.shape)
    line_copy = pltpu.make_async_copy(lines, share_out.at[:, :, pl.ds(columns, 128)], sems.at[1])
    line_copy.start()
    main_copy.wait()
    line_copy.wait()


def scan(core, peer, weight, mixed, part, shares, gelu, ahead, product, first):
    tokens, half = peer.shape
    channels = weight.shape[1]
    owners = shares.shape[0]
    return pl.pallas_call(
        scan_kernel,
        grid_spec=pltpu.PrefetchScalarGridSpec(
            num_scalar_prefetch=1,
            grid=(1,),
            in_specs=[
                resident,
                resident,
                resident,
                resident,
                resident,
                resident,
                resident,
                resident,
                anywhere,
            ],
            out_specs=[anywhere, whole((16, channels))],
            scratch_shapes=[
                pltpu.VMEM(ahead.shape, f32),
                pltpu.VMEM(ahead.shape, f32),
                pltpu.VMEM((owners // 2, 8, 4 * channels), bf16),
                pltpu.VMEM((owners, 8, 128), bf16),
                pltpu.SemaphoreType.DMA((2,)),
            ],
        ),
        out_shape=[pltpu.HBM(shares.shape, bf16), pltpu.HBM((16, channels), f32)],
        input_output_aliases={9: 0},
        compiler_params=params(),
        cost_estimate=pl.CostEstimate(
            flops=4 * tokens * half * channels, transcendentals=0, bytes_accessed=9 << 20
        ),
        name="scan",
    )(
        core, peer, near_by(weight), near_by(mixed), part, gelu, ahead, product, first, held(shares)
    )


def local_kernel(
    core_ref, peer_ref, weight_ref, part_ref, slope_ref, gelu_ref, ahead_ref,
    grad_y_ref, local_ref, state_grad,
):
    grad = part_ref[...] + dot(peer_ref[...], weight_ref[...], plain)
    grad_y_ref[...] = grad * slope_ref[...]
    segment_scan(grad * gelu_ref[...], ahead_ref, state_grad, local_ref)


def local_scan(core, peer, weight, part, slope, gelu, ahead):
    tokens, half = peer.shape
    channels = weight.shape[1]
    return pl.pallas_call(
        local_kernel,
        grid_spec=pltpu.PrefetchScalarGridSpec(
            num_scalar_prefetch=1,
            grid=(1,),
            in_specs=[
                whole((tokens, half)),
                pl.BlockSpec((half, channels), lambda i, c: (1 - c[0], 0)),
                whole((tokens, channels)),
                whole((tokens, channels)),
                whole((tokens, channels)),
                whole(ahead.shape),
            ],
            out_specs=[whole((tokens, channels)), whole(ahead.shape)],
            scratch_shapes=[pltpu.VMEM(ahead.shape, f32)],
        ),
        out_shape=[pltpu.HBM((tokens, channels), f32), pltpu.HBM(ahead.shape, f32)],
        compiler_params=params(),
        cost_estimate=pl.CostEstimate(
            flops=2 * tokens * half * channels, transcendentals=0, bytes_accessed=9 << 20
        ),
        name="local_scan",
    )(core, held(peer), held(weight), held(part), held(slope), held(gelu), held(ahead))


def tail_kernel(
    place_ref, share_ref, head_ref, taps_ref, a_ref, i_ref, *rest,
):
    sources, (out_hbm, project_ref), stores = rest[0:5], rest[5:7], rest[7:]
    local_ref, product_ref, keep_ref, input_ref, direct_ref = buffers = stores[0:5]
    adjoint, grads, out, in_sems, out_sems = stores[5:]
    blocks, tokens, span = local_ref.shape
    length = tokens // segments
    place = place_ref[0]

    def column(ref, c):
        return ref.at[c] if len(ref.shape) == 3 else ref.at[:, pl.ds(span * c, span)]

    copies = [
        [
            pltpu.make_async_copy(column(source, c), column(buffer, c), in_sems.at[c, k])
            for k, (source, buffer) in enumerate(zip(sources, buffers))
        ]
        for c in range(blocks)
    ]
    for group_copies in copies:
        for copy in group_copies:
            copy.start()

    own = jnp.zeros((4, span), f32)
    beyond = jnp.zeros((4, span), f32)
    columns = share_ref.shape[2] - 128
    channels = columns // 4
    summed = jnp.zeros((8, columns), f32)
    for j in reversed(range(share_ref.shape[0])):
        share = share_ref[j].astype(f32)
        summed = summed + share[:, 0:columns]
        line = share[:, columns:]
        decay = jnp.exp(-line[0:4])
        own = jnp.where(j > place, line[4:8] + decay * own, own)
        beyond = jnp.where(j > place + 1, line[4:8] + decay * beyond, beyond)

    for k in range(4):
        project_ref[8 * k : 8 * (k + 1), :] = summed[:, channels * k : channels * (k + 1)]
    results = []
    for c in range(blocks):
        at = slice(span * c, span * (c + 1))

        def conv_grad(value, keep, gate, direct):
            keep = (value * keep).astype(bf16)
            gate = (value * gate).astype(bf16)
            return value * direct + dot(keep, a_ref[c], inner) + dot(gate, i_ref[c], inner)

        for copy in copies[c]:
            copy.wait()
        carry = own[c : c + 1]
        for s in reversed(range(segments)):
            rows = slice(s * length, (s + 1) * length)
            piece = local_ref[c, rows, :] + product_ref[c, rows, :] * carry
            adjoint[rows, :] = piece
            carry = piece[0:1]
        grads[0:tokens, :] = conv_grad(
            adjoint[...], keep_ref[:, at], input_ref[:, at], direct_ref[:, at]
        )
        head = head_ref[:, at]
        spare = jnp.zeros((5, span), f32)
        three = lambda k: jnp.concatenate([head[3 * k : 3 * k + 3], spare], axis=0)
        later = three(0) + three(1) * beyond[c : c + 1]
        grads[tokens : tokens + 8, :] = conv_grad(later, three(2), three(3), three(4))
        total = taps_ref[0:1, at] * grads[3 : 3 + tokens, :]
        for j in range(1, 4):
            total = total + taps_ref[j : j + 1, at] * grads[3 - j : 3 - j + tokens, :]
        out[:, at] = total
        results.append(
            pltpu.make_async_copy(column(out, c), column(out_hbm, c), out_sems.at[c])
        )
        results[-1].start()
    for copy in results:
        copy.wait()


def tail(place, shares, head, local, product, keep, gate, direct, gate_a, gate_x, taps):
    blocks, tokens, span = local.shape
    channels = blocks * span
    rows = shares.shape[1]
    sources = (local, product, keep, gate, direct)
    return pl.pallas_call(
        tail_kernel,
        grid_spec=pltpu.PrefetchScalarGridSpec(
            num_scalar_prefetch=1,
            grid=(1,),
            in_specs=[
                resident,
                resident,
                whole((4, channels)),
                whole(gate_a.shape),
                whole(gate_x.shape),
            ]
            + [anywhere] * 5,
            out_specs=[anywhere, whole((4 * rows, channels))],
            scratch_shapes=[pltpu.VMEM(value.shape, f32) for value in sources]
            + [
                pltpu.VMEM((tokens, span), f32),
                pltpu.VMEM((tokens + 8, span), f32),
                pltpu.VMEM((tokens, channels), f32),
                pltpu.SemaphoreType.DMA((blocks, 5)),
                pltpu.SemaphoreType.DMA((blocks,)),
            ],
        ),
        out_shape=[
            pltpu.HBM((tokens, channels), f32),
            pltpu.HBM((4 * rows, channels), f32),
        ],
        compiler_params=params(),
        name="tail",
    )(place, shares, head, held(taps), held(gate_a), held(gate_x), *(held(v) for v in sources))


def exchange(value, axis):
    return lax.all_to_all(value, axis, split_axis=0, concat_axis=0, tiled=True)


def swapped(value):
    return lax.ppermute(value, "tp", [(0, 1), (1, 0)])


def shifted(value, axis, by):
    devices = lax.axis_size(axis)
    pairs = [(i, i + by) for i in range(devices) if 0 <= i + by < devices]
    return lax.ppermute(value, axis, pairs)


def body(
    cotangent,
    routes,
    route_weight,
    expert_rows,
    gate_w,
    up_w,
    down_w,
    in_x,
    in_y,
    state,
    conv_taps,
    gate_a,
    gate_x,
    decay_rate,
    out_weight,
):
    tokens = cotangent.shape[0]
    experts = lax.axis_size("sp")
    core = lax.axis_index("tp").astype(jnp.int32).reshape(1)
    taps = conv_taps.shape[0]

    place = lax.axis_index("sp").astype(jnp.int32).reshape(1)

    edge = shifted(
        jnp.concatenate([in_x[tokens - taps + 1 :], state[tokens - 1 :]], axis=0), "sp", 1
    )
    outgoing, target = send(core, routes.T, route_weight.T, cotangent, experts)
    arrived = exchange(outgoing, "sp")
    target = target.T

    gate_peer = swapped(gate_w[0])
    up_peer = swapped(up_w[0])
    packed, silu, slope, active = expert_pre(expert_rows[0], gate_w[0], up_w[0])
    mixed, y_slope, gelu, ahead, product, keep_part, input_part, direct, first = recur_pre(
        in_x, in_y, state, edge, conv_taps, gate_a, gate_x, decay_rate[None]
    )

    arrived_far = swapped(arrived)
    part, down_half = near(core, arrived, down_w[0])
    adj, gate_half, up_half = far(
        core, arrived_far, down_half, part, silu, slope, gate_w[0], up_w[0]
    )
    adj_peer = swapped(adj)
    own, gate_half, up_half = back_own(core, adj, gate_half, up_half, gate_peer, up_peer)
    returning = back_sum(adj_peer, own, gate_half, up_half, arrived.shape)
    returned = exchange(returning, "sp")

    grad_gate, grad_up = grad_in(packed, adj)
    grad_down = grad_down_of(core, active, arrived, arrived_far)

    stream_own, weight_half, mixed_here = combine(
        core, returned, target, cotangent, out_weight, mixed
    )
    stream_peer = swapped(stream_own)
    part, shares, weight_half = own_part(
        core, stream_own, weight_half, mixed_here, out_weight, experts
    )
    outgoing, head = scan(
        core, stream_peer, weight_half, mixed_here, part, shares, gelu, ahead, product, first
    )
    grad_y, local = local_scan(core, stream_peer, out_weight, part, y_slope, gelu, ahead)
    head = shifted(head, "sp", -1)
    shares = exchange(outgoing, "sp")
    grad_x, grad_proj = tail(
        place, shares, head, local, product, keep_part, input_part, direct,
        gate_a, gate_x, conv_taps,
    )
    return (grad_gate[None], grad_up[None], grad_down[None], grad_proj, grad_x, grad_y)


def solution(mesh):
    in_specs = (
        P("sp", None),
        P("sp", None),
        P("sp", None),
        P("sp", None, None),
        P("sp", None, "tp"),
        P("sp", None, "tp"),
        P("sp", "tp", None),
        P("sp", "tp"),
        P("sp", "tp"),
        P("sp", "tp"),
        P(None, "tp"),
        P("tp", None, None),
        P("tp", None, None),
        P("tp"),
        P(None, "tp"),
    )
    out_specs = (
        P("sp", None, "tp"),
        P("sp", None, "tp"),
        P("sp", "tp", None),
        P("sp", "tp"),
        P("sp", "tp"),
        P("sp", "tp"),
    )
    return jax.shard_map(body, mesh=mesh, in_specs=in_specs, out_specs=out_specs, check_vma=False)
```

```python
import jax
import jax.numpy as jnp
from jax import lax
from jax.experimental import pallas as pl
from jax.experimental.pallas import tpu as pltpu
from jax.sharding import PartitionSpec as P

rate_scale = 8.0
floor_square = 0.01
inv_root_two = 0.7071067811865476
inv_root_tau = 0.3989422804014327

f32 = jnp.float32
bf16 = jnp.bfloat16
inner = (((1,), (1,)), ((), ()))
outer = (((0,), (0,)), ((), ()))
plain = (((1,), (0,)), ((), ()))

group = 8
main = 16
extra = 2
main_rows = group * main
group_rows = group * (main + extra)
segments = 8


def dot(a, b, dims):
    return lax.dot_general(a, b, dims, preferred_element_type=f32)


def params(n=1, mb=32):
    return pltpu.CompilerParams(dimension_semantics=("arbitrary",) * n, vmem_limit_bytes=mb << 20)


def held(value):
    return pltpu.with_memory_space_constraint(value, pltpu.HBM)


def whole(shape):
    return pl.BlockSpec(shape, lambda *_: (0,) * len(shape))


def pack_extras(rows, scratch):
    for j in range(8):
        scratch[pl.ds(j, group * extra, stride=8), :] = rows[:, 128 * j : 128 * (j + 1)]
    return scratch[...]


def unpack_extras(tiles, scratch):
    scratch[...] = tiles
    return jnp.concatenate(
        [scratch[pl.ds(j, group * extra, stride=8), :] for j in range(8)], axis=1
    )


def send_kernel(core_ref, routes_ref, weight_ref, cot_ref, out_ref, target_ref, slot, scratch):
    step = pl.program_id(0)
    tokens = cot_ref.shape[0]
    experts = pl.num_programs(0) * out_ref.shape[0]

    @pl.when(step == 0)
    def _():
        first = routes_ref[0:1, :]
        second = routes_ref[1:2, :]
        expert = lax.broadcasted_iota(jnp.int32, (experts, tokens), 0)
        hit_first = (expert == first).astype(f32)
        hit_second = (expert == second).astype(f32)
        earlier = (
            lax.broadcasted_iota(jnp.int32, (tokens, tokens), 0)
            < lax.broadcasted_iota(jnp.int32, (tokens, tokens), 1)
        ).astype(f32)
        before = dot((hit_first + hit_second).astype(bf16), earlier.astype(bf16), plain)
        place_first = jnp.sum(before * hit_first, axis=0, keepdims=True).astype(jnp.int32)
        place_second = jnp.sum(before * hit_second, axis=0, keepdims=True).astype(jnp.int32)
        place_second = place_second + (first == second).astype(jnp.int32)
        for k, (name, place) in enumerate(((first, place_first), (second, place_second))):
            base = group_rows * (name >> 3)
            inside = name & 7
            slot[k : k + 1, :] = base + jnp.where(
                place < main, main * inside + place, main_rows + extra * inside + place - main
            )
        target_ref[...] = jnp.concatenate(
            [slot[0:2, :], jnp.zeros((6, tokens), jnp.int32)], axis=0
        )

    size = out_ref.shape[0] // group * group_rows
    rows = lax.broadcasted_iota(jnp.int32, (size, tokens), 0) + step * size
    hit_first = rows == slot[0:1, :]
    hit_second = rows == slot[1:2, :]
    chosen = jnp.where(hit_first | hit_second, 1.0, 0.0).astype(bf16)
    weight = jnp.sum(
        jnp.where(hit_first, weight_ref[0:1, :], 0.0)
        + jnp.where(hit_second, weight_ref[1:2, :], 0.0),
        axis=1,
        keepdims=True,
    )
    values = dot(chosen, cot_ref[...], plain) * weight
    pack_into(out_ref, values, scratch)


def send(core, routes, weight, cotangent, experts):
    tokens, model = cotangent.shape
    half = model // 2
    return pl.pallas_call(
        send_kernel,
        grid_spec=pltpu.PrefetchScalarGridSpec(
            num_scalar_prefetch=1,
            grid=(experts // (send_groups * group),),
            in_specs=[
                whole((2, tokens)),
                whole((2, tokens)),
                pl.BlockSpec((tokens, half), lambda i, c: (0, c[0])),
            ],
            out_specs=[
                pl.BlockSpec((send_groups * group, main, half + 128), lambda i, c: (i, 0, 0)),
                whole((8, tokens)),
            ],
            scratch_shapes=[pltpu.VMEM((8, tokens), jnp.int32), pltpu.VMEM((128, 128), f32)],
        ),
        out_shape=[
            pltpu.HBM((experts, main, half + 128), bf16),
            jax.ShapeDtypeStruct((8, tokens), jnp.int32),
        ],
        compiler_params=params(),
        name="send",
    )(core, held(routes), held(weight), held(cotangent))


pair = 2
send_groups = 4
all_groups = 8
sum_parts = 4


def expert_pre_kernel(rows_ref, gate_ref, up_ref, packed_ref, silu_ref, slope_ref, active_ref):
    out_row = lax.broadcasted_iota(jnp.int32, (group_rows, group_rows), 0)
    column = lax.broadcasted_iota(jnp.int32, (group_rows, group_rows), 1)
    late = out_row - main_rows
    source = jnp.where(
        out_row < main_rows,
        (main + extra) * (out_row >> 4) + (out_row & 15),
        (main + extra) * (late >> 1) + main + (late & 1),
    )
    order = jnp.where(column == source, 1.0, 0.0).astype(bf16)
    for g in range(pair):
        lo = g * group_rows
        packed_ref[lo : lo + group_rows, :] = dot(
            order, rows_ref[lo : lo + group_rows, :], plain
        ).astype(bf16)
    packed = packed_ref[...]
    pre_gate = dot(packed, gate_ref[...], plain)
    pre_up = dot(packed, up_ref[...], plain)
    gate = jax.nn.sigmoid(pre_gate)
    silu = pre_gate * gate
    silu_ref[...] = silu
    slope_ref[...] = pre_up * gate * (1.0 + pre_gate * (1.0 - gate))
    active_ref[...] = (silu * pre_up).astype(bf16)


def expert_pre(rows, gate, up):
    count, model = rows.shape
    hidden = gate.shape[1]
    size = pair * group_rows
    by_row = lambda width: pl.BlockSpec((size, width), lambda i: (i, 0))
    return pl.pallas_call(
        expert_pre_kernel,
        grid=(count // size,),
        in_specs=[by_row(model), whole((model, hidden)), whole((model, hidden))],
        out_specs=[by_row(model), by_row(hidden), by_row(hidden), by_row(hidden)],
        out_shape=[
            pltpu.HBM((count, model), bf16),
            pltpu.HBM((count, hidden), f32),
            pltpu.HBM((count, hidden), f32),
            pltpu.HBM((count, hidden), bf16),
        ],
        compiler_params=params(),
        cost_estimate=pl.CostEstimate(
            flops=4 * count * model * hidden, transcendentals=0, bytes_accessed=20 << 20
        ),
        name="expert_pre",
    )(held(rows), held(gate), held(up))


def recur_pre_kernel(
    x_ref, y_ref, state_ref, edge_ref, taps_ref, a_ref, i_ref, rate_ref,
    mixed_ref, grad_y_ref, gelu_ref, ahead_ref, product_ref, keep_ref, input_ref, direct_ref,
    first_ref, scratch,
):
    tokens = x_ref.shape[0]
    x = x_ref[...].astype(f32)
    edge = edge_ref[...].astype(f32)
    scratch[5:8, :] = edge[0:3]
    scratch[8 : 8 + tokens, :] = x
    conv_x = taps_ref[0:1, :] * scratch[5 : 5 + tokens, :]
    for j in range(1, 4):
        conv_x = conv_x + taps_ref[j : j + 1, :] * scratch[5 + j : 5 + j + tokens, :]
    conv_b = conv_x.astype(bf16)
    keep = jax.nn.sigmoid(dot(conv_b, a_ref[0], plain))
    gate = jax.nn.sigmoid(dot(conv_b, i_ref[0], plain))
    rate = rate_ref[...]
    decay = jnp.exp(-rate_scale * keep * rate)
    norm = jnp.sqrt(1.0 - decay * decay + floor_square)
    state = state_ref[...].astype(f32)
    scratch[7:8, :] = edge[3:4]
    scratch[8 : 8 + tokens, :] = state
    state_prev = scratch[7 : 7 + tokens, :]
    log_part = decay * state_prev - conv_x * gate * decay * decay / norm
    keep_ref[...] = log_part * (-rate_scale * rate) * keep * (1.0 - keep)
    input_ref[...] = conv_x * norm * gate * (1.0 - gate)
    direct_ref[...] = gate * norm
    y = y_ref[...].astype(f32)
    below = 0.5 * (1.0 + lax.erf(y * inv_root_two))
    gelu = y * below
    gelu_ref[...] = gelu
    mixed_ref[...] = (state * gelu).astype(bf16)
    grad_y_ref[...] = state * (below + y * jnp.exp(-0.5 * y * y) * inv_root_tau)
    scratch[0:tokens, :] = decay
    scratch[tokens : tokens + 8, :] = jnp.ones((8, decay.shape[1]), f32)
    ahead_ref[0] = scratch[1 : 1 + tokens, :]
    length = tokens // segments
    product = None
    for j in reversed(range(length)):
        step = scratch[pl.ds(j + 1, segments, stride=length), :]
        product = step if product is None else step * product
        product_ref[0, pl.ds(j, segments, stride=length), :] = product
    rest = product[1:2]
    for s in range(2, segments):
        rest = rest * product[s : s + 1]
    total = decay[0:1] * product[0:1] * rest
    first_ref[...] = jnp.concatenate(
        [
            decay[0:1],
            total,
            rate_scale * rate * jnp.sum(keep, axis=0, keepdims=True),
            product_ref[0, 0:3, :] * rest,
            keep_ref[0:3, :],
            input_ref[0:3, :],
            direct_ref[0:3, :],
            jnp.zeros_like(total),
        ],
        axis=0,
    )


def recur_pre(in_x, in_y, state, edge, taps, gate_a, gate_x, rate):
    tokens, channels = in_x.shape
    blocks, span = gate_a.shape[:2]
    col = lambda rows: pl.BlockSpec((rows, span), lambda i: (0, i))
    block = pl.BlockSpec((1, span, span), lambda i: (i, 0, 0))
    cube = pl.BlockSpec((1, tokens, span), lambda i: (i, 0, 0))
    big = pltpu.HBM((tokens, channels), f32)
    return pl.pallas_call(
        recur_pre_kernel,
        grid=(blocks,),
        in_specs=[col(tokens), col(tokens), col(tokens), col(4), col(4), block, block, col(1)],
        out_specs=[col(tokens)] * 3 + [cube] * 2 + [col(tokens)] * 3 + [col(16)],
        out_shape=[pltpu.HBM((tokens, channels), bf16)]
        + [big] * 2
        + [pltpu.HBM((blocks, tokens, span), f32)] * 2
        + [big] * 3
        + [pltpu.HBM((16, channels), f32)],
        scratch_shapes=[pltpu.VMEM((tokens + 16, span), f32)],
        compiler_params=params(),
        cost_estimate=pl.CostEstimate(
            flops=2000 * tokens * channels, transcendentals=0, bytes_accessed=8 << 20
        ),
        name="recur_pre",
    )(held(in_x), held(in_y), held(state), held(edge), held(taps), held(gate_a), held(gate_x), held(rate))


def unpack(block, scratch):
    width = block.shape[2] - 128
    parts = []
    for g in range(block.shape[0] // group):
        own = block[g * group : (g + 1) * group]
        parts.append(own[:, :, 0:width].reshape(main_rows, width))
        tiles = own[:, :, width:].reshape(128, 128).astype(f32)
        parts.append(unpack_extras(tiles, scratch).astype(bf16))
    return jnp.concatenate(parts, axis=0)


def pack_into(out_ref, values, scratch):
    width = values.shape[1]
    for g in range(out_ref.shape[0] // group):
        lo = g * group_rows
        out_ref[g * group : (g + 1) * group, :, 0:width] = (
            values[lo : lo + main_rows].astype(bf16).reshape(group, main, width)
        )
        tiles = pack_extras(values[lo + main_rows : lo + group_rows], scratch)
        out_ref[g * group : (g + 1) * group, :, width:] = tiles.astype(bf16).reshape(
            group, main, 128
        )


def near_by(value):
    return pltpu.with_memory_space_constraint(value, pltpu.VMEM)


def load_beside(copies):
    @pl.when(pl.program_id(0) == 0)
    def _():
        for copy in copies:
            copy.start()

    return copies


def finish(copies):
    @pl.when(pl.program_id(0) == pl.num_programs(0) - 1)
    def _():
        for copy in copies:
            copy.wait()


anywhere = pl.BlockSpec(memory_space=pl.ANY)
resident = pl.BlockSpec(memory_space=pltpu.VMEM)


def near_kernel(core_ref, block_ref, down_ref, down_all, part_ref, down_next, scratch, sems):
    half = down_ref.shape[1]
    other = pl.multiple_of((1 - core_ref[0]) * half, half)
    copies = load_beside(
        [pltpu.make_async_copy(down_all.at[:, pl.ds(other, half)], down_next, sems.at[0])]
    )
    rows = unpack(block_ref[...], scratch)
    part_ref[...] = dot(rows, down_ref[...], inner)
    finish(copies)


def near(core, arrived, down):
    experts, _, wide = arrived.shape
    half = wide - 128
    hidden = down.shape[0]
    count = experts * (main + extra)
    size = all_groups * group_rows
    return pl.pallas_call(
        near_kernel,
        grid_spec=pltpu.PrefetchScalarGridSpec(
            num_scalar_prefetch=1,
            grid=(count // size,),
            in_specs=[
                pl.BlockSpec((all_groups * group, main, wide), lambda i, c: (i, 0, 0)),
                pl.BlockSpec((hidden, half), lambda i, c: (0, c[0])),
                anywhere,
            ],
            out_specs=[pl.BlockSpec((size, hidden), lambda i, c: (i, 0)), anywhere],
            scratch_shapes=[pltpu.VMEM((128, 128), f32), pltpu.SemaphoreType.DMA((1,))],
        ),
        out_shape=[
            jax.ShapeDtypeStruct((count, hidden), f32),
            pltpu.VMEM((hidden, half), bf16),
        ],
        compiler_params=params(),
        cost_estimate=pl.CostEstimate(
            flops=2 * count * half * hidden, transcendentals=0, bytes_accessed=9 << 20
        ),
        name="near",
    )(core, arrived, held(down), held(down))


def far_kernel(
    core_ref, block_ref, down_ref, part_ref, silu_ref, slope_ref, gate_all, up_all,
    adj_ref, gate_next, up_next, scratch, sems,
):
    half = gate_next.shape[0]
    own = pl.multiple_of(core_ref[0] * half, half)
    copies = load_beside(
        [
            pltpu.make_async_copy(gate_all.at[pl.ds(own, half)], gate_next, sems.at[0]),
            pltpu.make_async_copy(up_all.at[pl.ds(own, half)], up_next, sems.at[1]),
        ]
    )
    rows = unpack(block_ref[...], scratch)
    grad = part_ref[...] + dot(rows, down_ref[...], inner)
    hidden = grad.shape[1]
    adj_ref[:, 0:hidden] = (grad * slope_ref[...]).astype(bf16)
    adj_ref[:, hidden:] = (grad * silu_ref[...]).astype(bf16)
    finish(copies)


def far(core, arrived, down_half, part, silu, slope, gate, up):
    experts, _, _ = arrived.shape
    hidden, half = down_half.shape
    count = experts * (main + extra)
    size = all_groups * group_rows
    by_row = lambda width: pl.BlockSpec((size, width), lambda i, c: (i, 0))
    return pl.pallas_call(
        far_kernel,
        grid_spec=pltpu.PrefetchScalarGridSpec(
            num_scalar_prefetch=1,
            grid=(count // size,),
            in_specs=[
                resident,
                resident,
                resident,
                resident,
                resident,
                anywhere,
                anywhere,
            ],
            out_specs=[by_row(2 * hidden), anywhere, anywhere],
            scratch_shapes=[pltpu.VMEM((128, 128), f32), pltpu.SemaphoreType.DMA((2,))],
        ),
        out_shape=[
            jax.ShapeDtypeStruct((count, 2 * hidden), bf16),
            pltpu.VMEM((half, hidden), bf16),
            pltpu.VMEM((half, hidden), bf16),
        ],
        compiler_params=params(),
        cost_estimate=pl.CostEstimate(
            flops=2 * count * half * hidden, transcendentals=0, bytes_accessed=16 << 20
        ),
        name="far",
    )(core, arrived, near_by(down_half), part, silu, slope, held(gate), held(up))


def back_rows(adj, gate, up):
    hidden = gate.shape[1]
    back = dot(adj[:, 0:hidden], gate, inner) + dot(adj[:, hidden:], up, inner)
    return back.astype(bf16)


def back_own_kernel(
    core_ref, adj_ref, gate_ref, up_ref, gate_all, up_all, back_ref, gate_next, up_next, sems
):
    half = gate_next.shape[0]
    own = pl.multiple_of(core_ref[0] * half, half)
    copies = load_beside(
        [
            pltpu.make_async_copy(gate_all.at[pl.ds(own, half)], gate_next, sems.at[0]),
            pltpu.make_async_copy(up_all.at[pl.ds(own, half)], up_next, sems.at[1]),
        ]
    )
    back_ref[...] = back_rows(adj_ref[...], gate_ref[...], up_ref[...])
    finish(copies)


def back_own(core, adj, gate_half, up_half, gate_peer, up_peer):
    count = adj.shape[0]
    half, hidden = gate_half.shape
    size = all_groups * group_rows
    by_row = lambda width: pl.BlockSpec((size, width), lambda i, c: (i, 0))
    return pl.pallas_call(
        back_own_kernel,
        grid_spec=pltpu.PrefetchScalarGridSpec(
            num_scalar_prefetch=1,
            grid=(count // size,),
            in_specs=[
                resident,
                resident,
                resident,
                anywhere,
                anywhere,
            ],
            out_specs=[by_row(half), anywhere, anywhere],
            scratch_shapes=[pltpu.SemaphoreType.DMA((2,))],
        ),
        out_shape=[
            jax.ShapeDtypeStruct((count, half), bf16),
            pltpu.VMEM((half, hidden), bf16),
            pltpu.VMEM((half, hidden), bf16),
        ],
        compiler_params=params(),
        cost_estimate=pl.CostEstimate(
            flops=4 * count * half * hidden, transcendentals=0, bytes_accessed=7 << 20
        ),
        name="back_own",
    )(core, adj, near_by(gate_half), near_by(up_half), held(gate_peer), held(up_peer))


def back_sum_kernel(adj_ref, own_ref, gate_ref, up_ref, out_ref, packed, scratch, sems):
    parts = sems.shape[0]
    size = adj_ref.shape[0] // parts
    blocks = packed.shape[0] // parts
    copies = []
    for k in range(parts):
        rows = slice(k * size, (k + 1) * size)
        peer = back_rows(adj_ref[rows, :], gate_ref[...], up_ref[...])
        part = packed.at[k * blocks : (k + 1) * blocks]
        pack_into(part, own_ref[rows, :].astype(f32) + peer.astype(f32), scratch)
        copies.append(
            pltpu.make_async_copy(part, out_ref.at[k * blocks : (k + 1) * blocks], sems.at[k])
        )
        copies[-1].start()
    for copy in copies:
        copy.wait()


def back_sum(adj, own, gate_half, up_half, shape):
    count = adj.shape[0]
    half, hidden = gate_half.shape
    return pl.pallas_call(
        back_sum_kernel,
        grid=(1,),
        in_specs=[resident] * 4,
        out_specs=anywhere,
        scratch_shapes=[
            pltpu.VMEM(shape, bf16),
            pltpu.VMEM((128, 128), f32),
            pltpu.SemaphoreType.DMA((sum_parts,)),
        ],
        out_shape=pltpu.HBM(shape, bf16),
        compiler_params=params(),
        cost_estimate=pl.CostEstimate(
            flops=4 * count * half * hidden, transcendentals=0, bytes_accessed=7 << 20
        ),
        name="back_sum",
    )(adj, own, near_by(gate_half), near_by(up_half))


def grad_in_kernel(packed_ref, adj_ref, gate_ref, up_ref):
    grad = dot(packed_ref[...], adj_ref[...], outer).astype(bf16)
    hidden = gate_ref.shape[1]
    gate_ref[...] = grad[:, 0:hidden]
    up_ref[...] = grad[:, hidden:]


def grad_in(packed, adj):
    count, model = packed.shape
    hidden = adj.shape[1] // 2
    size = 512
    out = pl.BlockSpec((size, hidden), lambda i: (i, 0))
    return pl.pallas_call(
        grad_in_kernel,
        grid=(model // size,),
        in_specs=[pl.BlockSpec((count, size), lambda i: (0, i)), whole((count, 2 * hidden))],
        out_specs=[out, out],
        out_shape=[jax.ShapeDtypeStruct((model, hidden), bf16)] * 2,
        compiler_params=params(),
        cost_estimate=pl.CostEstimate(
            flops=4 * count * model * hidden, transcendentals=0, bytes_accessed=11 << 20
        ),
        name="grad_in",
    )(held(packed), held(adj))


def grad_down_kernel(core_ref, active_ref, near_ref, far_ref, out_ref, scratch):
    active = active_ref[...]

    @pl.when(pl.program_id(0) == 0)
    def _():
        out_ref[...] = dot(active, unpack(near_ref[...], scratch), outer).astype(bf16)

    @pl.when(pl.program_id(0) == 1)
    def _():
        out_ref[...] = dot(active, unpack(far_ref[...], scratch), outer).astype(bf16)


def grad_down_of(core, active, arrived, arrived_far):
    count, hidden = active.shape
    half = arrived.shape[2] - 128
    return pl.pallas_call(
        grad_down_kernel,
        grid_spec=pltpu.PrefetchScalarGridSpec(
            num_scalar_prefetch=1,
            grid=(2,),
            in_specs=[whole((count, hidden)), whole(arrived.shape), whole(arrived.shape)],
            out_specs=pl.BlockSpec((hidden, half), lambda i, c: (0, i + c[0] - 2 * i * c[0])),
            scratch_shapes=[pltpu.VMEM((128, 128), f32)],
        ),
        out_shape=jax.ShapeDtypeStruct((hidden, 2 * half), bf16),
        compiler_params=params(),
        cost_estimate=pl.CostEstimate(
            flops=4 * count * half * hidden, transcendentals=0, bytes_accessed=9 << 20
        ),
        name="grad_down",
    )(core, held(active), held(arrived), held(arrived_far))


def combine_kernel(
    core_ref, block_ref, target_ref, cot_ref, weight_all, mixed_all,
    out_ref, weight_next, mixed_next, scratch, sems,
):
    half = weight_next.shape[0]
    own = pl.multiple_of(core_ref[0] * half, half)
    copies = load_beside(
        [
            pltpu.make_async_copy(weight_all.at[pl.ds(own, half)], weight_next, sems.at[0]),
            pltpu.make_async_copy(mixed_all, mixed_next, sems.at[1]),
        ]
    )
    tokens = cot_ref.shape[0]
    rows = unpack(block_ref[...], scratch)
    place = lax.broadcasted_iota(jnp.int32, (tokens, rows.shape[0]), 1)
    chosen = jnp.where(
        (place == target_ref[:, 0:1]) | (place == target_ref[:, 1:2]), 1.0, 0.0
    ).astype(bf16)
    out_ref[...] = (cot_ref[...].astype(f32) + dot(chosen, rows, plain)).astype(bf16)
    finish(copies)


def combine(core, returned, target, cotangent, weight, mixed):
    half = returned.shape[2] - 128
    tokens = cotangent.shape[0]
    return pl.pallas_call(
        combine_kernel,
        grid_spec=pltpu.PrefetchScalarGridSpec(
            num_scalar_prefetch=1,
            grid=(1,),
            in_specs=[
                resident,
                whole((tokens, 8)),
                pl.BlockSpec((tokens, half), lambda i, c: (0, c[0])),
                anywhere,
                anywhere,
            ],
            out_specs=[whole((tokens, half)), anywhere, anywhere],
            scratch_shapes=[pltpu.VMEM((128, 128), f32), pltpu.SemaphoreType.DMA((2,))],
        ),
        out_shape=[
            jax.ShapeDtypeStruct((tokens, half), bf16),
            pltpu.VMEM((half, weight.shape[1]), bf16),
            pltpu.VMEM(mixed.shape, bf16),
        ],
        compiler_params=params(),
        name="combine",
    )(core, returned, held(target), held(cotangent), held(weight), held(mixed))


def write_shares(ref, values):
    pieces = values.astype(bf16).reshape(ref.shape[0], 4, 8, values.shape[1])
    channels = values.shape[1]
    for k in range(4):
        ref[:, :, channels * k : channels * (k + 1)] = pieces[:, k]


def own_kernel(
    core_ref, own_ref, weight_ref, mixed_ref, weight_all, grad_ref, share_out, weight_next, share, sems
):
    half = weight_next.shape[0]
    other = pl.multiple_of((1 - core_ref[0]) * half, half)
    copies = load_beside(
        [pltpu.make_async_copy(weight_all.at[pl.ds(other, half)], weight_next, sems.at[1])]
    )
    owners = share.shape[0]
    at = pl.ds(pl.multiple_of(core_ref[0] * owners, owners), owners)
    own = own_ref[...]
    write_shares(share, dot(own, mixed_ref[...], outer))
    copy = pltpu.make_async_copy(share, share_out.at[at, :, pl.ds(0, share.shape[2])], sems.at[0])
    copy.start()
    grad_ref[...] = dot(own, weight_ref[...], plain)
    copy.wait()
    finish(copies)


def own_part(core, own, weight_half, mixed, weight, owners):
    tokens, half = own.shape
    channels = mixed.shape[1]
    return pl.pallas_call(
        own_kernel,
        grid_spec=pltpu.PrefetchScalarGridSpec(
            num_scalar_prefetch=1,
            grid=(1,),
            in_specs=[
                resident,
                resident,
                resident,
                anywhere,
            ],
            out_specs=[whole((tokens, channels)), anywhere, anywhere],
            scratch_shapes=[
                pltpu.VMEM((owners // 2, 8, 4 * channels), bf16),
                pltpu.SemaphoreType.DMA((2,)),
            ],
        ),
        out_shape=[
            jax.ShapeDtypeStruct((tokens, channels), f32),
            pltpu.HBM((owners, 8, 4 * channels + 128), bf16),
            pltpu.VMEM((half, channels), bf16),
        ],
        compiler_params=params(),
        cost_estimate=pl.CostEstimate(
            flops=4 * tokens * half * channels, transcendentals=0, bytes_accessed=4 << 20
        ),
        name="own_part",
    )(core, own, near_by(weight_half), near_by(mixed), held(weight))


def segment_scan(values, ahead_ref, state_grad, local):
    blocks, tokens, span = state_grad.shape
    length = tokens // segments
    for b in range(blocks):
        state_grad[b] = values[:, span * b : span * (b + 1)]
    last = [None] * blocks
    for j in reversed(range(length)):
        at = pl.ds(j, segments, stride=length)
        for b in range(blocks):
            here = state_grad[b, at, :]
            last[b] = here if last[b] is None else here + ahead_ref[b, at, :] * last[b]
            local[b, at, :] = last[b]
    return last


def scan_kernel(
    core_ref, peer_ref, weight_ref, mixed_ref, part_ref, gelu_ref, ahead_ref, product_ref, first_ref,
    share_in, share_out, head_ref,
    state_grad, local, share, lines, sems,
):
    owners = share.shape[0]
    other = pl.ds(pl.multiple_of((1 - core_ref[0]) * owners, owners), owners)
    columns = share.shape[2]
    peer = peer_ref[...]
    grad = part_ref[...] + dot(peer, weight_ref[...], plain)
    write_shares(share, dot(peer, mixed_ref[...], outer))
    main_copy = pltpu.make_async_copy(share, share_out.at[other, :, pl.ds(0, columns)], sems.at[0])
    main_copy.start()
    values = grad * gelu_ref[...]
    blocks, tokens, _ = state_grad.shape
    length = tokens // segments
    last = segment_scan(values, ahead_ref, state_grad, local)
    tiles = []
    for b in range(blocks):
        at = slice(128 * b, 128 * (b + 1))
        value = last[b]
        product = product_ref[b, pl.ds(0, segments, stride=length), :]
        carry = value[segments - 1 : segments]
        for s in reversed(range(1, segments - 1)):
            carry = value[s : s + 1] + product[s : s + 1] * carry
        ends = local[b, 0:3, :] + product_ref[b, 0:3, :] * carry
        tiles.append(first_ref[0:1, at] * ends[0:1])
        head_ref[:, at] = jnp.concatenate(
            [ends, first_ref[3:15, at], jnp.zeros((1, 128), f32)], axis=0
        )
    power = [first_ref[2:3, 128 * b : 128 * (b + 1)] for b in range(blocks)]
    line = jnp.concatenate(power + tiles, axis=0).astype(bf16)
    lines[...] = jnp.broadcast_to(line[None], lines.shape)
    line_copy = pltpu.make_async_copy(lines, share_out.at[:, :, pl.ds(columns, 128)], sems.at[1])
    line_copy.start()
    main_copy.wait()
    line_copy.wait()


def scan(core, peer, weight, mixed, part, shares, gelu, ahead, product, first):
    tokens, half = peer.shape
    channels = weight.shape[1]
    owners = shares.shape[0]
    return pl.pallas_call(
        scan_kernel,
        grid_spec=pltpu.PrefetchScalarGridSpec(
            num_scalar_prefetch=1,
            grid=(1,),
            in_specs=[
                resident,
                resident,
                resident,
                resident,
                resident,
                resident,
                resident,
                resident,
                anywhere,
            ],
            out_specs=[anywhere, whole((16, channels))],
            scratch_shapes=[
                pltpu.VMEM(ahead.shape, f32),
                pltpu.VMEM(ahead.shape, f32),
                pltpu.VMEM((owners // 2, 8, 4 * channels), bf16),
                pltpu.VMEM((owners, 8, 128), bf16),
                pltpu.SemaphoreType.DMA((2,)),
            ],
        ),
        out_shape=[pltpu.HBM(shares.shape, bf16), pltpu.HBM((16, channels), f32)],
        input_output_aliases={9: 0},
        compiler_params=params(),
        cost_estimate=pl.CostEstimate(
            flops=4 * tokens * half * channels, transcendentals=0, bytes_accessed=9 << 20
        ),
        name="scan",
    )(
        core, peer, near_by(weight), near_by(mixed), part, gelu, ahead, product, first, held(shares)
    )


def local_kernel(
    core_ref, peer_ref, weight_ref, part_ref, slope_ref, gelu_ref, ahead_ref,
    grad_y_ref, local_ref, state_grad,
):
    grad = part_ref[...] + dot(peer_ref[...], weight_ref[...], plain)
    grad_y_ref[...] = grad * slope_ref[...]
    segment_scan(grad * gelu_ref[...], ahead_ref, state_grad, local_ref)


def local_scan(core, peer, weight, part, slope, gelu, ahead):
    tokens, half = peer.shape
    channels = weight.shape[1]
    return pl.pallas_call(
        local_kernel,
        grid_spec=pltpu.PrefetchScalarGridSpec(
            num_scalar_prefetch=1,
            grid=(1,),
            in_specs=[
                whole((tokens, half)),
                pl.BlockSpec((half, channels), lambda i, c: (1 - c[0], 0)),
                whole((tokens, channels)),
                whole((tokens, channels)),
                whole((tokens, channels)),
                whole(ahead.shape),
            ],
            out_specs=[whole((tokens, channels)), whole(ahead.shape)],
            scratch_shapes=[pltpu.VMEM(ahead.shape, f32)],
        ),
        out_shape=[pltpu.HBM((tokens, channels), f32), pltpu.HBM(ahead.shape, f32)],
        compiler_params=params(),
        cost_estimate=pl.CostEstimate(
            flops=2 * tokens * half * channels, transcendentals=0, bytes_accessed=9 << 20
        ),
        name="local_scan",
    )(core, held(peer), held(weight), held(part), held(slope), held(gelu), held(ahead))


def tail_kernel(
    place_ref, share_ref, head_ref, taps_ref, a_ref, i_ref, *rest,
):
    sources, (out_hbm, project_ref), stores = rest[0:5], rest[5:7], rest[7:]
    local_ref, product_ref, keep_ref, input_ref, direct_ref = buffers = stores[0:5]
    adjoint, grads, out, in_sems, out_sems = stores[5:]
    blocks, tokens, span = local_ref.shape
    length = tokens // segments
    place = place_ref[0]

    def column(ref, c):
        return ref.at[c] if len(ref.shape) == 3 else ref.at[:, pl.ds(span * c, span)]

    copies = [
        [
            pltpu.make_async_copy(column(source, c), column(buffer, c), in_sems.at[c, k])
            for k, (source, buffer) in enumerate(zip(sources, buffers))
        ]
        for c in range(blocks)
    ]
    for group_copies in copies:
        for copy in group_copies:
            copy.start()

    own = jnp.zeros((4, span), f32)
    beyond = jnp.zeros((4, span), f32)
    columns = share_ref.shape[2] - 128
    channels = columns // 4
    summed = jnp.zeros((8, columns), f32)
    for j in reversed(range(share_ref.shape[0])):
        share = share_ref[j].astype(f32)
        summed = summed + share[:, 0:columns]
        line = share[:, columns:]
        decay = jnp.exp(-line[0:4])
        own = jnp.where(j > place, line[4:8] + decay * own, own)
        beyond = jnp.where(j > place + 1, line[4:8] + decay * beyond, beyond)

    for k in range(4):
        project_ref[8 * k : 8 * (k + 1), :] = summed[:, channels * k : channels * (k + 1)]
    results = []
    for c in range(blocks):
        at = slice(span * c, span * (c + 1))

        def conv_grad(value, keep, gate, direct):
            keep = (value * keep).astype(bf16)
            gate = (value * gate).astype(bf16)
            return value * direct + dot(keep, a_ref[c], inner) + dot(gate, i_ref[c], inner)

        for copy in copies[c]:
            copy.wait()
        carry = own[c : c + 1]
        for s in reversed(range(segments)):
            rows = slice(s * length, (s + 1) * length)
            piece = local_ref[c, rows, :] + product_ref[c, rows, :] * carry
            adjoint[rows, :] = piece
            carry = piece[0:1]
        grads[0:tokens, :] = conv_grad(
            adjoint[...], keep_ref[:, at], input_ref[:, at], direct_ref[:, at]
        )
        head = head_ref[:, at]
        spare = jnp.zeros((5, span), f32)
        three = lambda k: jnp.concatenate([head[3 * k : 3 * k + 3], spare], axis=0)
        later = three(0) + three(1) * beyond[c : c + 1]
        grads[tokens : tokens + 8, :] = conv_grad(later, three(2), three(3), three(4))
        total = taps_ref[0:1, at] * grads[3 : 3 + tokens, :]
        for j in range(1, 4):
            total = total + taps_ref[j : j + 1, at] * grads[3 - j : 3 - j + tokens, :]
        out[:, at] = total
        results.append(
            pltpu.make_async_copy(column(out, c), column(out_hbm, c), out_sems.at[c])
        )
        results[-1].start()
    for copy in results:
        copy.wait()


def tail(place, shares, head, local, product, keep, gate, direct, gate_a, gate_x, taps):
    blocks, tokens, span = local.shape
    channels = blocks * span
    rows = shares.shape[1]
    sources = (local, product, keep, gate, direct)
    return pl.pallas_call(
        tail_kernel,
        grid_spec=pltpu.PrefetchScalarGridSpec(
            num_scalar_prefetch=1,
            grid=(1,),
            in_specs=[
                resident,
                resident,
                whole((4, channels)),
                whole(gate_a.shape),
                whole(gate_x.shape),
            ]
            + [anywhere] * 5,
            out_specs=[anywhere, whole((4 * rows, channels))],
            scratch_shapes=[pltpu.VMEM(value.shape, f32) for value in sources]
            + [
                pltpu.VMEM((tokens, span), f32),
                pltpu.VMEM((tokens + 8, span), f32),
                pltpu.VMEM((tokens, channels), f32),
                pltpu.SemaphoreType.DMA((blocks, 5)),
                pltpu.SemaphoreType.DMA((blocks,)),
            ],
        ),
        out_shape=[
            pltpu.HBM((tokens, channels), f32),
            pltpu.HBM((4 * rows, channels), f32),
        ],
        compiler_params=params(),
        name="tail",
    )(place, shares, head, held(taps), held(gate_a), held(gate_x), *(held(v) for v in sources))


def exchange(value, axis):
    return lax.all_to_all(value, axis, split_axis=0, concat_axis=0, tiled=True)


def swapped(value):
    return lax.ppermute(value, "tp", [(0, 1), (1, 0)])


def shifted(value, axis, by):
    devices = lax.axis_size(axis)
    pairs = [(i, i + by) for i in range(devices) if 0 <= i + by < devices]
    return lax.ppermute(value, axis, pairs)


def body(
    cotangent,
    routes,
    route_weight,
    expert_rows,
    gate_w,
    up_w,
    down_w,
    in_x,
    in_y,
    state,
    conv_taps,
    gate_a,
    gate_x,
    decay_rate,
    out_weight,
):
    tokens = cotangent.shape[0]
    experts = lax.axis_size("sp")
    core = lax.axis_index("tp").astype(jnp.int32).reshape(1)
    taps = conv_taps.shape[0]

    place = lax.axis_index("sp").astype(jnp.int32).reshape(1)

    edge = shifted(
        jnp.concatenate([in_x[tokens - taps + 1 :], state[tokens - 1 :]], axis=0), "sp", 1
    )
    outgoing, target = send(core, routes.T, route_weight.T, cotangent, experts)
    arrived = exchange(outgoing, "sp")
    target = target.T

    gate_peer = swapped(gate_w[0])
    up_peer = swapped(up_w[0])
    packed, silu, slope, active = expert_pre(expert_rows[0], gate_w[0], up_w[0])
    mixed, y_slope, gelu, ahead, product, keep_part, input_part, direct, first = recur_pre(
        in_x, in_y, state, edge, conv_taps, gate_a, gate_x, decay_rate[None]
    )

    arrived_far = swapped(arrived)
    part, down_half = near(core, arrived, down_w[0])
    adj, gate_half, up_half = far(
        core, arrived_far, down_half, part, silu, slope, gate_w[0], up_w[0]
    )
    adj_peer = swapped(adj)
    own, gate_half, up_half = back_own(core, adj, gate_half, up_half, gate_peer, up_peer)
    returning = back_sum(adj_peer, own, gate_half, up_half, arrived.shape)
    returned = exchange(returning, "sp")

    grad_gate, grad_up = grad_in(packed, adj)
    grad_down = grad_down_of(core, active, arrived, arrived_far)

    stream_own, weight_half, mixed_here = combine(
        core, returned, target, cotangent, out_weight, mixed
    )
    stream_peer = swapped(stream_own)
    part, shares, weight_half = own_part(
        core, stream_own, weight_half, mixed_here, out_weight, experts
    )
    outgoing, head = scan(
        core, stream_peer, weight_half, mixed_here, part, shares, gelu, ahead, product, first
    )
    grad_y, local = local_scan(core, stream_peer, out_weight, part, y_slope, gelu, ahead)
    head = shifted(head, "sp", -1)
    shares = exchange(outgoing, "sp")
    grad_x, grad_proj = tail(
        place, shares, head, local, product, keep_part, input_part, direct,
        gate_a, gate_x, conv_taps,
    )
    return (grad_gate[None], grad_up[None], grad_down[None], grad_proj, grad_x, grad_y)


def solution(mesh):
    in_specs = (
        P("sp", None),
        P("sp", None),
        P("sp", None),
        P("sp", None, None),
        P("sp", None, "tp"),
        P("sp", None, "tp"),
        P("sp", "tp", None),
        P("sp", "tp"),
        P("sp", "tp"),
        P("sp", "tp"),
        P(None, "tp"),
        P("tp", None, None),
        P("tp", None, None),
        P("tp"),
        P(None, "tp"),
    )
    out_specs = (
        P("sp", None, "tp"),
        P("sp", None, "tp"),
        P("sp", "tp", None),
        P("sp", "tp"),
        P("sp", "tp"),
        P("sp", "tp"),
    )
    return jax.shard_map(body, mesh=mesh, in_specs=in_specs, out_specs=out_specs, check_vma=False)
```

```python
import jax
import jax.numpy as jnp
from jax import lax
from jax.experimental import pallas as pl
from jax.experimental.pallas import tpu as pltpu
from jax.sharding import PartitionSpec as P

rate_scale = 8.0
floor_square = 0.01
inv_root_two = 0.7071067811865476
inv_root_tau = 0.3989422804014327

f32 = jnp.float32
bf16 = jnp.bfloat16
inner = (((1,), (1,)), ((), ()))
outer = (((0,), (0,)), ((), ()))
plain = (((1,), (0,)), ((), ()))

group = 8
main = 16
extra = 2
main_rows = group * main
group_rows = group * (main + extra)
segments = 8


def dot(a, b, dims):
    return lax.dot_general(a, b, dims, preferred_element_type=f32)


def params(n=1, mb=32):
    return pltpu.CompilerParams(dimension_semantics=("arbitrary",) * n, vmem_limit_bytes=mb << 20)


def held(value):
    return pltpu.with_memory_space_constraint(value, pltpu.HBM)


def whole(shape):
    return pl.BlockSpec(shape, lambda *_: (0,) * len(shape))


def pack_extras(rows, scratch):
    for j in range(8):
        scratch[pl.ds(j, group * extra, stride=8), :] = rows[:, 128 * j : 128 * (j + 1)]
    return scratch[...]


def unpack_extras(tiles, scratch):
    scratch[...] = tiles
    return jnp.concatenate(
        [scratch[pl.ds(j, group * extra, stride=8), :] for j in range(8)], axis=1
    )


def send_kernel(core_ref, routes_ref, weight_ref, cot_ref, out_ref, target_ref, slot, scratch):
    step = pl.program_id(0)
    tokens = cot_ref.shape[0]
    experts = pl.num_programs(0) * out_ref.shape[0]

    @pl.when(step == 0)
    def _():
        first = routes_ref[0:1, :]
        second = routes_ref[1:2, :]
        expert = lax.broadcasted_iota(jnp.int32, (experts, tokens), 0)
        hit_first = (expert == first).astype(f32)
        hit_second = (expert == second).astype(f32)
        earlier = (
            lax.broadcasted_iota(jnp.int32, (tokens, tokens), 0)
            < lax.broadcasted_iota(jnp.int32, (tokens, tokens), 1)
        ).astype(f32)
        before = dot((hit_first + hit_second).astype(bf16), earlier.astype(bf16), plain)
        place_first = jnp.sum(before * hit_first, axis=0, keepdims=True).astype(jnp.int32)
        place_second = jnp.sum(before * hit_second, axis=0, keepdims=True).astype(jnp.int32)
        place_second = place_second + (first == second).astype(jnp.int32)
        for k, (name, place) in enumerate(((first, place_first), (second, place_second))):
            base = group_rows * (name >> 3)
            inside = name & 7
            slot[k : k + 1, :] = base + jnp.where(
                place < main, main * inside + place, main_rows + extra * inside + place - main
            )
        target_ref[...] = jnp.concatenate(
            [slot[0:2, :], jnp.zeros((6, tokens), jnp.int32)], axis=0
        )

    size = out_ref.shape[0] // group * group_rows
    rows = lax.broadcasted_iota(jnp.int32, (size, tokens), 0) + step * size
    hit_first = rows == slot[0:1, :]
    hit_second = rows == slot[1:2, :]
    chosen = jnp.where(hit_first | hit_second, 1.0, 0.0).astype(bf16)
    weight = jnp.sum(
        jnp.where(hit_first, weight_ref[0:1, :], 0.0)
        + jnp.where(hit_second, weight_ref[1:2, :], 0.0),
        axis=1,
        keepdims=True,
    )
    values = dot(chosen, cot_ref[...], plain) * weight
    pack_into(out_ref, values, scratch)


def send(core, routes, weight, cotangent, experts):
    tokens, model = cotangent.shape
    half = model // 2
    return pl.pallas_call(
        send_kernel,
        grid_spec=pltpu.PrefetchScalarGridSpec(
            num_scalar_prefetch=1,
            grid=(experts // (send_groups * group),),
            in_specs=[
                whole((2, tokens)),
                whole((2, tokens)),
                pl.BlockSpec((tokens, half), lambda i, c: (0, c[0])),
            ],
            out_specs=[
                pl.BlockSpec((send_groups * group, main, half + 128), lambda i, c: (i, 0, 0)),
                whole((8, tokens)),
            ],
            scratch_shapes=[pltpu.VMEM((8, tokens), jnp.int32), pltpu.VMEM((128, 128), f32)],
        ),
        out_shape=[
            pltpu.HBM((experts, main, half + 128), bf16),
            jax.ShapeDtypeStruct((8, tokens), jnp.int32),
        ],
        compiler_params=params(),
        name="send",
    )(core, held(routes), held(weight), held(cotangent))


pair = 2
send_groups = 4
all_groups = 8
sum_parts = 4


def expert_pre_kernel(rows_ref, gate_ref, up_ref, packed_ref, silu_ref, slope_ref, active_ref):
    out_row = lax.broadcasted_iota(jnp.int32, (group_rows, group_rows), 0)
    column = lax.broadcasted_iota(jnp.int32, (group_rows, group_rows), 1)
    late = out_row - main_rows
    source = jnp.where(
        out_row < main_rows,
        (main + extra) * (out_row >> 4) + (out_row & 15),
        (main + extra) * (late >> 1) + main + (late & 1),
    )
    order = jnp.where(column == source, 1.0, 0.0).astype(bf16)
    for g in range(pair):
        lo = g * group_rows
        packed_ref[lo : lo + group_rows, :] = dot(
            order, rows_ref[lo : lo + group_rows, :], plain
        ).astype(bf16)
    packed = packed_ref[...]
    pre_gate = dot(packed, gate_ref[...], plain)
    pre_up = dot(packed, up_ref[...], plain)
    gate = jax.nn.sigmoid(pre_gate)
    silu = pre_gate * gate
    silu_ref[...] = silu
    slope_ref[...] = pre_up * gate * (1.0 + pre_gate * (1.0 - gate))
    active_ref[...] = (silu * pre_up).astype(bf16)


def expert_pre(rows, gate, up):
    count, model = rows.shape
    hidden = gate.shape[1]
    size = pair * group_rows
    by_row = lambda width: pl.BlockSpec((size, width), lambda i: (i, 0))
    return pl.pallas_call(
        expert_pre_kernel,
        grid=(count // size,),
        in_specs=[by_row(model), whole((model, hidden)), whole((model, hidden))],
        out_specs=[by_row(model), by_row(hidden), by_row(hidden), by_row(hidden)],
        out_shape=[
            pltpu.HBM((count, model), bf16),
            pltpu.HBM((count, hidden), f32),
            pltpu.HBM((count, hidden), f32),
            pltpu.HBM((count, hidden), bf16),
        ],
        compiler_params=params(),
        cost_estimate=pl.CostEstimate(
            flops=4 * count * model * hidden, transcendentals=0, bytes_accessed=20 << 20
        ),
        name="expert_pre",
    )(held(rows), held(gate), held(up))


def recur_pre_kernel(
    x_ref, y_ref, state_ref, edge_ref, taps_ref, a_ref, i_ref, rate_ref,
    mixed_ref, grad_y_ref, gelu_ref, ahead_ref, product_ref, keep_ref, input_ref, direct_ref,
    first_ref, scratch,
):
    tokens = x_ref.shape[0]
    x = x_ref[...].astype(f32)
    edge = edge_ref[...].astype(f32)
    scratch[5:8, :] = edge[0:3]
    scratch[8 : 8 + tokens, :] = x
    conv_x = taps_ref[0:1, :] * scratch[5 : 5 + tokens, :]
    for j in range(1, 4):
        conv_x = conv_x + taps_ref[j : j + 1, :] * scratch[5 + j : 5 + j + tokens, :]
    conv_b = conv_x.astype(bf16)
    keep = jax.nn.sigmoid(dot(conv_b, a_ref[0], plain))
    gate = jax.nn.sigmoid(dot(conv_b, i_ref[0], plain))
    rate = rate_ref[...]
    decay = jnp.exp(-rate_scale * keep * rate)
    norm = jnp.sqrt(1.0 - decay * decay + floor_square)
    state = state_ref[...].astype(f32)
    scratch[7:8, :] = edge[3:4]
    scratch[8 : 8 + tokens, :] = state
    state_prev = scratch[7 : 7 + tokens, :]
    log_part = decay * state_prev - conv_x * gate * decay * decay / norm
    keep_ref[...] = log_part * (-rate_scale * rate) * keep * (1.0 - keep)
    input_ref[...] = conv_x * norm * gate * (1.0 - gate)
    direct_ref[...] = gate * norm
    y = y_ref[...].astype(f32)
    below = 0.5 * (1.0 + lax.erf(y * inv_root_two))
    gelu = y * below
    gelu_ref[...] = gelu
    mixed_ref[...] = (state * gelu).astype(bf16)
    grad_y_ref[...] = state * (below + y * jnp.exp(-0.5 * y * y) * inv_root_tau)
    scratch[0:tokens, :] = decay
    scratch[tokens : tokens + 8, :] = jnp.ones((8, decay.shape[1]), f32)
    ahead_ref[0] = scratch[1 : 1 + tokens, :]
    length = tokens // segments
    product = None
    for j in reversed(range(length)):
        step = scratch[pl.ds(j + 1, segments, stride=length), :]
        product = step if product is None else step * product
        product_ref[0, pl.ds(j, segments, stride=length), :] = product
    rest = product[1:2]
    for s in range(2, segments):
        rest = rest * product[s : s + 1]
    total = decay[0:1] * product[0:1] * rest
    first_ref[...] = jnp.concatenate(
        [
            decay[0:1],
            total,
            rate_scale * rate * jnp.sum(keep, axis=0, keepdims=True),
            product_ref[0, 0:3, :] * rest,
            keep_ref[0:3, :],
            input_ref[0:3, :],
            direct_ref[0:3, :],
            jnp.zeros_like(total),
        ],
        axis=0,
    )


def recur_pre(in_x, in_y, state, edge, taps, gate_a, gate_x, rate):
    tokens, channels = in_x.shape
    blocks, span = gate_a.shape[:2]
    col = lambda rows: pl.BlockSpec((rows, span), lambda i: (0, i))
    block = pl.BlockSpec((1, span, span), lambda i: (i, 0, 0))
    cube = pl.BlockSpec((1, tokens, span), lambda i: (i, 0, 0))
    big = pltpu.HBM((tokens, channels), f32)
    return pl.pallas_call(
        recur_pre_kernel,
        grid=(blocks,),
        in_specs=[col(tokens), col(tokens), col(tokens), col(4), col(4), block, block, col(1)],
        out_specs=[col(tokens)] * 3 + [cube] * 2 + [col(tokens)] * 3 + [col(16)],
        out_shape=[pltpu.HBM((tokens, channels), bf16)]
        + [big] * 2
        + [pltpu.HBM((blocks, tokens, span), f32)] * 2
        + [big] * 3
        + [pltpu.HBM((16, channels), f32)],
        scratch_shapes=[pltpu.VMEM((tokens + 16, span), f32)],
        compiler_params=params(),
        cost_estimate=pl.CostEstimate(
            flops=2000 * tokens * channels, transcendentals=0, bytes_accessed=8 << 20
        ),
        name="recur_pre",
    )(held(in_x), held(in_y), held(state), held(edge), held(taps), held(gate_a), held(gate_x), held(rate))


def unpack(block, scratch):
    width = block.shape[2] - 128
    parts = []
    for g in range(block.shape[0] // group):
        own = block[g * group : (g + 1) * group]
        parts.append(own[:, :, 0:width].reshape(main_rows, width))
        tiles = own[:, :, width:].reshape(128, 128).astype(f32)
        parts.append(unpack_extras(tiles, scratch).astype(bf16))
    return jnp.concatenate(parts, axis=0)


def pack_into(out_ref, values, scratch):
    width = values.shape[1]
    for g in range(out_ref.shape[0] // group):
        lo = g * group_rows
        out_ref[g * group : (g + 1) * group, :, 0:width] = (
            values[lo : lo + main_rows].astype(bf16).reshape(group, main, width)
        )
        tiles = pack_extras(values[lo + main_rows : lo + group_rows], scratch)
        out_ref[g * group : (g + 1) * group, :, width:] = tiles.astype(bf16).reshape(
            group, main, 128
        )


def near_by(value):
    return pltpu.with_memory_space_constraint(value, pltpu.VMEM)


def load_beside(copies):
    @pl.when(pl.program_id(0) == 0)
    def _():
        for copy in copies:
            copy.start()

    return copies


def finish(copies):
    @pl.when(pl.program_id(0) == pl.num_programs(0) - 1)
    def _():
        for copy in copies:
            copy.wait()


anywhere = pl.BlockSpec(memory_space=pl.ANY)
resident = pl.BlockSpec(memory_space=pltpu.VMEM)


def near_kernel(core_ref, block_ref, down_ref, down_all, part_ref, down_next, scratch, sems):
    half = down_ref.shape[1]
    other = pl.multiple_of((1 - core_ref[0]) * half, half)
    copies = load_beside(
        [pltpu.make_async_copy(down_all.at[:, pl.ds(other, half)], down_next, sems.at[0])]
    )
    rows = unpack(block_ref[...], scratch)
    part_ref[...] = dot(rows, down_ref[...], inner)
    finish(copies)


def near(core, arrived, down):
    experts, _, wide = arrived.shape
    half = wide - 128
    hidden = down.shape[0]
    count = experts * (main + extra)
    size = all_groups * group_rows
    return pl.pallas_call(
        near_kernel,
        grid_spec=pltpu.PrefetchScalarGridSpec(
            num_scalar_prefetch=1,
            grid=(count // size,),
            in_specs=[
                pl.BlockSpec((all_groups * group, main, wide), lambda i, c: (i, 0, 0)),
                pl.BlockSpec((hidden, half), lambda i, c: (0, c[0])),
                anywhere,
            ],
            out_specs=[pl.BlockSpec((size, hidden), lambda i, c: (i, 0)), anywhere],
            scratch_shapes=[pltpu.VMEM((128, 128), f32), pltpu.SemaphoreType.DMA((1,))],
        ),
        out_shape=[
            jax.ShapeDtypeStruct((count, hidden), f32),
            pltpu.VMEM((hidden, half), bf16),
        ],
        compiler_params=params(),
        cost_estimate=pl.CostEstimate(
            flops=2 * count * half * hidden, transcendentals=0, bytes_accessed=9 << 20
        ),
        name="near",
    )(core, arrived, held(down), held(down))


def far_kernel(
    core_ref, block_ref, down_ref, part_ref, silu_ref, slope_ref, gate_all, up_all,
    adj_ref, gate_next, up_next, scratch, sems,
):
    half = gate_next.shape[0]
    own = pl.multiple_of(core_ref[0] * half, half)
    copies = load_beside(
        [
            pltpu.make_async_copy(gate_all.at[pl.ds(own, half)], gate_next, sems.at[0]),
            pltpu.make_async_copy(up_all.at[pl.ds(own, half)], up_next, sems.at[1]),
        ]
    )
    rows = unpack(block_ref[...], scratch)
    grad = part_ref[...] + dot(rows, down_ref[...], inner)
    hidden = grad.shape[1]
    adj_ref[:, 0:hidden] = (grad * slope_ref[...]).astype(bf16)
    adj_ref[:, hidden:] = (grad * silu_ref[...]).astype(bf16)
    finish(copies)


def far(core, arrived, down_half, part, silu, slope, gate, up):
    experts, _, wide = arrived.shape
    hidden, half = down_half.shape
    count = experts * (main + extra)
    size = all_groups * group_rows
    by_row = lambda width: pl.BlockSpec((size, width), lambda i, c: (i, 0))
    return pl.pallas_call(
        far_kernel,
        grid_spec=pltpu.PrefetchScalarGridSpec(
            num_scalar_prefetch=1,
            grid=(count // size,),
            in_specs=[
                pl.BlockSpec((all_groups * group, main, wide), lambda i, c: (i, 0, 0)),
                whole((hidden, half)),
                by_row(hidden),
                by_row(hidden),
                by_row(hidden),
                anywhere,
                anywhere,
            ],
            out_specs=[by_row(2 * hidden), anywhere, anywhere],
            scratch_shapes=[pltpu.VMEM((128, 128), f32), pltpu.SemaphoreType.DMA((2,))],
        ),
        out_shape=[
            jax.ShapeDtypeStruct((count, 2 * hidden), bf16),
            pltpu.VMEM((half, hidden), bf16),
            pltpu.VMEM((half, hidden), bf16),
        ],
        compiler_params=params(),
        cost_estimate=pl.CostEstimate(
            flops=2 * count * half * hidden, transcendentals=0, bytes_accessed=16 << 20
        ),
        name="far",
    )(core, arrived, near_by(down_half), part, silu, slope, held(gate), held(up))


def back_rows(adj, gate, up):
    hidden = gate.shape[1]
    back = dot(adj[:, 0:hidden], gate, inner) + dot(adj[:, hidden:], up, inner)
    return back.astype(bf16)


def back_own_kernel(
    core_ref, adj_ref, gate_ref, up_ref, gate_all, up_all, back_ref, gate_next, up_next, sems
):
    half = gate_next.shape[0]
    own = pl.multiple_of(core_ref[0] * half, half)
    copies = load_beside(
        [
            pltpu.make_async_copy(gate_all.at[pl.ds(own, half)], gate_next, sems.at[0]),
            pltpu.make_async_copy(up_all.at[pl.ds(own, half)], up_next, sems.at[1]),
        ]
    )
    back_ref[...] = back_rows(adj_ref[...], gate_ref[...], up_ref[...])
    finish(copies)


def back_own(core, adj, gate_half, up_half, gate_peer, up_peer):
    count = adj.shape[0]
    half, hidden = gate_half.shape
    size = all_groups * group_rows
    by_row = lambda width: pl.BlockSpec((size, width), lambda i, c: (i, 0))
    return pl.pallas_call(
        back_own_kernel,
        grid_spec=pltpu.PrefetchScalarGridSpec(
            num_scalar_prefetch=1,
            grid=(count // size,),
            in_specs=[
                by_row(2 * hidden),
                whole((half, hidden)),
                whole((half, hidden)),
                anywhere,
                anywhere,
            ],
            out_specs=[by_row(half), anywhere, anywhere],
            scratch_shapes=[pltpu.SemaphoreType.DMA((2,))],
        ),
        out_shape=[
            jax.ShapeDtypeStruct((count, half), bf16),
            pltpu.VMEM((half, hidden), bf16),
            pltpu.VMEM((half, hidden), bf16),
        ],
        compiler_params=params(),
        cost_estimate=pl.CostEstimate(
            flops=4 * count * half * hidden, transcendentals=0, bytes_accessed=7 << 20
        ),
        name="back_own",
    )(core, adj, near_by(gate_half), near_by(up_half), held(gate_peer), held(up_peer))


def back_sum_kernel(adj_ref, own_ref, gate_ref, up_ref, out_ref, packed, scratch, sems):
    parts = sems.shape[0]
    size = adj_ref.shape[0] // parts
    blocks = packed.shape[0] // parts
    copies = []
    for k in range(parts):
        rows = slice(k * size, (k + 1) * size)
        peer = back_rows(adj_ref[rows, :], gate_ref[...], up_ref[...])
        part = packed.at[k * blocks : (k + 1) * blocks]
        pack_into(part, own_ref[rows, :].astype(f32) + peer.astype(f32), scratch)
        copies.append(
            pltpu.make_async_copy(part, out_ref.at[k * blocks : (k + 1) * blocks], sems.at[k])
        )
        copies[-1].start()
    for copy in copies:
        copy.wait()


def back_sum(adj, own, gate_half, up_half, shape):
    count = adj.shape[0]
    half, hidden = gate_half.shape
    return pl.pallas_call(
        back_sum_kernel,
        grid=(1,),
        in_specs=[resident] * 4,
        out_specs=anywhere,
        scratch_shapes=[
            pltpu.VMEM(shape, bf16),
            pltpu.VMEM((128, 128), f32),
            pltpu.SemaphoreType.DMA((sum_parts,)),
        ],
        out_shape=pltpu.HBM(shape, bf16),
        compiler_params=params(),
        cost_estimate=pl.CostEstimate(
            flops=4 * count * half * hidden, transcendentals=0, bytes_accessed=7 << 20
        ),
        name="back_sum",
    )(adj, own, near_by(gate_half), near_by(up_half))


def grad_in_kernel(packed_ref, adj_ref, gate_ref, up_ref):
    grad = dot(packed_ref[...], adj_ref[...], outer).astype(bf16)
    hidden = gate_ref.shape[1]
    gate_ref[...] = grad[:, 0:hidden]
    up_ref[...] = grad[:, hidden:]


def grad_in(packed, adj):
    count, model = packed.shape
    hidden = adj.shape[1] // 2
    size = 512
    out = pl.BlockSpec((size, hidden), lambda i: (i, 0))
    return pl.pallas_call(
        grad_in_kernel,
        grid=(model // size,),
        in_specs=[pl.BlockSpec((count, size), lambda i: (0, i)), whole((count, 2 * hidden))],
        out_specs=[out, out],
        out_shape=[jax.ShapeDtypeStruct((model, hidden), bf16)] * 2,
        compiler_params=params(),
        cost_estimate=pl.CostEstimate(
            flops=4 * count * model * hidden, transcendentals=0, bytes_accessed=11 << 20
        ),
        name="grad_in",
    )(held(packed), held(adj))


def grad_down_kernel(core_ref, active_ref, near_ref, far_ref, out_ref, scratch):
    active = active_ref[...]

    @pl.when(pl.program_id(0) == 0)
    def _():
        out_ref[...] = dot(active, unpack(near_ref[...], scratch), outer).astype(bf16)

    @pl.when(pl.program_id(0) == 1)
    def _():
        out_ref[...] = dot(active, unpack(far_ref[...], scratch), outer).astype(bf16)


def grad_down_of(core, active, arrived, arrived_far):
    count, hidden = active.shape
    half = arrived.shape[2] - 128
    return pl.pallas_call(
        grad_down_kernel,
        grid_spec=pltpu.PrefetchScalarGridSpec(
            num_scalar_prefetch=1,
            grid=(2,),
            in_specs=[whole((count, hidden)), whole(arrived.shape), whole(arrived.shape)],
            out_specs=pl.BlockSpec((hidden, half), lambda i, c: (0, i + c[0] - 2 * i * c[0])),
            scratch_shapes=[pltpu.VMEM((128, 128), f32)],
        ),
        out_shape=jax.ShapeDtypeStruct((hidden, 2 * half), bf16),
        compiler_params=params(),
        cost_estimate=pl.CostEstimate(
            flops=4 * count * half * hidden, transcendentals=0, bytes_accessed=9 << 20
        ),
        name="grad_down",
    )(core, held(active), held(arrived), held(arrived_far))


def combine_kernel(core_ref, block_ref, target_ref, cot_ref, out_ref, total, scratch):
    step = pl.program_id(0)
    tokens = cot_ref.shape[0]
    rows = unpack(block_ref[...], scratch)
    size = rows.shape[0]
    place = lax.broadcasted_iota(jnp.int32, (tokens, size), 1) + step * size
    chosen = jnp.where(
        (place == target_ref[:, 0:1]) | (place == target_ref[:, 1:2]), 1.0, 0.0
    ).astype(bf16)
    found = dot(chosen, rows, plain)

    @pl.when(step == 0)
    def _():
        total[...] = found

    @pl.when(step > 0)
    def _():
        total[...] = total[...] + found

    @pl.when(step == pl.num_programs(0) - 1)
    def _():
        out_ref[...] = (cot_ref[...].astype(f32) + total[...]).astype(bf16)


def combine(core, returned, target, cotangent):
    experts, _, wide = returned.shape
    half = wide - 128
    tokens = cotangent.shape[0]
    return pl.pallas_call(
        combine_kernel,
        grid_spec=pltpu.PrefetchScalarGridSpec(
            num_scalar_prefetch=1,
            grid=(experts // (all_groups * group),),
            in_specs=[
                pl.BlockSpec((all_groups * group, main, wide), lambda i, c: (i, 0, 0)),
                whole((tokens, 8)),
                pl.BlockSpec((tokens, half), lambda i, c: (0, c[0])),
            ],
            out_specs=whole((tokens, half)),
            scratch_shapes=[pltpu.VMEM((tokens, half), f32), pltpu.VMEM((128, 128), f32)],
        ),
        out_shape=jax.ShapeDtypeStruct((tokens, half), bf16),
        compiler_params=params(),
        name="combine",
    )(core, returned, held(target), held(cotangent))


def write_shares(ref, values):
    pieces = values.astype(bf16).reshape(ref.shape[0], 4, 8, values.shape[1])
    channels = values.shape[1]
    for k in range(4):
        ref[:, :, channels * k : channels * (k + 1)] = pieces[:, k]


def own_kernel(core_ref, own_ref, weight_ref, mixed_ref, grad_ref, share_out, share, sems):
    owners = share.shape[0]
    at = pl.ds(pl.multiple_of(core_ref[0] * owners, owners), owners)
    own = own_ref[...]
    write_shares(share, dot(own, mixed_ref[...], outer))
    copy = pltpu.make_async_copy(share, share_out.at[at, :, pl.ds(0, share.shape[2])], sems.at[0])
    copy.start()
    grad_ref[...] = dot(own, weight_ref[...], plain)
    copy.wait()


def own_part(core, own, weight, mixed, owners):
    tokens, half = own.shape
    channels = mixed.shape[1]
    return pl.pallas_call(
        own_kernel,
        grid_spec=pltpu.PrefetchScalarGridSpec(
            num_scalar_prefetch=1,
            grid=(1,),
            in_specs=[
                whole((tokens, half)),
                pl.BlockSpec((half, channels), lambda i, c: (c[0], 0)),
                whole((tokens, channels)),
            ],
            out_specs=[whole((tokens, channels)), anywhere],
            scratch_shapes=[
                pltpu.VMEM((owners // 2, 8, 4 * channels), bf16),
                pltpu.SemaphoreType.DMA((1,)),
            ],
        ),
        out_shape=[
            jax.ShapeDtypeStruct((tokens, channels), f32),
            pltpu.HBM((owners, 8, 4 * channels + 128), bf16),
        ],
        compiler_params=params(),
        cost_estimate=pl.CostEstimate(
            flops=4 * tokens * half * channels, transcendentals=0, bytes_accessed=4 << 20
        ),
        name="own_part",
    )(core, own, weight, mixed)


def segment_scan(values, ahead_ref, state_grad, local, b):
    length = state_grad.shape[1] // segments
    state_grad[b] = values[:, 128 * b : 128 * (b + 1)]
    value = None
    for j in reversed(range(length)):
        at = pl.ds(j, segments, stride=length)
        here = state_grad[b, at, :]
        value = here if value is None else here + ahead_ref[b, at, :] * value
        local[b, at, :] = value
    return value


def scan_kernel(
    core_ref, peer_ref, weight_ref, mixed_ref, part_ref, gelu_ref, ahead_ref, product_ref, first_ref,
    share_in, share_out, head_ref,
    state_grad, local, share, lines, sems,
):
    owners = share.shape[0]
    other = pl.ds(pl.multiple_of((1 - core_ref[0]) * owners, owners), owners)
    columns = share.shape[2]
    peer = peer_ref[...]
    grad = part_ref[...] + dot(peer, weight_ref[...], plain)
    write_shares(share, dot(peer, mixed_ref[...], outer))
    main_copy = pltpu.make_async_copy(share, share_out.at[other, :, pl.ds(0, columns)], sems.at[0])
    main_copy.start()
    values = grad * gelu_ref[...]
    blocks, tokens, _ = state_grad.shape
    length = tokens // segments
    tiles = []
    for b in range(blocks):
        at = slice(128 * b, 128 * (b + 1))
        value = segment_scan(values, ahead_ref, state_grad, local, b)
        product = product_ref[b, pl.ds(0, segments, stride=length), :]
        carry = value[segments - 1 : segments]
        for s in reversed(range(1, segments - 1)):
            carry = value[s : s + 1] + product[s : s + 1] * carry
        ends = local[b, 0:3, :] + product_ref[b, 0:3, :] * carry
        tiles.append(first_ref[0:1, at] * ends[0:1])
        head_ref[:, at] = jnp.concatenate(
            [ends, first_ref[3:15, at], jnp.zeros((1, 128), f32)], axis=0
        )
    power = [first_ref[2:3, 128 * b : 128 * (b + 1)] for b in range(blocks)]
    line = jnp.concatenate(power + tiles, axis=0).astype(bf16)
    lines[...] = jnp.broadcast_to(line[None], lines.shape)
    line_copy = pltpu.make_async_copy(lines, share_out.at[:, :, pl.ds(columns, 128)], sems.at[1])
    line_copy.start()
    main_copy.wait()
    line_copy.wait()


def scan(core, peer, weight, mixed, part, shares, gelu, ahead, product, first):
    tokens, half = peer.shape
    channels = weight.shape[1]
    owners = shares.shape[0]
    return pl.pallas_call(
        scan_kernel,
        grid_spec=pltpu.PrefetchScalarGridSpec(
            num_scalar_prefetch=1,
            grid=(1,),
            in_specs=[
                whole((tokens, half)),
                pl.BlockSpec((half, channels), lambda i, c: (1 - c[0], 0)),
                whole((tokens, channels)),
                whole((tokens, channels)),
                whole((tokens, channels)),
                whole(ahead.shape),
                whole(ahead.shape),
                whole((16, channels)),
                anywhere,
            ],
            out_specs=[anywhere, whole((16, channels))],
            scratch_shapes=[
                pltpu.VMEM(ahead.shape, f32),
                pltpu.VMEM(ahead.shape, f32),
                pltpu.VMEM((owners // 2, 8, 4 * channels), bf16),
                pltpu.VMEM((owners, 8, 128), bf16),
                pltpu.SemaphoreType.DMA((2,)),
            ],
        ),
        out_shape=[pltpu.HBM(shares.shape, bf16), pltpu.HBM((16, channels), f32)],
        input_output_aliases={9: 0},
        compiler_params=params(),
        cost_estimate=pl.CostEstimate(
            flops=4 * tokens * half * channels, transcendentals=0, bytes_accessed=9 << 20
        ),
        name="scan",
    )(core, peer, weight, mixed, part, gelu, ahead, product, first, held(shares))


def local_kernel(
    core_ref, peer_ref, weight_ref, part_ref, slope_ref, gelu_ref, ahead_ref,
    grad_y_ref, local_ref, state_grad,
):
    grad = part_ref[...] + dot(peer_ref[...], weight_ref[...], plain)
    grad_y_ref[...] = grad * slope_ref[...]
    values = grad * gelu_ref[...]
    for b in range(state_grad.shape[0]):
        segment_scan(values, ahead_ref, state_grad, local_ref, b)


def local_scan(core, peer, weight, part, slope, gelu, ahead):
    tokens, half = peer.shape
    channels = weight.shape[1]
    return pl.pallas_call(
        local_kernel,
        grid_spec=pltpu.PrefetchScalarGridSpec(
            num_scalar_prefetch=1,
            grid=(1,),
            in_specs=[
                whole((tokens, half)),
                pl.BlockSpec((half, channels), lambda i, c: (1 - c[0], 0)),
                whole((tokens, channels)),
                whole((tokens, channels)),
                whole((tokens, channels)),
                whole(ahead.shape),
            ],
            out_specs=[whole((tokens, channels)), whole(ahead.shape)],
            scratch_shapes=[pltpu.VMEM(ahead.shape, f32)],
        ),
        out_shape=[pltpu.HBM((tokens, channels), f32), pltpu.HBM(ahead.shape, f32)],
        compiler_params=params(),
        cost_estimate=pl.CostEstimate(
            flops=2 * tokens * half * channels, transcendentals=0, bytes_accessed=9 << 20
        ),
        name="local_scan",
    )(core, held(peer), held(weight), held(part), held(slope), held(gelu), held(ahead))


def tail_kernel(
    place_ref, line_ref, head_ref, taps_ref, a_ref, i_ref, *rest,
):
    sources, (out_hbm,), stores = rest[0:5], rest[5:6], rest[6:]
    local_ref, product_ref, keep_ref, input_ref, direct_ref = buffers = stores[0:5]
    adjoint, grads, out, in_sems, out_sems = stores[5:]
    blocks, tokens, span = local_ref.shape
    length = tokens // segments
    place = place_ref[0]

    def column(ref, c):
        return ref.at[c] if len(ref.shape) == 3 else ref.at[:, pl.ds(span * c, span)]

    copies = [
        [
            pltpu.make_async_copy(column(source, c), column(buffer, c), in_sems.at[c, k])
            for k, (source, buffer) in enumerate(zip(sources, buffers))
        ]
        for c in range(blocks)
    ]
    for group_copies in copies:
        for copy in group_copies:
            copy.start()

    own = jnp.zeros((4, span), f32)
    beyond = jnp.zeros((4, span), f32)
    for j in reversed(range(line_ref.shape[0])):
        line = line_ref[j].astype(f32)
        decay = jnp.exp(-line[0:4])
        own = jnp.where(j > place, line[4:8] + decay * own, own)
        beyond = jnp.where(j > place + 1, line[4:8] + decay * beyond, beyond)

    results = []
    for c in range(blocks):
        at = slice(span * c, span * (c + 1))

        def conv_grad(value, keep, gate, direct):
            keep = (value * keep).astype(bf16)
            gate = (value * gate).astype(bf16)
            return value * direct + dot(keep, a_ref[c], inner) + dot(gate, i_ref[c], inner)

        for copy in copies[c]:
            copy.wait()
        carry = own[c : c + 1]
        for s in reversed(range(segments)):
            rows = slice(s * length, (s + 1) * length)
            piece = local_ref[c, rows, :] + product_ref[c, rows, :] * carry
            adjoint[rows, :] = piece
            carry = piece[0:1]
        grads[0:tokens, :] = conv_grad(
            adjoint[...], keep_ref[:, at], input_ref[:, at], direct_ref[:, at]
        )
        head = head_ref[:, at]
        spare = jnp.zeros((5, span), f32)
        three = lambda k: jnp.concatenate([head[3 * k : 3 * k + 3], spare], axis=0)
        later = three(0) + three(1) * beyond[c : c + 1]
        grads[tokens : tokens + 8, :] = conv_grad(later, three(2), three(3), three(4))
        total = taps_ref[0:1, at] * grads[3 : 3 + tokens, :]
        for j in range(1, 4):
            total = total + taps_ref[j : j + 1, at] * grads[3 - j : 3 - j + tokens, :]
        out[:, at] = total
        results.append(
            pltpu.make_async_copy(column(out, c), column(out_hbm, c), out_sems.at[c])
        )
        results[-1].start()
    for copy in results:
        copy.wait()


def tail(place, shares, head, local, product, keep, gate, direct, gate_a, gate_x, taps):
    blocks, tokens, span = local.shape
    channels = blocks * span
    owners, rows, _ = shares.shape
    sources = (local, product, keep, gate, direct)
    return pl.pallas_call(
        tail_kernel,
        grid_spec=pltpu.PrefetchScalarGridSpec(
            num_scalar_prefetch=1,
            grid=(1,),
            in_specs=[
                pl.BlockSpec((owners, rows, 128), lambda i, c: (0, 0, 4 * channels // 128)),
                whole((16, channels)),
                whole((4, channels)),
                whole(gate_a.shape),
                whole(gate_x.shape),
            ]
            + [anywhere] * 5,
            out_specs=anywhere,
            scratch_shapes=[pltpu.VMEM(value.shape, f32) for value in sources]
            + [
                pltpu.VMEM((tokens, span), f32),
                pltpu.VMEM((tokens + 8, span), f32),
                pltpu.VMEM((tokens, channels), f32),
                pltpu.SemaphoreType.DMA((blocks, 5)),
                pltpu.SemaphoreType.DMA((blocks,)),
            ],
        ),
        out_shape=pltpu.HBM((tokens, channels), f32),
        compiler_params=params(),
        name="tail",
    )(place, shares, head, held(taps), held(gate_a), held(gate_x), *(held(v) for v in sources))


def exchange(value, axis):
    return lax.all_to_all(value, axis, split_axis=0, concat_axis=0, tiled=True)


def swapped(value):
    return lax.ppermute(value, "tp", [(0, 1), (1, 0)])


def shifted(value, axis, by):
    devices = lax.axis_size(axis)
    pairs = [(i, i + by) for i in range(devices) if 0 <= i + by < devices]
    return lax.ppermute(value, axis, pairs)


def body(
    cotangent,
    routes,
    route_weight,
    expert_rows,
    gate_w,
    up_w,
    down_w,
    in_x,
    in_y,
    state,
    conv_taps,
    gate_a,
    gate_x,
    decay_rate,
    out_weight,
):
    tokens = cotangent.shape[0]
    experts = lax.axis_size("sp")
    core = lax.axis_index("tp").astype(jnp.int32).reshape(1)
    taps = conv_taps.shape[0]
    channels = in_x.shape[1]

    place = lax.axis_index("sp").astype(jnp.int32).reshape(1)

    edge = shifted(
        jnp.concatenate([in_x[tokens - taps + 1 :], state[tokens - 1 :]], axis=0), "sp", 1
    )
    outgoing, target = send(core, routes.T, route_weight.T, cotangent, experts)
    arrived = exchange(outgoing, "sp")
    target = target.T

    gate_peer = swapped(gate_w[0])
    up_peer = swapped(up_w[0])
    packed, silu, slope, active = expert_pre(expert_rows[0], gate_w[0], up_w[0])
    mixed, y_slope, gelu, ahead, product, keep_part, input_part, direct, first = recur_pre(
        in_x, in_y, state, edge, conv_taps, gate_a, gate_x, decay_rate[None]
    )

    arrived_far = swapped(arrived)
    part, down_half = near(core, arrived, down_w[0])
    adj, gate_half, up_half = far(
        core, arrived_far, down_half, part, silu, slope, gate_w[0], up_w[0]
    )
    adj_peer = swapped(adj)
    own, gate_half, up_half = back_own(core, adj, gate_half, up_half, gate_peer, up_peer)
    returning = back_sum(adj_peer, own, gate_half, up_half, arrived.shape)
    returned = exchange(returning, "sp")

    grad_gate, grad_up = grad_in(packed, adj)
    grad_down = grad_down_of(core, active, arrived, arrived_far)

    stream_own = combine(core, returned, target, cotangent)
    stream_peer = swapped(stream_own)
    part, shares = own_part(core, stream_own, out_weight, mixed, experts)
    outgoing, head = scan(
        core, stream_peer, out_weight, mixed, part, shares, gelu, ahead, product, first
    )
    grad_y, local = local_scan(core, stream_peer, out_weight, part, y_slope, gelu, ahead)
    head = shifted(head, "sp", -1)
    shares = exchange(outgoing, "sp")
    grad_x = tail(
        place, shares, head, local, product, keep_part, input_part, direct,
        gate_a, gate_x, conv_taps,
    )
    summed = jnp.sum(shares[:, :, : 4 * channels].astype(f32), axis=0)
    grad_proj = jnp.concatenate(
        [summed[:, channels * k : channels * (k + 1)] for k in range(4)], axis=0
    )
    return (grad_gate[None], grad_up[None], grad_down[None], grad_proj, grad_x, grad_y)


def solution(mesh):
    in_specs = (
        P("sp", None),
        P("sp", None),
        P("sp", None),
        P("sp", None, None),
        P("sp", None, "tp"),
        P("sp", None, "tp"),
        P("sp", "tp", None),
        P("sp", "tp"),
        P("sp", "tp"),
        P("sp", "tp"),
        P(None, "tp"),
        P("tp", None, None),
        P("tp", None, None),
        P("tp"),
        P(None, "tp"),
    )
    out_specs = (
        P("sp", None, "tp"),
        P("sp", None, "tp"),
        P("sp", "tp", None),
        P("sp", "tp"),
        P("sp", "tp"),
        P("sp", "tp"),
    )
    return jax.shard_map(body, mesh=mesh, in_specs=in_specs, out_specs=out_specs, check_vma=False)
```
